32 devices in a mesh: ep: 16 (over z, y, x), tp: 2 (over core).
Axes of the slice: x: 2, y: 2, z: 4, core: 2. Of those that a mesh axis runs over, the one named last changes fastest.
Arguments:
- tokens: bfloat16 [256, 2048], P('ep'), may hold values from -6 to 6
- lengths: int32 [256], P('ep'), may hold values from 1 to 1024, as said below
- attn_gain: float32 [2048], replicated, may hold values from 0.1 to 1.9
- w_query: bfloat16 [2048, 1024], P(None, 'tp'), may hold values from -0.125 to 0.125
- w_key: bfloat16 [2048, 128], P(None, 'tp'), may hold values from -0.125 to 0.125
- w_value: bfloat16 [2048, 128], P(None, 'tp'), may hold values from -0.125 to 0.125
- head_bias: float32 [16], P('tp'), may hold values from -7 to -2
- key_cache: bfloat16 [256, 2, 64, 1024], P('ep', 'tp'), may hold values from -6 to 6
- value_cache: bfloat16 [256, 2, 64, 1024], P('ep', 'tp'), may hold values from -6 to 6
- w_attn_out: bfloat16 [1024, 2048], P('tp'), may hold values from -0.1875 to 0.1875
- ffn_gain: float32 [2048], replicated, may hold values from 0.1 to 1.9
- w_router: bfloat16 [2048, 16], replicated, may hold values from -0.125 to 0.125
- routes: int32 [256, 6], P('ep'), may hold values from 0 to 15, all different within a row; in each aligned block of 16 rows (0 to 15, 16 to 31, ...) at most 12 rows name the same one
- w_dense_gate: bfloat16 [2048, 512], P('ep', 'tp'), may hold values from -0.125 to 0.125
- w_dense_up: bfloat16 [2048, 512], P('ep', 'tp'), may hold values from -0.125 to 0.125
- w_dense_down: bfloat16 [512, 2048], P('tp', 'ep'), may hold values from -0.25 to 0.25
- dense_mix: float32 [2048], replicated, may hold values from -0.125 to 0.125
- w_expert_gate: bfloat16 [16, 2048, 512], P('ep', None, 'tp'), may hold values from -0.125 to 0.125
- w_expert_up: bfloat16 [16, 2048, 512], P('ep', None, 'tp'), may hold values from -0.125 to 0.125
- w_expert_down: bfloat16 [16, 512, 2048], P('ep', 'tp'), may hold values from -0.25 to 0.25
Outputs:
- layer_out: bfloat16 [256, 2048], P('ep', 'tp')
- new_keys: bfloat16 [256, 128], P('ep', 'tp')
- new_values: bfloat16 [256, 128], P('ep', 'tp')
The draws below stay inside these ranges and needn't reach their ends.
Inputs may be any that keep to these rules, and one draw needn't show every extreme that they name: `lengths`: every sequence holds between 1 and 1024 cached positions; in every draw some sequence holds exactly 1024. `routes`: each token names 6 different experts. Among the rows of one device no expert is named by more than 12 rows.
All inputs are finite; a program needn't handle non-finite values.
Results may differ from the reference program's by a relative error of at most 0.014.
Values may be sent and summed in bfloat16 or wider, within the bound.
A program may use at most 64 MiB of HBM per device.

```python
import math
import jax
import jax.numpy as jnp
import numpy as np
from jax import lax

D = 2048
HEADS = 16
KV_HEADS = 2
HEAD = 64
EXPERT_WIDTH = 512
SHARED = 512
TOP_K = 6
SEQ_DEV = 16
CACHE = 1024
EXPERTS = 16
TOKENS = 256
CAP = 12
N_EP = 16
N_TP = 2


def draw_lengths(key, part):
    key_caps = jax.random.fold_in(key, 11)
    key_rows = jax.random.fold_in(key, 12)
    key_full = jax.random.fold_in(key, 13)
    group_total = TOKENS // SEQ_DEV
    device_caps = jax.random.randint(key_caps, (group_total, 1), CACHE // 8, CACHE + 1)
    drawn = jax.random.randint(key_rows, (group_total, SEQ_DEV), 1, device_caps + 1).reshape(-1)
    full_at = jax.random.randint(key_full, (), 0, TOKENS)
    drawn = jnp.where(jnp.arange(TOKENS, dtype=jnp.int32) == full_at, CACHE, drawn)
    return drawn.astype(jnp.int32)


def levels(rng, shape, pieces, least, top_value):
    level, own = 1.0, jax.random.fold_in(rng, 6)
    for position, shards_of in pieces:
        steps = jnp.exp(jax.random.uniform(jax.random.fold_in(own, position), (shards_of,), jnp.float32, least / len(pieces), top_value / len(pieces)))
        level = level * jnp.repeat(steps, shape[position] // shards_of).reshape([-1 if axis == position else 1 for axis in range(len(shape))])
    return level


def shared_out(own_key, own, number, rows, number_of, top, limit, slope):
    order = jax.random.permutation(own_key, number_of)
    crowded, ordinary = shares(number_of, rows * top, limit, slope, True), shares(number_of, rows * top, limit, slope, False)
    places = jnp.arange(number_of)

    def named(sizes, rotation):
        used = int((sizes > 0).sum())
        fixed = max(1, used // 4)
        shifted = fixed + (places - fixed + rotation * (used - fixed)) % max(1, number_of - fixed)
        return jnp.zeros((number_of,), jnp.int32).at[order[jnp.where(places < fixed, places, shifted)]].set(jnp.asarray(sizes, jnp.int32))

    sizes = jnp.where(number % 4 == 0, named(crowded, number // 4), named(ordinary, number - number // 4 - 1))
    mixed = jax.random.permutation(jax.random.fold_in(own, 3), number_of)
    donor, taker = mixed[0:number_of // 2 * 2:2], mixed[1:number_of // 2 * 2:2]
    margin = jnp.minimum(sizes[donor] - 1, limit - sizes[taker]) // 2
    margin = jnp.where((donor == order[0]) | (taker == order[0]) | (sizes[taker] == 0), 0, jnp.maximum(margin, 0))
    shifted = jax.random.randint(jax.random.fold_in(own, 4), (number_of // 2,), 0, 1 << 20) % (margin + 1)
    sizes = sizes.at[donor].add(-shifted).at[taker].add(shifted)
    members = jnp.searchsorted(jnp.cumsum(sizes), jnp.arange(rows * top), side="right").astype(jnp.int32)
    listing = members.reshape(top, rows).T
    listing = listing[jax.random.permutation(jax.random.fold_in(own, 1), rows)]
    rotation = jax.random.randint(jax.random.fold_in(own, 2), (rows, 1), 0, top)
    return jnp.take_along_axis(listing, (jnp.arange(top)[None, :] + rotation) % top, axis=1)


def shares(number_of, total, most, skew, full):
    loads = [(1 << 20) // math.isqrt(standing ** skew) + 1 for standing in range(1, number_of + 1)]
    largest = most if full else min(most, max(-(-total // number_of), total * loads[0] // sum(loads)))
    least = 1 if total - largest >= number_of - 1 else 0
    given, rest = [largest] + [least] * (number_of - 1), total - largest - least * (number_of - 1)
    while rest > 0:
        free = [i for i in range(1, number_of) if given[i] < largest] or [i for i in range(1, number_of) if given[i] < most]
        mass, budget = sum([loads[i] for i in free]), rest
        for i in free:
            addition = min(most - given[i], max(1, budget * loads[i] // mass), rest)
            given[i] = given[i] + addition
            rest = rest - addition
    return np.array(given)


def gaussian(own_key, extent, spread, most, split=(), held_as=jnp.bfloat16):
    level = levels(own_key, extent, split, -0.22, 0.18) if split else 1.0
    entries = jax.random.normal(own_key, extent, jnp.float32) * spread * level
    return jnp.minimum(jnp.maximum(entries, -most), most).astype(held_as)


def setup_inputs(seed: int = 0) -> dict:
    streams_of = jax.random.split(jax.random.key(seed), 21)
    tokens = gaussian(streams_of[0], (TOKENS, D), 1.0, 6.0, ((0, 16),))
    lengths = draw_lengths(jax.random.fold_in(streams_of[20], 71), 0)
    attn_gain = jnp.clip(1.0 + 0.18 * jax.random.normal(streams_of[2], (D,), jnp.float32), 0.1, 1.9)
    w_query = gaussian(streams_of[3], (D, HEADS * HEAD), D ** -0.5, 0.125, ((1, 2),))
    w_key = gaussian(streams_of[4], (D, KV_HEADS * HEAD), D ** -0.5, 0.125, ((1, 2),))
    w_value = gaussian(streams_of[5], (D, KV_HEADS * HEAD), D ** -0.5, 0.125, ((1, 2),))
    head_bias = jnp.clip(-7.0 + 5.0 * jax.random.uniform(streams_of[6], (HEADS,), jnp.float32) ** levels(streams_of[6], (HEADS,), ((0, 2),), -0.2, 0.2), -7.0, -2.0)
    key_cache = gaussian(streams_of[7], (TOKENS, KV_HEADS, HEAD, CACHE), 1.0, 6.0, ((0, 16), (1, 2)))
    value_cache = gaussian(streams_of[8], (TOKENS, KV_HEADS, HEAD, CACHE), 1.0, 6.0, ((0, 16), (1, 2)))
    w_attn_out = gaussian(streams_of[9], (HEADS * HEAD, D), (HEADS * HEAD) ** -0.5, 0.1875, ((0, 2),))
    ffn_gain = jnp.clip(1.0 + 0.18 * jax.random.normal(streams_of[10], (D,), jnp.float32), 0.1, 1.9)
    w_router = gaussian(streams_of[11], (D, EXPERTS), D ** -0.5, 0.125)
    routes_keys = jax.random.split(jax.random.fold_in(streams_of[12], 1), TOKENS // SEQ_DEV)
    routes_turns = jax.random.permutation(jax.random.fold_in(streams_of[12], 3), TOKENS // SEQ_DEV)
    routes = jax.vmap(lambda own, number: shared_out(jax.random.fold_in(streams_of[12], 2), own, number, SEQ_DEV, EXPERTS, TOP_K, CAP, 2))(routes_keys, routes_turns).reshape((TOKENS, TOP_K))
    w_dense_gate = gaussian(streams_of[13], (D, SHARED), D ** -0.5, 0.125, ((0, 16), (1, 2)))
    w_dense_up = gaussian(streams_of[14], (D, SHARED), D ** -0.5, 0.125, ((0, 16), (1, 2)))
    w_dense_down = gaussian(streams_of[15], (SHARED, D), SHARED ** -0.5, 0.25, ((0, 2), (1, 16)))
    dense_mix = gaussian(streams_of[16], (D,), D ** -0.5, 0.125, (), jnp.float32)
    w_expert_gate = gaussian(streams_of[17], (EXPERTS, D, EXPERT_WIDTH), D ** -0.5, 0.125, ((0, 16), (2, 2)))
    w_expert_up = gaussian(streams_of[18], (EXPERTS, D, EXPERT_WIDTH), D ** -0.5, 0.125, ((0, 16), (2, 2)))
    w_expert_down = gaussian(streams_of[19], (EXPERTS, EXPERT_WIDTH, D), EXPERT_WIDTH ** -0.5, 0.25, ((0, 16), (1, 2)))
    return {"tokens": tokens, "lengths": lengths, "attn_gain": attn_gain, "w_query": w_query, "w_key": w_key, "w_value": w_value, "head_bias": head_bias, "key_cache": key_cache, "value_cache": value_cache, "w_attn_out": w_attn_out, "ffn_gain": ffn_gain, "w_router": w_router, "routes": routes, "w_dense_gate": w_dense_gate, "w_dense_up": w_dense_up, "w_dense_down": w_dense_down, "dense_mix": dense_mix, "w_expert_gate": w_expert_gate, "w_expert_up": w_expert_up, "w_expert_down": w_expert_down}


def rms_scale(values, gain):
    wide = values.astype(jnp.float32)
    return wide * lax.rsqrt(lax.optimization_barrier(jnp.mean(wide * wide, axis=-1, keepdims=True)) + 1e-06) * gain

def halves_sum(hidden, down, rows):
    split_hidden = hidden.reshape(rows, N_TP, -1).astype(jnp.float32)
    split_down = down.reshape(N_TP, -1, D).astype(jnp.float32)
    parts = jnp.einsum('rnf,nfd->nrd', split_hidden, split_down).astype(jnp.bfloat16)
    return lax.optimization_barrier(jnp.sum(parts.astype(jnp.float32), axis=0))

def reference(tokens, lengths, attn_gain, w_query, w_key, w_value, head_bias, key_cache, value_cache, w_attn_out, ffn_gain, w_router, routes, w_dense_gate, w_dense_up, w_dense_down, dense_mix, w_expert_gate, w_expert_up, w_expert_down):
    normed = rms_scale(tokens, attn_gain).astype(jnp.bfloat16)
    queries = jnp.dot(normed, w_query, preferred_element_type=jnp.float32).astype(jnp.bfloat16)
    new_keys = jnp.dot(normed, w_key, preferred_element_type=jnp.float32).astype(jnp.bfloat16)
    new_values = jnp.dot(normed, w_value, preferred_element_type=jnp.float32).astype(jnp.bfloat16)
    group_size = HEADS // KV_HEADS
    block_total = TOKENS // SEQ_DEV
    grouped = queries.reshape(block_total, SEQ_DEV, KV_HEADS, group_size, HEAD)
    key_blocks = key_cache.reshape(block_total, SEQ_DEV, KV_HEADS, HEAD, CACHE)
    value_blocks = value_cache.reshape(block_total, SEQ_DEV, KV_HEADS, HEAD, CACHE)
    length_blocks = lengths.reshape(block_total, SEQ_DEV)
    head_shift = head_bias.reshape(1, KV_HEADS, group_size, 1)

    def attend(inputs):
        block_queries, block_keys, block_values, block_lengths = inputs
        scores = jnp.einsum('skgd,skdc->skgc', block_queries.astype(jnp.float32), block_keys.astype(jnp.float32)) * HEAD ** (-0.5) + head_shift
        visible = (jnp.arange(CACHE, dtype=jnp.int32)[None, :] < block_lengths[:, None])[:, None, None, :]
        log_keep = jnp.where(visible, jax.nn.log_sigmoid(-scores), 0.0)
        log_after = lax.cumsum(log_keep, axis=3, reverse=True) - log_keep
        weights = jnp.where(visible, jnp.exp(jax.nn.log_sigmoid(scores) + log_after), 0.0).astype(jnp.bfloat16)
        mixed = jnp.einsum('skgc,skdc->skgd', weights.astype(jnp.float32), block_values.astype(jnp.float32))
        return mixed.reshape(SEQ_DEV, HEADS * HEAD).astype(jnp.bfloat16)
    heads_out = lax.map(attend, (grouped, key_blocks, value_blocks, length_blocks)).reshape(TOKENS, HEADS * HEAD)
    attn = halves_sum(heads_out, w_attn_out, TOKENS)
    residual = (tokens.astype(jnp.float32) + attn).astype(jnp.bfloat16)
    normed2 = rms_scale(residual, ffn_gain).astype(jnp.bfloat16)
    probs = jax.nn.sigmoid(jnp.dot(normed2, w_router, preferred_element_type=jnp.float32))
    hits = routes[:, :, None] == jnp.arange(EXPERTS, dtype=jnp.int32)[None, None, :]
    picked = lax.optimization_barrier(jnp.sum(jnp.where(hits, probs[:, None, :], 0.0), axis=-1))
    gates = picked / lax.optimization_barrier(jnp.sum(picked, axis=-1, keepdims=True)) * 2.5
    flat_routes = routes.reshape(-1)
    route_total = TOKENS * TOP_K
    bound = N_EP * CAP
    padded_inputs = jnp.concatenate([normed2, jnp.zeros((1, D), jnp.bfloat16)], axis=0)

    def expert_pass(inputs):
        expert_id, gate_w, up_w, down_w = inputs
        chosen = jnp.nonzero(flat_routes == expert_id, size=bound, fill_value=route_total)[0].astype(jnp.int32)
        rows_in = padded_inputs[chosen // TOP_K]
        gate_rows = jnp.dot(rows_in, gate_w, preferred_element_type=jnp.float32)
        up_rows = jnp.dot(rows_in, up_w, preferred_element_type=jnp.float32)
        hidden = (jax.nn.silu(gate_rows) * up_rows).astype(jnp.bfloat16)
        return (halves_sum(hidden, down_w, bound).astype(jnp.bfloat16), chosen)
    expert_rows, chosen_all = lax.map(expert_pass, (jnp.arange(EXPERTS, dtype=jnp.int32), w_expert_gate, w_expert_up, w_expert_down))
    route_rows = jnp.zeros((route_total + 1, D), jnp.bfloat16).at[chosen_all.reshape(-1)].set(expert_rows.reshape(-1, D))[:route_total]
    routed = lax.optimization_barrier(jnp.sum(gates[:, :, None] * route_rows.reshape(TOKENS, TOP_K, D).astype(jnp.float32), axis=1))
    dense_gate_rows = jnp.dot(normed2, w_dense_gate, preferred_element_type=jnp.float32)
    dense_up_rows = jnp.dot(normed2, w_dense_up, preferred_element_type=jnp.float32)
    dense_hidden = (jax.nn.silu(dense_gate_rows) * dense_up_rows).astype(jnp.bfloat16)
    dense = halves_sum(dense_hidden, w_dense_down, TOKENS)
    mix_gate = jax.nn.sigmoid(lax.optimization_barrier(jnp.sum(normed2.astype(jnp.float32) * dense_mix, axis=-1)))
    layer_out = (residual.astype(jnp.float32) + mix_gate[:, None] * dense + routed).astype(jnp.bfloat16)
    return (layer_out, new_keys, new_values)
```

```python
import functools

import jax
import jax.numpy as jnp
from jax import lax
from jax.experimental import pallas as pl
from jax.experimental.pallas import tpu as pltpu
from jax.sharding import PartitionSpec as P

MESH = pl.DeviceIdType.MESH


def whole_layer(
    n,
    group_size,
    tokens_ref,
    attn_gain_ref,
    lengths_ref,
    bias_ref,
    w_key_ref,
    w_value_ref,
    gain_ref,
    router_ref,
    routes_ref,
    mix_ref,
    dense_gate_ref,
    dense_up_ref,
    down_ref,
    w_query_hbm,
    w_out_hbm,
    w_gate_hbm,
    w_up_hbm,
    w_down_hbm,
    keys_hbm,
    values_hbm,
    out_ref,
    new_keys_ref,
    new_values_ref,
    w_query,
    w_out,
    w_gate,
    w_up,
    w_down,
    keys,
    values,
    load_sem,
    keys_sem,
    values_sem,
    query_ref,
    score_ref,
    read_ref,
    normed_ref,
    dense_gate_all,
    dense_up_all,
    down_all,
    attn_mine,
    attn_peer,
    res_ref,
    norm_all,
    part_send,
    part_recv,
    hidden_ref,
    dense_all,
    cols_send,
    cols_recv,
    other_ref,
    mine_ref,
    peer_ref,
    back_send,
    back_recv,
    pair_sems,
    dense_gate_sems,
    dense_up_sems,
    down_sems,
    norm_sems,
    pass_sems,
    part_sems,
    dense_sems,
    cols_send_sem,
    cols_recv_sem,
    back_sems,
):
    me = lax.axis_index("ep")
    core = lax.axis_index("tp")
    peer = 1 - core
    rows, model = tokens_ref.shape
    half = model // 2
    width = dense_gate_ref.shape[0]
    window = width * group_size
    place = me % group_size
    team = me // group_size
    teams = n // group_size
    first = team * window
    owner = first // half
    lane = pl.multiple_of(first % half, window)
    f32 = jnp.float32
    local_heads = bias_ref.shape[1]
    head_dim, cache_len = keys_hbm.shape[1:]
    span = 4

    def remote(source, target, send_sem, recv_sem, ep, tp):
        return pltpu.make_async_remote_copy(
            src_ref=source,
            dst_ref=target,
            send_sem=send_sem,
            recv_sem=recv_sem,
            device_id=(ep, tp),
            device_id_type=MESH,
        )

    pairs = (
        (w_query_hbm, w_query),
        (w_gate_hbm, w_gate),
        (w_up_hbm, w_up),
        (w_down_hbm, w_down),
        (w_out_hbm, w_out),
    )
    loads = [
        pltpu.make_async_copy(source, target, load_sem.at[i])
        for i, (source, target) in enumerate(pairs)
    ]

    def keys_load(c):
        block = pl.ds(c * span, span)
        return pltpu.make_async_copy(keys_hbm.at[block], keys.at[block], keys_sem.at[c])

    def values_load(c):
        block = pl.ds(c * span, span)
        return pltpu.make_async_copy(values_hbm.at[block], values.at[block], values_sem.at[c])

    loads[0].start()
    for c in range(rows // span):
        keys_load(c).start()
        values_load(c).start()
    for load in (loads[4], loads[1], loads[2], loads[3]):
        load.start()

    barrier = pltpu.get_barrier_semaphore()

    def greet(k, carry):
        other = lax.rem(me + k, n)
        pl.semaphore_signal(barrier, inc=1, device_id=(other, core), device_id_type=MESH)
        pl.semaphore_signal(barrier, inc=1, device_id=(other, peer), device_id_type=MESH)
        return carry

    lax.fori_loop(1, n, greet, 0)
    pl.semaphore_signal(barrier, inc=1, device_id=(me, peer), device_id_type=MESH)

    start = tokens_ref[...].astype(f32)
    normed_ref[...] = (
        start
        * lax.rsqrt(jnp.mean(start * start, axis=-1, keepdims=True) + 1e-06)
        * attn_gain_ref[...]
    ).astype(jnp.bfloat16)
    loads[0].wait()
    queries = jnp.dot(normed_ref[...], w_query[...], preferred_element_type=f32)
    queries = queries.astype(jnp.bfloat16).astype(f32)
    for h in range(local_heads):
        query_ref[:, h, :] = queries[:, h * head_dim : (h + 1) * head_dim]
    pl.semaphore_wait(barrier, 2 * n - 1)

    def team_copy(source, gathered, sems, origin, other):
        return remote(
            source,
            gathered.at[origin],
            sems.at[0, other],
            sems.at[1, origin],
            team * group_size + other,
            core,
        )

    def send_weights(k, carry):
        other = lax.rem(place + k, group_size)
        team_copy(dense_gate_ref, dense_gate_all, dense_gate_sems, place, other).start()
        team_copy(dense_up_ref, dense_up_all, dense_up_sems, place, other).start()
        team_copy(down_ref, down_all, down_sems, place, other).start()
        return carry

    lax.fori_loop(1, group_size, send_weights, 0)
    dense_gate_all[place] = dense_gate_ref[...]
    dense_up_all[place] = dense_up_ref[...]
    down_all[place] = down_ref[...]

    block_len = min(256, cache_len)
    after_mask = (
        lax.broadcasted_iota(jnp.int32, (block_len, block_len), 0)
        > lax.broadcasted_iota(jnp.int32, (block_len, block_len), 1)
    ).astype(jnp.bfloat16)
    position = lax.broadcasted_iota(jnp.int32, (span * local_heads, block_len), 1)

    head_row = lax.broadcasted_iota(jnp.int32, (local_heads, local_heads), 0)
    head_col = lax.broadcasted_iota(jnp.int32, (local_heads, local_heads), 1)
    bias = jnp.sum(jnp.where(head_row == head_col, bias_ref[...], 0.0), axis=1, keepdims=True)
    lines = span * local_heads
    line_seq = lax.broadcasted_iota(jnp.int32, (lines, rows), 0) // local_heads
    seq_lane = lax.broadcasted_iota(jnp.int32, (lines, rows), 1)
    lengths_row = lengths_ref[...].astype(f32)

    def attend(c, carry):
        keys_load(c).wait()
        for i in range(span):
            s = c * span + i
            score_ref[s] = (
                jnp.dot(query_ref[s].astype(jnp.bfloat16), keys[s], preferred_element_type=f32)
                * head_dim ** (-0.5)
                + bias
            )
        limits = jnp.sum(
            jnp.where(seq_lane == line_seq + c * span, lengths_row, 0.0), axis=1, keepdims=True
        ).astype(jnp.int32)
        later = jnp.zeros((lines, 1), f32)
        for first_pos in range(cache_len - block_len, -1, -block_len):
            columns = slice(first_pos, first_pos + block_len)
            scores = score_ref[pl.ds(c * span, span), :, columns].reshape(lines, block_len)
            visible = position + first_pos < limits
            keep = -(jnp.maximum(scores, 0.0) + jnp.log1p(jnp.exp(-jnp.abs(scores))))
            log_take = scores + keep
            keep = jnp.where(visible, keep, 0.0)
            top = keep.astype(jnp.bfloat16)
            rest = keep - top.astype(f32)
            middle = rest.astype(jnp.bfloat16)
            low = (rest - middle.astype(f32)).astype(jnp.bfloat16)
            sums = jnp.dot(
                jnp.concatenate([top, middle, low], axis=0),
                after_mask,
                preferred_element_type=f32,
            )
            after = sums[:lines] + sums[lines : 2 * lines] + sums[2 * lines :] + later
            later = later + jnp.sum(keep, axis=-1, keepdims=True)
            stick = jnp.where(visible, jnp.exp(log_take + after), 0.0)
            score_ref[pl.ds(c * span, span), :, columns] = stick.reshape(
                span, local_heads, block_len
            )
        values_load(c).wait()
        for i in range(span):
            s = c * span + i
            read_ref[s] = lax.dot_general(
                score_ref[s].astype(jnp.bfloat16),
                values[s],
                (((1,), (1,)), ((), ())),
                preferred_element_type=f32,
            )
        return carry

    lax.fori_loop(0, rows // span, attend, 0)
    heads_out = jnp.concatenate(
        [read_ref[:, h, :] for h in range(local_heads)], axis=1
    ).astype(jnp.bfloat16)
    loads[4].wait()
    attn_mine[...] = jnp.dot(heads_out, w_out[...], preferred_element_type=f32).astype(
        jnp.bfloat16
    )

    swap = remote(attn_mine, attn_peer, pair_sems.at[0], pair_sems.at[1], me, peer)
    swap.start()
    swap.wait()
    attn = attn_mine[...].astype(f32) + attn_peer[...].astype(f32)
    residual = (tokens_ref[...].astype(f32) + attn).astype(jnp.bfloat16)
    res_ref[...] = residual
    wide = residual.astype(f32)
    normed = (
        wide * lax.rsqrt(jnp.mean(wide * wide, axis=-1, keepdims=True) + 1e-06) * gain_ref[...]
    ).astype(jnp.bfloat16)
    norm_all[0, me] = normed[:, :half]
    norm_all[1, me] = normed[:, half:]

    def norm_copy(j, other):
        return remote(
            norm_all.at[core, j],
            norm_all.at[core, j],
            norm_sems.at[0, other],
            norm_sems.at[1, j],
            other,
            core,
        )

    def pass_copy(j, which):
        return remote(
            norm_all.at[which, j],
            norm_all.at[which, j],
            pass_sems.at[0, j],
            pass_sems.at[1, j],
            me,
            peer,
        )

    def send_norm(k, carry):
        norm_copy(me, lax.rem(me + k, n)).start()
        return carry

    lax.fori_loop(1, n, send_norm, 0)

    across = (((1,), (1,)), ((), ()))
    probs = jax.nn.sigmoid(
        lax.dot_general(router_ref[...], normed, across, preferred_element_type=f32)
    )
    expert_total = probs.shape[0]
    expert_row = lax.broadcasted_iota(jnp.int32, (expert_total, rows), 0)
    hits = jnp.zeros((expert_total, rows), f32)
    for k in range(routes_ref.shape[0]):
        hits = jnp.where(routes_ref[k : k + 1, :] == expert_row, 1.0, hits)
    picked = jnp.where(hits > 0.0, probs, 0.0)
    gates = (picked / jnp.sum(picked, axis=0, keepdims=True) * 2.5).T
    expert_index = lax.broadcasted_iota(jnp.int32, (rows, expert_total), 1)
    mix_gate = jax.nn.sigmoid(
        jnp.sum(normed.astype(f32) * mix_ref[...], axis=-1, keepdims=True)
    )

    for weight, target in ((w_key_ref, new_keys_ref), (w_value_ref, new_values_ref)):
        target[...] = lax.dot_general(
            normed_ref[...], weight[...], across, preferred_element_type=f32
        ).astype(jnp.bfloat16)

    def take_norm(k, carry):
        j = lax.rem(me + n - k, n)
        norm_copy(j, me).wait_recv()
        pass_copy(j, core).start()
        return carry

    lax.fori_loop(1, n, take_norm, 0)

    def take_pass(k, carry):
        pass_copy(lax.rem(me + n - k, n), peer).wait_recv()
        return carry

    lax.fori_loop(1, n, take_pass, 0)

    def part_copy(m, other):
        return remote(
            part_send.at[other],
            part_recv.at[m],
            part_sems.at[0, other],
            part_sems.at[1, m],
            other * group_size + place,
            core,
        )

    def back_copy(j, other):
        return remote(
            back_send.at[other],
            back_recv.at[j],
            back_sems.at[0, other],
            back_sems.at[1, j],
            other,
            core,
        )

    def dense_copy(m, other):
        return remote(
            dense_all.at[m],
            dense_all.at[m],
            dense_sems.at[0, other],
            dense_sems.at[1, m],
            other * group_size + place,
            core,
        )

    group = min(n, 16)
    groups = n // group
    block = group * rows

    def take_weights(k, carry):
        other = lax.rem(place + k, group_size)
        team_copy(dense_gate_ref, dense_gate_all, dense_gate_sems, other, place).wait_recv()
        team_copy(dense_up_ref, dense_up_all, dense_up_sems, other, place).wait_recv()
        team_copy(down_ref, down_all, down_sems, other, place).wait_recv()
        return carry

    lax.fori_loop(1, group_size, take_weights, 0)
    features = jnp.concatenate(
        [norm_all[owner, m * group_size + place, :, pl.ds(lane, window)] for m in range(teams)],
        axis=0,
    )
    hidden_cols = dense_gate_ref.shape[1]
    for gathered, columns in (
        (dense_gate_all, slice(0, hidden_cols)),
        (dense_up_all, slice(hidden_cols, 2 * hidden_cols)),
    ):
        value = jnp.dot(
            features, gathered[...].reshape(window, hidden_cols), preferred_element_type=f32
        )
        part_send[:, :, columns] = value.astype(jnp.bfloat16).reshape(teams, rows, hidden_cols)

    def send_part(k, carry):
        part_copy(team, lax.rem(team + k, teams)).start()
        return carry

    lax.fori_loop(1, teams, send_part, 0)

    loads[1].wait()
    loads[2].wait()

    def expert_first(c, carry):
        base = c * group
        low = norm_all[0, pl.ds(base, group)].reshape(block, half)
        high = norm_all[1, pl.ds(base, group)].reshape(block, half)
        gate_rows = jnp.dot(low, w_gate[:half], preferred_element_type=f32) + jnp.dot(
            high, w_gate[half:], preferred_element_type=f32
        )
        up_rows = jnp.dot(low, w_up[:half], preferred_element_type=f32) + jnp.dot(
            high, w_up[half:], preferred_element_type=f32
        )
        hidden_ref[pl.ds(c, 1)] = (jax.nn.silu(gate_rows) * up_rows).astype(jnp.bfloat16)[None]
        return carry

    lax.fori_loop(0, groups, expert_first, 0)

    def take_part(k, total):
        m = lax.rem(team + teams - k, teams)
        part_copy(m, team).wait_recv()
        return total + part_recv[m].astype(f32)

    paired = lax.fori_loop(1, teams, take_part, part_send[team].astype(f32))
    dense_all[team] = (jax.nn.silu(paired[:, :hidden_cols]) * paired[:, hidden_cols:]).astype(
        jnp.bfloat16
    )

    def send_dense(k, carry):
        dense_copy(team, lax.rem(team + k, teams)).start()
        return carry

    lax.fori_loop(1, teams, send_dense, 0)

    loads[3].wait()
    far = pl.ds(pl.multiple_of(peer * half, half), half)
    near = pl.ds(pl.multiple_of(core * half, half), half)

    def expert_far(c, carry):
        value = jnp.dot(hidden_ref[c], w_down[:, far], preferred_element_type=f32)
        other_ref[pl.ds(c * group, group)] = value.astype(jnp.bfloat16).reshape(group, rows, half)
        return carry

    lax.fori_loop(0, groups, expert_far, 0)
    trade = remote(other_ref, peer_ref, pair_sems.at[2], pair_sems.at[3], me, peer)
    trade.start()

    def expert_near(c, carry):
        value = jnp.dot(hidden_ref[c], w_down[:, near], preferred_element_type=f32)
        mine_ref[pl.ds(c * group, group)] = value.astype(jnp.bfloat16).reshape(group, rows, half)
        return carry

    lax.fori_loop(0, groups, expert_near, 0)
    trade.wait()

    def send_back(k, carry):
        other = lax.rem(me + k, n)
        total = mine_ref[other].astype(f32) + peer_ref[other].astype(f32)
        back_send[other] = total.astype(jnp.bfloat16)

        @pl.when(k > 0)
        def _():
            back_copy(me, other).start()

        return carry

    lax.fori_loop(0, n, send_back, 0)

    def take_dense(k, carry):
        dense_copy(lax.rem(team + teams - k, teams), team).wait_recv()
        return carry

    lax.fori_loop(1, teams, take_dense, 0)
    dense_rows = dense_all[...].reshape(teams * rows, hidden_cols)
    columns = [
        jnp.dot(dense_rows, down_all[q], preferred_element_type=f32) for q in range(group_size)
    ]
    cols_send[...] = (
        jnp.concatenate(columns, axis=1).astype(jnp.bfloat16).reshape(cols_send.shape)
    )

    def cols_copy(from_core, m, other, target):
        return remote(
            cols_send.at[other],
            cols_recv.at[from_core, m],
            cols_send_sem.at[other],
            cols_recv_sem.at[from_core, m],
            other * group_size + place,
            target,
        )

    def send_cols(k, carry):
        cols_copy(core, team, lax.rem(team + k, teams), owner).start()
        return carry

    lax.fori_loop(1, teams, send_cols, 0)

    @pl.when(owner == core)
    def _():
        cols_recv[core, team] = cols_send[team]

    @pl.when(owner != core)
    def _():
        cols_copy(core, team, team, peer).start()

    side = teams // 2

    def take_cols(k, carry):
        m = core * side + k

        @pl.when(m != team)
        def _():
            cols_copy(core, m, team, core).wait_recv()

        cols_copy(peer, m, team, core).wait_recv()
        return carry

    lax.fori_loop(0, side, take_cols, 0)
    dense = jnp.concatenate(
        [
            cols_recv[0, core * side + q].astype(f32) + cols_recv[1, core * side + q].astype(f32)
            for q in range(side)
        ],
        axis=1,
    )
    total = res_ref[:, near].astype(f32) + mix_gate * dense

    def take_back(k, total):
        j = lax.rem(me + n - k, n)

        @pl.when(k > 0)
        def _():
            back_copy(j, me).wait_recv()

        @pl.when(k == 0)
        def _():
            back_recv[me] = back_send[me]

        gate = jnp.sum(jnp.where(expert_index == j, gates, 0.0), axis=-1, keepdims=True)
        return total + gate * back_recv[j].astype(f32)

    out_ref[...] = lax.fori_loop(0, n, take_back, total).astype(jnp.bfloat16)

    def drain(k, carry):
        other = lax.rem(me + k, n)
        norm_copy(me, other).wait_send()
        pass_copy(other, core).wait_send()
        back_copy(me, other).wait_send()
        return carry

    lax.fori_loop(1, n, drain, 0)

    def drain_team(k, carry):
        other = lax.rem(place + k, group_size)
        team_copy(dense_gate_ref, dense_gate_all, dense_gate_sems, place, other).wait_send()
        team_copy(dense_up_ref, dense_up_all, dense_up_sems, place, other).wait_send()
        team_copy(down_ref, down_all, down_sems, place, other).wait_send()
        return carry

    lax.fori_loop(1, group_size, drain_team, 0)

    def drain_dense(k, carry):
        other = lax.rem(team + k, teams)
        part_copy(team, other).wait_send()
        dense_copy(team, other).wait_send()
        cols_copy(core, team, other, owner).wait_send()
        return carry

    lax.fori_loop(1, teams, drain_dense, 0)

    @pl.when(owner != core)
    def _():
        cols_copy(core, team, team, peer).wait_send()


def flip(place, k):
    result, bit = place, 1
    while bit <= k:
        if k & bit:
            result = result + bit * (1 - 2 * ((place // bit) % 2))
        bit *= 2
    return result


def routed_layer(
    n,
    inner,
    tokens_hbm,
    attn_gain_hbm,
    lengths_hbm,
    bias_hbm,
    w_key_hbm,
    w_value_hbm,
    gain_hbm,
    router_hbm,
    routes_hbm,
    mix_hbm,
    dense_gate_hbm,
    dense_up_hbm,
    down_hbm,
    w_query_hbm,
    w_out_hbm,
    w_gate_hbm,
    w_up_hbm,
    w_down_hbm,
    keys_hbm,
    values_hbm,
    out_ref,
    new_keys_ref,
    new_values_ref,
    tokens_ref,
    attn_gain_ref,
    lengths_ref,
    bias_ref,
    w_key_ref,
    w_value_ref,
    gain_ref,
    router_ref,
    routes_ref,
    mix_ref,
    dense_gate_ref,
    dense_up_ref,
    down_ref,
    w_query,
    w_out,
    w_gate,
    w_up,
    w_down,
    keys,
    values,
    query_ref,
    score_ref,
    read_ref,
    normed_ref,
    small_send,
    small,
    hits_all,
    attn_mine,
    attn_peer,
    res_ref,
    norm_all,
    first_send,
    first_recv,
    plane_send,
    plane_recv,
    line_send,
    line_recv,
    load_sem,
    keys_sem,
    values_sem,
    pair_sems,
    swap_sems,
    small_send_sem,
    small_recv_sem,
    down_send_sem,
    down_recv_sem,
    hits_sems,
    line_sems,
    spread_sems,
    first_sems,
    plane_sems,
    back_sems,
):
    me = lax.axis_index("ep")
    core = lax.axis_index("tp")
    peer = 1 - core
    f32, bf16 = jnp.float32, jnp.bfloat16
    rows, model = tokens_ref.shape
    half = model // 2
    width, hidden_cols = dense_gate_ref.shape
    units = hidden_cols // n
    outer = n // inner
    z, p = me // inner, me % inner
    side = n // 2
    owner, slot = me // side, me % side
    local_heads = bias_ref.shape[1]
    head_dim, cache_len = keys_hbm.shape[1:]
    hidden = w_gate_hbm.shape[1]
    expert_total = router_ref.shape[0]
    lanes = small.shape[0]
    router_at = 4 * units
    mix_at = router_at + expert_total
    span = 4
    lines = span * local_heads

    def remote(source, target, send_sem, recv_sem, ep, tp):
        return pltpu.make_async_remote_copy(
            src_ref=source,
            dst_ref=target,
            send_sem=send_sem,
            recv_sem=recv_sem,
            device_id=(ep, tp),
            device_id_type=MESH,
        )

    near = pl.ds(pl.multiple_of(core * half, half), half)
    far = pl.ds(pl.multiple_of(peer * half, half), half)
    mine = pl.ds(pl.multiple_of(core * hidden, hidden), hidden)
    pairs = (
        (tokens_hbm, tokens_ref),
        (attn_gain_hbm, attn_gain_ref),
        (dense_gate_hbm, dense_gate_ref),
        (dense_up_hbm, dense_up_ref),
        (routes_hbm, routes_ref),
        (w_query_hbm, w_query),
        (bias_hbm, bias_ref),
        (lengths_hbm, lengths_ref),
        (router_hbm, router_ref),
        (mix_hbm, mix_ref),
        (down_hbm, down_ref),
        (gain_hbm, gain_ref),
        (w_out_hbm, w_out),
        (w_key_hbm, w_key_ref),
        (w_value_hbm, w_value_ref),
        (w_gate_hbm.at[near, :], w_gate.at[:, mine]),
        (w_up_hbm.at[near, :], w_up.at[:, mine]),
        (w_down_hbm.at[:, near], w_down.at[mine, :]),
    )
    loads = [
        pltpu.make_async_copy(source, target, load_sem.at[i])
        for i, (source, target) in enumerate(pairs)
    ]
    load_of = {id(target): load for (_, target), load in zip(pairs, loads)}

    def arrived(*targets):
        for target in targets:
            load_of[id(target)].wait()

    def keys_load(c):
        block = pl.ds(c * span, span)
        return pltpu.make_async_copy(keys_hbm.at[block], keys.at[block], keys_sem.at[c])

    def values_load(c):
        block = pl.ds(c * span, span)
        return pltpu.make_async_copy(values_hbm.at[block], values.at[block], values_sem.at[c])

    for load in loads[:8]:
        load.start()
    for c in range(rows // span):
        keys_load(c).start()
        values_load(c).start()
    for load in loads[8:]:
        load.start()

    barrier = pltpu.get_barrier_semaphore()

    def greet(k, carry):
        other = lax.rem(me + k, n)
        pl.semaphore_signal(barrier, inc=1, device_id=(other, core), device_id_type=MESH)
        pl.semaphore_signal(barrier, inc=1, device_id=(other, peer), device_id_type=MESH)
        return carry

    lax.fori_loop(1, n, greet, 0)
    pl.semaphore_signal(barrier, inc=1, device_id=(me, peer), device_id_type=MESH)

    arrived(tokens_ref, attn_gain_ref)
    start = tokens_ref[...].astype(f32)
    normed_ref[...] = (
        start
        * lax.rsqrt(jnp.mean(start * start, axis=-1, keepdims=True) + 1e-06)
        * attn_gain_ref[...]
    ).astype(bf16)
    arrived(dense_gate_ref, dense_up_ref, routes_ref)
    small_send[:, :units, :] = dense_gate_ref[...].T.reshape(n, units, width)
    small_send[:, units:, :] = dense_up_ref[...].T.reshape(n, units, width)
    lane_row = lax.broadcasted_iota(jnp.int32, (lanes, rows), 0)
    hits = jnp.zeros((lanes, rows), f32)
    for k in range(routes_ref.shape[0]):
        hits = jnp.where(routes_ref[k : k + 1, :] + router_at == lane_row, 1.0, hits)
    hits_all[me] = hits.T.astype(bf16)

    arrived(w_query)
    queries = jnp.dot(normed_ref[...], w_query[...], preferred_element_type=f32)
    queries = queries.astype(bf16).astype(f32)
    for h in range(local_heads):
        query_ref[:, h, :] = queries[:, h * head_dim : (h + 1) * head_dim]

    block_len = min(256, cache_len)
    after_mask = (
        lax.broadcasted_iota(jnp.int32, (block_len, block_len), 0)
        > lax.broadcasted_iota(jnp.int32, (block_len, block_len), 1)
    ).astype(bf16)
    position = lax.broadcasted_iota(jnp.int32, (lines, block_len), 1)
    arrived(bias_ref, lengths_ref)
    head_row = lax.broadcasted_iota(jnp.int32, (local_heads, local_heads), 0)
    head_col = lax.broadcasted_iota(jnp.int32, (local_heads, local_heads), 1)
    bias = jnp.sum(jnp.where(head_row == head_col, bias_ref[...], 0.0), axis=1, keepdims=True)
    line_seq = lax.broadcasted_iota(jnp.int32, (lines, rows), 0) // local_heads
    seq_lane = lax.broadcasted_iota(jnp.int32, (lines, rows), 1)
    lengths_row = lengths_ref[...].astype(f32)

    def attend(c, carry):
        keys_load(c).wait()
        for i in range(span):
            s = c * span + i
            score_ref[s] = (
                jnp.dot(query_ref[s].astype(bf16), keys[s], preferred_element_type=f32)
                * head_dim ** (-0.5)
                + bias
            )
        limits = jnp.sum(
            jnp.where(seq_lane == line_seq + c * span, lengths_row, 0.0), axis=1, keepdims=True
        ).astype(jnp.int32)
        later = jnp.zeros((lines, 1), f32)
        for first_pos in range(cache_len - block_len, -1, -block_len):
            columns = slice(first_pos, first_pos + block_len)
            scores = score_ref[pl.ds(c * span, span), :, columns].reshape(lines, block_len)
            visible = position + first_pos < limits
            keep = -(jnp.maximum(scores, 0.0) + jnp.log1p(jnp.exp(-jnp.abs(scores))))
            log_take = scores + keep
            keep = jnp.where(visible, keep, 0.0)
            top = keep.astype(bf16)
            rest = keep - top.astype(f32)
            middle = rest.astype(bf16)
            low = (rest - middle.astype(f32)).astype(bf16)
            sums = jnp.dot(
                jnp.concatenate([top, middle, low], axis=0),
                after_mask,
                preferred_element_type=f32,
            )
            after = sums[:lines] + sums[lines : 2 * lines] + sums[2 * lines :] + later
            later = later + jnp.sum(keep, axis=-1, keepdims=True)
            stick = jnp.where(visible, jnp.exp(log_take + after), 0.0)
            score_ref[pl.ds(c * span, span), :, columns] = stick.reshape(
                span, local_heads, block_len
            )
        values_load(c).wait()
        for i in range(span):
            s = c * span + i
            read_ref[s] = lax.dot_general(
                score_ref[s].astype(bf16),
                values[s],
                (((1,), (1,)), ((), ())),
                preferred_element_type=f32,
            )
        return carry

    steps = rows // span
    lax.fori_loop(0, steps // 2, attend, 0)

    pl.semaphore_wait(barrier, 2 * n - 1)
    trades = [
        remote(
            w_gate_hbm.at[far, :], w_gate.at[:, mine], pair_sems.at[0, 0], pair_sems.at[1, 0], me, peer
        ),
        remote(
            w_up_hbm.at[far, :], w_up.at[:, mine], pair_sems.at[0, 1], pair_sems.at[1, 1], me, peer
        ),
        remote(
            w_down_hbm.at[:, far], w_down.at[mine, :], pair_sems.at[0, 2], pair_sems.at[1, 2], me, peer
        ),
    ]
    for trade in trades:
        trade.start()

    def small_copy(other, tp):
        return remote(
            small_send.at[other],
            small.at[pl.ds(core * 2 * units, 2 * units), pl.ds(pl.multiple_of(slot * width, width), width)],
            small_send_sem.at[other],
            small_recv_sem.at[core, slot],
            other,
            tp,
        )

    def down_copy(other, tp):
        return remote(
            down_ref.at[pl.ds(pl.multiple_of(other * units, units), units), :],
            w_down.at[
                pl.ds(2 * hidden + core * 2 * units, units),
                pl.ds(pl.multiple_of(slot * width, width), width),
            ],
            down_send_sem.at[other],
            down_recv_sem.at[core, slot],
            other,
            tp,
        )

    def hits_copy(origin, other):
        return remote(
            hits_all.at[origin],
            hits_all.at[origin],
            hits_sems.at[0, other],
            hits_sems.at[1, origin],
            other,
            core,
        )

    arrived(router_ref, mix_ref, down_ref)
    spread_rows = lanes - mix_at
    mix_row = mix_ref[...]
    mix_top = mix_row.astype(bf16)
    mix_rest = mix_row - mix_top.astype(f32)
    mix_mid = mix_rest.astype(bf16)
    mix_low = (mix_rest - mix_mid.astype(f32)).astype(bf16)
    mix_index = lax.broadcasted_iota(jnp.int32, (spread_rows, model), 0)
    mix_rows = jnp.where(
        mix_index == 0,
        mix_top.astype(f32),
        jnp.where(
            mix_index == 1,
            mix_mid.astype(f32),
            jnp.where(mix_index == 2, mix_low.astype(f32), 0.0),
        ),
    ).astype(bf16)
    small[pl.ds(router_at, expert_total), :] = jnp.where(
        core == 0, router_ref[:, :half], router_ref[:, half:]
    )
    small[pl.ds(mix_at, spread_rows), :] = jnp.where(
        core == 0, mix_rows[:, :half], mix_rows[:, half:]
    )
    for base in (units, 3 * units):
        w_down[pl.ds(2 * hidden + base, units), :] = jnp.zeros((units, half), bf16)
    tail = lanes - 4 * units
    w_down[pl.ds(2 * hidden + 4 * units, tail), :] = jnp.zeros((tail, half), bf16)

    def send_small(k, carry):
        other = lax.rem(me + k, n)
        small_copy(other, owner).start()
        down_copy(other, owner).start()
        hits_copy(me, other).start()
        return carry

    lax.fori_loop(1, n, send_small, 0)

    @pl.when(owner == core)
    def _():
        here = pl.ds(pl.multiple_of(slot * width, width), width)
        small[pl.ds(pl.multiple_of(core * 2 * units, 2 * units), 2 * units), here] = small_send[me]
        w_down[
            pl.ds(pl.multiple_of(2 * hidden + core * 2 * units, units), units), here
        ] = down_ref[pl.ds(pl.multiple_of(me * units, units), units), :]

    @pl.when(owner != core)
    def _():
        small_copy(me, peer).start()
        down_copy(me, peer).start()

    lax.fori_loop(steps // 2, steps, attend, 0)
    heads_out = jnp.concatenate([read_ref[:, h, :] for h in range(local_heads)], axis=1).astype(
        bf16
    )
    arrived(w_out)
    swaps = []
    for i in range(2):
        attn_mine[i] = jnp.dot(
            heads_out, w_out[:, i * half : (i + 1) * half], preferred_element_type=f32
        ).astype(bf16)
        swaps.append(
            remote(
                attn_mine.at[i], attn_peer.at[i], swap_sems.at[0, i], swap_sems.at[1, i], me, peer
            )
        )
        swaps[i].start()
    arrived(gain_ref)
    wide = []
    for i in range(2):
        swaps[i].wait_recv()
        columns = slice(i * half, (i + 1) * half)
        res_ref[i] = (
            tokens_ref[:, columns].astype(f32)
            + (attn_mine[i].astype(f32) + attn_peer[i].astype(f32))
        ).astype(bf16)
        wide.append(res_ref[i].astype(f32))
    squares = sum(jnp.sum(part * part, axis=-1, keepdims=True) for part in wide)
    scale = lax.rsqrt(squares / model + 1e-06)
    norm_all[me] = (
        jnp.where(core == 0, wide[0], wide[1])
        * scale
        * jnp.where(core == 0, gain_ref[:, :half], gain_ref[:, half:])
    ).astype(bf16)

    def line_copy(k):
        return remote(
            norm_all.at[me],
            norm_all.at[me],
            line_sems.at[0, k],
            line_sems.at[1, k],
            flip(z, k) * inner + p,
            core,
        )

    def spread_copy(k, j):
        origin = flip(z, k) * inner + p
        return remote(
            norm_all.at[origin],
            norm_all.at[origin],
            spread_sems.at[0, k, j],
            spread_sems.at[1, k, j],
            z * inner + flip(p, j),
            core,
        )

    for k in range(1, outer):
        line_copy(k).start()
    for j in range(1, inner):
        spread_copy(0, j).start()

    across = (((1,), (1,)), ((), ()))
    arrived(w_key_ref, w_value_ref)
    for weight, target in ((w_key_ref, new_keys_ref), (w_value_ref, new_values_ref)):
        target[...] = lax.dot_general(
            normed_ref[...], weight[...], across, preferred_element_type=f32
        ).astype(bf16)

    def take_small(k, carry):
        source = core * side + k

        @pl.when(source != me)
        def _():
            remote(
                small_send.at[0],
                small.at[
                    pl.ds(core * 2 * units, 2 * units), pl.ds(pl.multiple_of(k * width, width), width)
                ],
                small_send_sem.at[0],
                small_recv_sem.at[core, k],
                me,
                peer,
            ).wait_recv()
            remote(
                down_ref.at[pl.ds(0, units), :],
                w_down.at[
                    pl.ds(2 * hidden + core * 2 * units, units),
                    pl.ds(pl.multiple_of(k * width, width), width),
                ],
                down_send_sem.at[0],
                down_recv_sem.at[core, k],
                me,
                peer,
            ).wait_recv()

        remote(
            small_send.at[0],
            small.at[
                pl.ds(peer * 2 * units, 2 * units), pl.ds(pl.multiple_of(k * width, width), width)
            ],
            small_send_sem.at[0],
            small_recv_sem.at[peer, k],
            me,
            peer,
        ).wait_recv()
        remote(
            down_ref.at[pl.ds(0, units), :],
            w_down.at[
                pl.ds(2 * hidden + peer * 2 * units, units),
                pl.ds(pl.multiple_of(k * width, width), width),
            ],
            down_send_sem.at[0],
            down_recv_sem.at[peer, k],
            me,
            peer,
        ).wait_recv()
        return carry

    lax.fori_loop(0, side, take_small, 0)

    def take_hits(k, carry):
        hits_copy(lax.rem(me + n - k, n), me).wait_recv()
        return carry

    lax.fori_loop(1, n, take_hits, 0)
    arrived(*[target for _, target in pairs[15:]])
    for trade in trades:
        trade.wait_recv()

    for k in range(1, outer):
        line_copy(k).wait_recv()
        for j in range(1, inner):
            spread_copy(k, j).start()

    chunk = inner * rows
    lane = lax.broadcasted_iota(jnp.int32, (chunk, lanes), 1)
    routed = (lane >= router_at) & (lane < mix_at)
    dense_lane = (lane < units) | ((lane >= 2 * units) & (lane < 3 * units))

    def first_copy(k):
        return remote(
            first_send.at[k], first_recv.at[k], first_sems.at[0, k], first_sems.at[1, k], me, peer
        )

    def group(k):
        return pl.ds(pl.multiple_of(flip(z, k) * inner, inner), inner)

    def first(k):
        for j in range(1, inner):
            spread_copy(k, j).wait_recv()
        x = norm_all[group(k)].reshape(chunk, half)
        first_send[k, :, : 2 * hidden] = jnp.dot(x, w_gate[...], preferred_element_type=f32)
        first_send[k, :, 2 * hidden : 4 * hidden] = jnp.dot(
            x, w_up[...], preferred_element_type=f32
        )
        first_send[k, :, 4 * hidden :] = lax.dot_general(
            x, small[...], across, preferred_element_type=f32
        )
        first_copy(k).start()

    def plane_copy(k, j):
        other = flip(p, j)
        return remote(
            plane_send.at[k, other],
            plane_recv.at[k, j],
            plane_sems.at[0, k, j],
            plane_sems.at[1, k, j],
            z * inner + other,
            core,
        )

    def second(k):
        first_copy(k).wait_recv()
        gate_rows = first_send[k, :, : 2 * hidden] + first_recv[k, :, : 2 * hidden]
        up_rows = (
            first_send[k, :, 2 * hidden : 4 * hidden] + first_recv[k, :, 2 * hidden : 4 * hidden]
        )
        rest = first_send[k, :, 4 * hidden :] + first_recv[k, :, 4 * hidden :]
        chosen = hits_all[group(k)].reshape(chunk, lanes).astype(f32)
        picked = jnp.where(routed & (chosen > 0.0), jax.nn.sigmoid(rest), 0.0)
        total = jnp.sum(picked, axis=-1, keepdims=True)
        own = jnp.sum(jnp.where(lane == router_at + me, picked, 0.0), axis=-1, keepdims=True)
        gate = own / total * 2.5
        mix_sum = jnp.sum(jnp.where(lane >= mix_at, rest, 0.0), axis=-1, keepdims=True)
        mix_gate = jax.nn.sigmoid(mix_sum)
        dense = jax.nn.silu(rest) * pltpu.roll(rest, lanes - units, 1) * mix_gate
        dense = jnp.where(dense_lane, dense, 0.0).astype(bf16)
        act = (jax.nn.silu(gate_rows) * up_rows * gate).astype(bf16)
        value = jnp.dot(act, w_down[: 2 * hidden], preferred_element_type=f32) + jnp.dot(
            dense, w_down[2 * hidden :], preferred_element_type=f32
        )
        plane_send[k] = value.astype(bf16).reshape(inner, rows, half)
        for j in range(inner - 1, 0, -1):
            plane_copy(k, j).start()

    def back_copy(k):
        return remote(
            line_send.at[k],
            line_recv.at[k],
            back_sems.at[0, k],
            back_sems.at[1, k],
            flip(z, k) * inner + p,
            core,
        )

    def collect(k):
        total = plane_send[k, p].astype(f32)
        for j in range(1, inner):
            plane_copy(k, j).wait_recv()
            total = total + plane_recv[k, j].astype(f32)
        return total

    def third(k):
        line_send[k] = collect(k).astype(bf16)
        back_copy(k).start()

    first(0)
    for k in range(1, outer):
        first(k)
        second(k - 1)
    second(outer - 1)
    for k in range(1, outer):
        third(k)
    total = res_ref[core].astype(f32) + collect(0)
    for k in range(1, outer):
        back_copy(k).wait_recv()
        total = total + line_recv[k].astype(f32)
    out_ref[...] = total.astype(bf16)

    def drain(k, carry):
        other = lax.rem(me + k, n)
        small_copy(other, owner).wait_send()
        down_copy(other, owner).wait_send()
        hits_copy(me, other).wait_send()
        return carry

    lax.fori_loop(1, n, drain, 0)

    @pl.when(owner != core)
    def _():
        small_copy(me, peer).wait_send()
        down_copy(me, peer).wait_send()

    for copy in trades + swaps:
        copy.wait_send()
    for k in range(outer):
        if k:
            line_copy(k).wait_send()
            back_copy(k).wait_send()
        first_copy(k).wait_send()
        for j in range(1, inner):
            spread_copy(k, j).wait_send()
            plane_copy(k, j).wait_send()


def routed_shards(n, inner, arrays):
    tokens = arrays[0]
    w_key, head_bias = arrays[4], arrays[3]
    keys, w_gate, w_down = arrays[18], arrays[15], arrays[17]
    rows, model = tokens.shape
    half = model // 2
    width, hidden_cols = arrays[10].shape
    units = hidden_cols // n
    outer = n // inner
    seq_count, head_dim, cache_len = keys.shape
    local_heads = head_bias.shape[1]
    hidden = w_gate.shape[1]
    lanes = 128
    chunk = inner * rows
    bf16, f32 = jnp.bfloat16, jnp.float32
    vmem = pl.BlockSpec(memory_space=pltpu.VMEM)
    anywhere = pl.BlockSpec(memory_space=pltpu.HBM)
    dma = pltpu.SemaphoreType.DMA
    small_inputs = [pltpu.VMEM(a.shape, a.dtype) for a in arrays[:15]]
    return pl.pallas_call(
        functools.partial(routed_layer, n, inner),
        out_shape=(
            jax.ShapeDtypeStruct((rows, half), bf16),
            jax.ShapeDtypeStruct((rows, w_key.shape[0]), bf16),
            jax.ShapeDtypeStruct((rows, w_key.shape[0]), bf16),
        ),
        in_specs=[anywhere] * 20,
        out_specs=(vmem, vmem, vmem),
        scratch_shapes=small_inputs
        + [
            pltpu.VMEM((half, 2 * hidden), bf16),
            pltpu.VMEM((half, 2 * hidden), bf16),
            pltpu.VMEM((2 * hidden + lanes, half), bf16),
            pltpu.VMEM(keys.shape, bf16),
            pltpu.VMEM(keys.shape, bf16),
            pltpu.VMEM((rows, local_heads, head_dim), f32),
            pltpu.VMEM((rows, local_heads, cache_len), f32),
            pltpu.VMEM((rows, local_heads, head_dim), f32),
            pltpu.VMEM((rows, model), bf16),
            pltpu.VMEM((n, 2 * units, width), bf16),
            pltpu.VMEM((lanes, half), bf16),
            pltpu.VMEM((n, rows, lanes), bf16),
            pltpu.VMEM((2, rows, half), bf16),
            pltpu.VMEM((2, rows, half), bf16),
            pltpu.VMEM((2, rows, half), bf16),
            pltpu.VMEM((n, rows, half), bf16),
            pltpu.VMEM((outer, chunk, 4 * hidden + lanes), f32),
            pltpu.VMEM((outer, chunk, 4 * hidden + lanes), f32),
            pltpu.VMEM((outer, inner, rows, half), bf16),
            pltpu.VMEM((outer, inner, rows, half), bf16),
            pltpu.VMEM((outer, rows, half), bf16),
            pltpu.VMEM((outer, rows, half), bf16),
            dma((18,)),
            dma((rows // 4,)),
            dma((rows // 4,)),
            dma((2, 3)),
            dma((2, 2)),
            dma((n,)),
            dma((2, n // 2)),
            dma((n,)),
            dma((2, n // 2)),
            dma((2, n)),
            dma((2, outer)),
            dma((2, outer, inner)),
            dma((2, outer)),
            dma((2, outer, inner)),
            dma((2, outer)),
        ],
        compiler_params=pltpu.CompilerParams(
            collective_id=0, has_side_effects=True, vmem_limit_bytes=48 * 1024 * 1024
        ),
        name="routed_layer",
    )(*[pltpu.with_memory_space_constraint(a, pltpu.HBM) for a in arrays])


def shards(
    n,
    tokens,
    lengths,
    attn_gain,
    w_query,
    w_key,
    w_value,
    head_bias,
    key_cache,
    value_cache,
    w_attn_out,
    ffn_gain,
    w_router,
    routes,
    w_dense_gate,
    w_dense_up,
    w_dense_down,
    dense_mix,
    w_expert_gate,
    w_expert_up,
    w_expert_down,
):
    rows, model = tokens.shape
    half = model // 2
    width, hidden_cols = w_dense_gate.shape
    group_size = min(n, max(4, 128 // width))
    teams = n // group_size
    window = width * group_size
    seq_count, local_kv, head_dim, cache_len = key_cache.shape
    local_heads = head_bias.shape[0]
    keys = key_cache.reshape(seq_count, head_dim, cache_len)
    values = value_cache.reshape(seq_count, head_dim, cache_len)
    w_gate, w_up, w_down = w_expert_gate[0], w_expert_up[0], w_expert_down[0]
    expert_hidden = w_gate.shape[1]
    arrays = (
        tokens,
        attn_gain.reshape(1, model),
        lengths.reshape(1, seq_count),
        head_bias.reshape(1, local_heads),
        w_key.T,
        w_value.T,
        ffn_gain.reshape(1, model),
        w_router.T,
        routes.T,
        dense_mix.reshape(1, model),
        w_dense_gate,
        w_dense_up,
        w_dense_down,
        w_query,
        w_attn_out,
        w_gate,
        w_up,
        w_down,
        keys,
        values,
    )
    inner = 1
    while (2 * inner) ** 2 <= n:
        inner *= 2
    small_rows = 4 * (hidden_cols // n) + w_router.shape[1]
    if hidden_cols % (16 * n) == 0 and width % 128 == 0 and small_rows <= 112:
        return routed_shards(n, inner, arrays)
    bf16, f32 = jnp.bfloat16, jnp.float32
    block = min(n, 16) * rows
    vmem = pl.BlockSpec(memory_space=pltpu.VMEM)
    anywhere = pl.BlockSpec(memory_space=pltpu.HBM)
    dma = pltpu.SemaphoreType.DMA
    return pl.pallas_call(
        functools.partial(whole_layer, n, group_size),
        out_shape=(
            jax.ShapeDtypeStruct((rows, half), bf16),
            jax.ShapeDtypeStruct((rows, w_key.shape[1]), bf16),
            jax.ShapeDtypeStruct((rows, w_value.shape[1]), bf16),
        ),
        in_specs=[vmem] * 13 + [anywhere] * 7,
        out_specs=(vmem, vmem, vmem),
        scratch_shapes=[
            pltpu.VMEM(w_query.shape, bf16),
            pltpu.VMEM(w_attn_out.shape, bf16),
            pltpu.VMEM(w_gate.shape, bf16),
            pltpu.VMEM(w_up.shape, bf16),
            pltpu.VMEM(w_down.shape, bf16),
            pltpu.VMEM(keys.shape, bf16),
            pltpu.VMEM(values.shape, bf16),
            dma((5,)),
            dma((rows // 4,)),
            dma((rows // 4,)),
            pltpu.VMEM((rows, local_heads, head_dim), f32),
            pltpu.VMEM((rows, local_heads, cache_len), f32),
            pltpu.VMEM((rows, local_heads, head_dim), f32),
            pltpu.VMEM((rows, model), bf16),
            pltpu.VMEM((group_size, width, hidden_cols), bf16),
            pltpu.VMEM((group_size, width, hidden_cols), bf16),
            pltpu.VMEM((group_size, hidden_cols, width), bf16),
            pltpu.VMEM((rows, model), bf16),
            pltpu.VMEM((rows, model), bf16),
            pltpu.VMEM((rows, model), bf16),
            pltpu.VMEM((2, n, rows, half), bf16),
            pltpu.VMEM((teams, rows, 2 * hidden_cols), bf16),
            pltpu.VMEM((teams, rows, 2 * hidden_cols), bf16),
            pltpu.VMEM((n * rows // block, block, expert_hidden), bf16),
            pltpu.VMEM((teams, rows, hidden_cols), bf16),
            pltpu.VMEM((teams, rows, window), bf16),
            pltpu.VMEM((2, teams, rows, window), bf16),
            pltpu.VMEM((n, rows, half), bf16),
            pltpu.VMEM((n, rows, half), bf16),
            pltpu.VMEM((n, rows, half), bf16),
            pltpu.VMEM((n, rows, half), bf16),
            pltpu.VMEM((n, rows, half), bf16),
            dma((4,)),
            dma((2, group_size)),
            dma((2, group_size)),
            dma((2, group_size)),
            dma((2, n)),
            dma((2, n)),
            dma((2, teams)),
            dma((2, teams)),
            dma((teams,)),
            dma((2, teams)),
            dma((2, n)),
        ],
        compiler_params=pltpu.CompilerParams(
            collective_id=0, has_side_effects=True, vmem_limit_bytes=63 * 1024 * 1024
        ),
        name="whole_layer",
    )(*arrays)


def solution(mesh):
    return jax.shard_map(
        functools.partial(shards, mesh.shape["ep"]),
        mesh=mesh,
        in_specs=(
            P("ep", None),
            P("ep"),
            P(),
            P(None, "tp"),
            P(None, "tp"),
            P(None, "tp"),
            P("tp"),
            P("ep", "tp", None, None),
            P("ep", "tp", None, None),
            P("tp", None),
            P(),
            P(),
            P("ep", None),
            P("ep", "tp"),
            P("ep", "tp"),
            P("tp", "ep"),
            P(),
            P("ep", None, "tp"),
            P("ep", None, "tp"),
            P("ep", "tp", None),
        ),
        out_specs=(P("ep", "tp"), P("ep", "tp"), P("ep", "tp")),
        check_vma=False,
    )
```

```python
import functools

import jax
import jax.numpy as jnp
from jax import lax
from jax.experimental import pallas as pl
from jax.experimental.pallas import tpu as pltpu
from jax.sharding import PartitionSpec as P

MESH = pl.DeviceIdType.MESH


def whole_layer(
    n,
    group_size,
    tokens_ref,
    attn_gain_ref,
    lengths_ref,
    bias_ref,
    w_key_ref,
    w_value_ref,
    gain_ref,
    router_ref,
    routes_ref,
    mix_ref,
    dense_gate_ref,
    dense_up_ref,
    down_ref,
    w_query_hbm,
    w_out_hbm,
    w_gate_hbm,
    w_up_hbm,
    w_down_hbm,
    keys_hbm,
    values_hbm,
    out_ref,
    new_keys_ref,
    new_values_ref,
    w_query,
    w_out,
    w_gate,
    w_up,
    w_down,
    keys,
    values,
    load_sem,
    keys_sem,
    values_sem,
    query_ref,
    score_ref,
    read_ref,
    normed_ref,
    dense_gate_all,
    dense_up_all,
    down_all,
    attn_mine,
    attn_peer,
    res_ref,
    norm_all,
    part_send,
    part_recv,
    hidden_ref,
    dense_all,
    cols_send,
    cols_recv,
    other_ref,
    mine_ref,
    peer_ref,
    back_send,
    back_recv,
    pair_sems,
    dense_gate_sems,
    dense_up_sems,
    down_sems,
    norm_sems,
    pass_sems,
    part_sems,
    dense_sems,
    cols_send_sem,
    cols_recv_sem,
    back_sems,
):
    me = lax.axis_index("ep")
    core = lax.axis_index("tp")
    peer = 1 - core
    rows, model = tokens_ref.shape
    half = model // 2
    width = dense_gate_ref.shape[0]
    window = width * group_size
    place = me % group_size
    team = me // group_size
    teams = n // group_size
    first = team * window
    owner = first // half
    lane = pl.multiple_of(first % half, window)
    f32 = jnp.float32
    local_heads = bias_ref.shape[1]
    head_dim, cache_len = keys_hbm.shape[1:]
    span = 4

    def remote(source, target, send_sem, recv_sem, ep, tp):
        return pltpu.make_async_remote_copy(
            src_ref=source,
            dst_ref=target,
            send_sem=send_sem,
            recv_sem=recv_sem,
            device_id=(ep, tp),
            device_id_type=MESH,
        )

    pairs = (
        (w_query_hbm, w_query),
        (w_gate_hbm, w_gate),
        (w_up_hbm, w_up),
        (w_down_hbm, w_down),
        (w_out_hbm, w_out),
    )
    loads = [
        pltpu.make_async_copy(source, target, load_sem.at[i])
        for i, (source, target) in enumerate(pairs)
    ]

    def keys_load(c):
        block = pl.ds(c * span, span)
        return pltpu.make_async_copy(keys_hbm.at[block], keys.at[block], keys_sem.at[c])

    def values_load(c):
        block = pl.ds(c * span, span)
        return pltpu.make_async_copy(values_hbm.at[block], values.at[block], values_sem.at[c])

    loads[0].start()
    for c in range(rows // span):
        keys_load(c).start()
        values_load(c).start()
    for load in (loads[4], loads[1], loads[2], loads[3]):
        load.start()

    barrier = pltpu.get_barrier_semaphore()

    def greet(k, carry):
        other = lax.rem(me + k, n)
        pl.semaphore_signal(barrier, inc=1, device_id=(other, core), device_id_type=MESH)
        pl.semaphore_signal(barrier, inc=1, device_id=(other, peer), device_id_type=MESH)
        return carry

    lax.fori_loop(1, n, greet, 0)
    pl.semaphore_signal(barrier, inc=1, device_id=(me, peer), device_id_type=MESH)

    start = tokens_ref[...].astype(f32)
    normed_ref[...] = (
        start
        * lax.rsqrt(jnp.mean(start * start, axis=-1, keepdims=True) + 1e-06)
        * attn_gain_ref[...]
    ).astype(jnp.bfloat16)
    loads[0].wait()
    queries = jnp.dot(normed_ref[...], w_query[...], preferred_element_type=f32)
    queries = queries.astype(jnp.bfloat16).astype(f32)
    for h in range(local_heads):
        query_ref[:, h, :] = queries[:, h * head_dim : (h + 1) * head_dim]
    pl.semaphore_wait(barrier, 2 * n - 1)

    def team_copy(source, gathered, sems, origin, other):
        return remote(
            source,
            gathered.at[origin],
            sems.at[0, other],
            sems.at[1, origin],
            team * group_size + other,
            core,
        )

    def send_weights(k, carry):
        other = lax.rem(place + k, group_size)
        team_copy(dense_gate_ref, dense_gate_all, dense_gate_sems, place, other).start()
        team_copy(dense_up_ref, dense_up_all, dense_up_sems, place, other).start()
        team_copy(down_ref, down_all, down_sems, place, other).start()
        return carry

    lax.fori_loop(1, group_size, send_weights, 0)
    dense_gate_all[place] = dense_gate_ref[...]
    dense_up_all[place] = dense_up_ref[...]
    down_all[place] = down_ref[...]

    block_len = min(256, cache_len)
    after_mask = (
        lax.broadcasted_iota(jnp.int32, (block_len, block_len), 0)
        > lax.broadcasted_iota(jnp.int32, (block_len, block_len), 1)
    ).astype(jnp.bfloat16)
    position = lax.broadcasted_iota(jnp.int32, (span * local_heads, block_len), 1)

    head_row = lax.broadcasted_iota(jnp.int32, (local_heads, local_heads), 0)
    head_col = lax.broadcasted_iota(jnp.int32, (local_heads, local_heads), 1)
    bias = jnp.sum(jnp.where(head_row == head_col, bias_ref[...], 0.0), axis=1, keepdims=True)
    lines = span * local_heads
    line_seq = lax.broadcasted_iota(jnp.int32, (lines, rows), 0) // local_heads
    seq_lane = lax.broadcasted_iota(jnp.int32, (lines, rows), 1)
    lengths_row = lengths_ref[...].astype(f32)

    def attend(c, carry):
        keys_load(c).wait()
        for i in range(span):
            s = c * span + i
            score_ref[s] = (
                jnp.dot(query_ref[s].astype(jnp.bfloat16), keys[s], preferred_element_type=f32)
                * head_dim ** (-0.5)
                + bias
            )
        limits = jnp.sum(
            jnp.where(seq_lane == line_seq + c * span, lengths_row, 0.0), axis=1, keepdims=True
        ).astype(jnp.int32)
        later = jnp.zeros((lines, 1), f32)
        for first_pos in range(cache_len - block_len, -1, -block_len):
            columns = slice(first_pos, first_pos + block_len)
            scores = score_ref[pl.ds(c * span, span), :, columns].reshape(lines, block_len)
            visible = position + first_pos < limits
            keep = -(jnp.maximum(scores, 0.0) + jnp.log1p(jnp.exp(-jnp.abs(scores))))
            log_take = scores + keep
            keep = jnp.where(visible, keep, 0.0)
            top = keep.astype(jnp.bfloat16)
            rest = keep - top.astype(f32)
            middle = rest.astype(jnp.bfloat16)
            low = (rest - middle.astype(f32)).astype(jnp.bfloat16)
            sums = jnp.dot(
                jnp.concatenate([top, middle, low], axis=0),
                after_mask,
                preferred_element_type=f32,
            )
            after = sums[:lines] + sums[lines : 2 * lines] + sums[2 * lines :] + later
            later = later + jnp.sum(keep, axis=-1, keepdims=True)
            stick = jnp.where(visible, jnp.exp(log_take + after), 0.0)
            score_ref[pl.ds(c * span, span), :, columns] = stick.reshape(
                span, local_heads, block_len
            )
        values_load(c).wait()
        for i in range(span):
            s = c * span + i
            read_ref[s] = lax.dot_general(
                score_ref[s].astype(jnp.bfloat16),
                values[s],
                (((1,), (1,)), ((), ())),
                preferred_element_type=f32,
            )
        return carry

    lax.fori_loop(0, rows // span, attend, 0)
    heads_out = jnp.concatenate(
        [read_ref[:, h, :] for h in range(local_heads)], axis=1
    ).astype(jnp.bfloat16)
    loads[4].wait()
    attn_mine[...] = jnp.dot(heads_out, w_out[...], preferred_element_type=f32).astype(
        jnp.bfloat16
    )

    swap = remote(attn_mine, attn_peer, pair_sems.at[0], pair_sems.at[1], me, peer)
    swap.start()
    swap.wait()
    attn = attn_mine[...].astype(f32) + attn_peer[...].astype(f32)
    residual = (tokens_ref[...].astype(f32) + attn).astype(jnp.bfloat16)
    res_ref[...] = residual
    wide = residual.astype(f32)
    normed = (
        wide * lax.rsqrt(jnp.mean(wide * wide, axis=-1, keepdims=True) + 1e-06) * gain_ref[...]
    ).astype(jnp.bfloat16)
    norm_all[0, me] = normed[:, :half]
    norm_all[1, me] = normed[:, half:]

    def norm_copy(j, other):
        return remote(
            norm_all.at[core, j],
            norm_all.at[core, j],
            norm_sems.at[0, other],
            norm_sems.at[1, j],
            other,
            core,
        )

    def pass_copy(j, which):
        return remote(
            norm_all.at[which, j],
            norm_all.at[which, j],
            pass_sems.at[0, j],
            pass_sems.at[1, j],
            me,
            peer,
        )

    def send_norm(k, carry):
        norm_copy(me, lax.rem(me + k, n)).start()
        return carry

    lax.fori_loop(1, n, send_norm, 0)

    across = (((1,), (1,)), ((), ()))
    probs = jax.nn.sigmoid(
        lax.dot_general(router_ref[...], normed, across, preferred_element_type=f32)
    )
    expert_total = probs.shape[0]
    expert_row = lax.broadcasted_iota(jnp.int32, (expert_total, rows), 0)
    hits = jnp.zeros((expert_total, rows), f32)
    for k in range(routes_ref.shape[0]):
        hits = jnp.where(routes_ref[k : k + 1, :] == expert_row, 1.0, hits)
    picked = jnp.where(hits > 0.0, probs, 0.0)
    gates = (picked / jnp.sum(picked, axis=0, keepdims=True) * 2.5).T
    expert_index = lax.broadcasted_iota(jnp.int32, (rows, expert_total), 1)
    mix_gate = jax.nn.sigmoid(
        jnp.sum(normed.astype(f32) * mix_ref[...], axis=-1, keepdims=True)
    )

    for weight, target in ((w_key_ref, new_keys_ref), (w_value_ref, new_values_ref)):
        target[...] = lax.dot_general(
            normed_ref[...], weight[...], across, preferred_element_type=f32
        ).astype(jnp.bfloat16)

    def take_norm(k, carry):
        j = lax.rem(me + n - k, n)
        norm_copy(j, me).wait_recv()
        pass_copy(j, core).start()
        return carry

    lax.fori_loop(1, n, take_norm, 0)

    def take_pass(k, carry):
        pass_copy(lax.rem(me + n - k, n), peer).wait_recv()
        return carry

    lax.fori_loop(1, n, take_pass, 0)

    def part_copy(m, other):
        return remote(
            part_send.at[other],
            part_recv.at[m],
            part_sems.at[0, other],
            part_sems.at[1, m],
            other * group_size + place,
            core,
        )

    def back_copy(j, other):
        return remote(
            back_send.at[other],
            back_recv.at[j],
            back_sems.at[0, other],
            back_sems.at[1, j],
            other,
            core,
        )

    def dense_copy(m, other):
        return remote(
            dense_all.at[m],
            dense_all.at[m],
            dense_sems.at[0, other],
            dense_sems.at[1, m],
            other * group_size + place,
            core,
        )

    group = min(n, 16)
    groups = n // group
    block = group * rows

    def take_weights(k, carry):
        other = lax.rem(place + k, group_size)
        team_copy(dense_gate_ref, dense_gate_all, dense_gate_sems, other, place).wait_recv()
        team_copy(dense_up_ref, dense_up_all, dense_up_sems, other, place).wait_recv()
        team_copy(down_ref, down_all, down_sems, other, place).wait_recv()
        return carry

    lax.fori_loop(1, group_size, take_weights, 0)
    features = jnp.concatenate(
        [norm_all[owner, m * group_size + place, :, pl.ds(lane, window)] for m in range(teams)],
        axis=0,
    )
    hidden_cols = dense_gate_ref.shape[1]
    for gathered, columns in (
        (dense_gate_all, slice(0, hidden_cols)),
        (dense_up_all, slice(hidden_cols, 2 * hidden_cols)),
    ):
        value = jnp.dot(
            features, gathered[...].reshape(window, hidden_cols), preferred_element_type=f32
        )
        part_send[:, :, columns] = value.astype(jnp.bfloat16).reshape(teams, rows, hidden_cols)

    def send_part(k, carry):
        part_copy(team, lax.rem(team + k, teams)).start()
        return carry

    lax.fori_loop(1, teams, send_part, 0)

    loads[1].wait()
    loads[2].wait()

    def expert_first(c, carry):
        base = c * group
        low = norm_all[0, pl.ds(base, group)].reshape(block, half)
        high = norm_all[1, pl.ds(base, group)].reshape(block, half)
        gate_rows = jnp.dot(low, w_gate[:half], preferred_element_type=f32) + jnp.dot(
            high, w_gate[half:], preferred_element_type=f32
        )
        up_rows = jnp.dot(low, w_up[:half], preferred_element_type=f32) + jnp.dot(
            high, w_up[half:], preferred_element_type=f32
        )
        hidden_ref[pl.ds(c, 1)] = (jax.nn.silu(gate_rows) * up_rows).astype(jnp.bfloat16)[None]
        return carry

    lax.fori_loop(0, groups, expert_first, 0)

    def take_part(k, total):
        m = lax.rem(team + teams - k, teams)
        part_copy(m, team).wait_recv()
        return total + part_recv[m].astype(f32)

    paired = lax.fori_loop(1, teams, take_part, part_send[team].astype(f32))
    dense_all[team] = (jax.nn.silu(paired[:, :hidden_cols]) * paired[:, hidden_cols:]).astype(
        jnp.bfloat16
    )

    def send_dense(k, carry):
        dense_copy(team, lax.rem(team + k, teams)).start()
        return carry

    lax.fori_loop(1, teams, send_dense, 0)

    loads[3].wait()
    far = pl.ds(pl.multiple_of(peer * half, half), half)
    near = pl.ds(pl.multiple_of(core * half, half), half)

    def expert_far(c, carry):
        value = jnp.dot(hidden_ref[c], w_down[:, far], preferred_element_type=f32)
        other_ref[pl.ds(c * group, group)] = value.astype(jnp.bfloat16).reshape(group, rows, half)
        return carry

    lax.fori_loop(0, groups, expert_far, 0)
    trade = remote(other_ref, peer_ref, pair_sems.at[2], pair_sems.at[3], me, peer)
    trade.start()

    def expert_near(c, carry):
        value = jnp.dot(hidden_ref[c], w_down[:, near], preferred_element_type=f32)
        mine_ref[pl.ds(c * group, group)] = value.astype(jnp.bfloat16).reshape(group, rows, half)
        return carry

    lax.fori_loop(0, groups, expert_near, 0)
    trade.wait()

    def send_back(k, carry):
        other = lax.rem(me + k, n)
        total = mine_ref[other].astype(f32) + peer_ref[other].astype(f32)
        back_send[other] = total.astype(jnp.bfloat16)

        @pl.when(k > 0)
        def _():
            back_copy(me, other).start()

        return carry

    lax.fori_loop(0, n, send_back, 0)

    def take_dense(k, carry):
        dense_copy(lax.rem(team + teams - k, teams), team).wait_recv()
        return carry

    lax.fori_loop(1, teams, take_dense, 0)
    dense_rows = dense_all[...].reshape(teams * rows, hidden_cols)
    columns = [
        jnp.dot(dense_rows, down_all[q], preferred_element_type=f32) for q in range(group_size)
    ]
    cols_send[...] = (
        jnp.concatenate(columns, axis=1).astype(jnp.bfloat16).reshape(cols_send.shape)
    )

    def cols_copy(from_core, m, other, target):
        return remote(
            cols_send.at[other],
            cols_recv.at[from_core, m],
            cols_send_sem.at[other],
            cols_recv_sem.at[from_core, m],
            other * group_size + place,
            target,
        )

    def send_cols(k, carry):
        cols_copy(core, team, lax.rem(team + k, teams), owner).start()
        return carry

    lax.fori_loop(1, teams, send_cols, 0)

    @pl.when(owner == core)
    def _():
        cols_recv[core, team] = cols_send[team]

    @pl.when(owner != core)
    def _():
        cols_copy(core, team, team, peer).start()

    side = teams // 2

    def take_cols(k, carry):
        m = core * side + k

        @pl.when(m != team)
        def _():
            cols_copy(core, m, team, core).wait_recv()

        cols_copy(peer, m, team, core).wait_recv()
        return carry

    lax.fori_loop(0, side, take_cols, 0)
    dense = jnp.concatenate(
        [
            cols_recv[0, core * side + q].astype(f32) + cols_recv[1, core * side + q].astype(f32)
            for q in range(side)
        ],
        axis=1,
    )
    total = res_ref[:, near].astype(f32) + mix_gate * dense

    def take_back(k, total):
        j = lax.rem(me + n - k, n)

        @pl.when(k > 0)
        def _():
            back_copy(j, me).wait_recv()

        @pl.when(k == 0)
        def _():
            back_recv[me] = back_send[me]

        gate = jnp.sum(jnp.where(expert_index == j, gates, 0.0), axis=-1, keepdims=True)
        return total + gate * back_recv[j].astype(f32)

    out_ref[...] = lax.fori_loop(0, n, take_back, total).astype(jnp.bfloat16)

    def drain(k, carry):
        other = lax.rem(me + k, n)
        norm_copy(me, other).wait_send()
        pass_copy(other, core).wait_send()
        back_copy(me, other).wait_send()
        return carry

    lax.fori_loop(1, n, drain, 0)

    def drain_team(k, carry):
        other = lax.rem(place + k, group_size)
        team_copy(dense_gate_ref, dense_gate_all, dense_gate_sems, place, other).wait_send()
        team_copy(dense_up_ref, dense_up_all, dense_up_sems, place, other).wait_send()
        team_copy(down_ref, down_all, down_sems, place, other).wait_send()
        return carry

    lax.fori_loop(1, group_size, drain_team, 0)

    def drain_dense(k, carry):
        other = lax.rem(team + k, teams)
        part_copy(team, other).wait_send()
        dense_copy(team, other).wait_send()
        cols_copy(core, team, other, owner).wait_send()
        return carry

    lax.fori_loop(1, teams, drain_dense, 0)

    @pl.when(owner != core)
    def _():
        cols_copy(core, team, team, peer).wait_send()


def flip(place, k):
    result, bit = place, 1
    while bit <= k:
        if k & bit:
            result = result + bit * (1 - 2 * ((place // bit) % 2))
        bit *= 2
    return result


def finish(*refs):
    copies = [
        pltpu.make_async_copy(refs[i], refs[i + 3], refs[6].at[i]) for i in range(3)
    ]
    for copy in copies:
        copy.start()
    for copy in copies:
        copy.wait()


def routed_layer(
    n,
    inner,
    tokens_hbm,
    attn_gain_hbm,
    lengths_hbm,
    bias_hbm,
    w_key_hbm,
    w_value_hbm,
    gain_hbm,
    router_hbm,
    routes_hbm,
    mix_hbm,
    dense_gate_hbm,
    dense_up_hbm,
    down_hbm,
    w_query_hbm,
    w_out_hbm,
    w_gate_hbm,
    w_up_hbm,
    w_down_hbm,
    keys_hbm,
    values_hbm,
    out_ref,
    new_keys_ref,
    new_values_ref,
    tokens_ref,
    attn_gain_ref,
    lengths_ref,
    bias_ref,
    w_key_ref,
    w_value_ref,
    gain_ref,
    router_ref,
    routes_ref,
    mix_ref,
    dense_gate_ref,
    dense_up_ref,
    down_ref,
    w_query,
    w_out,
    w_gate,
    w_up,
    w_down,
    keys,
    values,
    query_ref,
    score_ref,
    read_ref,
    stick_ref,
    normed_ref,
    small_send,
    small,
    routes_all,
    hits_ref,
    attn_mine,
    attn_peer,
    res_ref,
    norm_all,
    first_send,
    first_recv,
    plane_send,
    plane_recv,
    far_recv,
    line_send,
    line_recv,
    load_sem,
    keys_sem,
    values_sem,
    pair_sems,
    swap_sems,
    small_send_sem,
    small_recv_sem,
    down_send_sem,
    down_recv_sem,
    routes_sems,
    line_sems,
    spread_sems,
    first_sems,
    plane_sems,
    far_sems,
    back_sems,
):
    me = lax.axis_index("ep")
    core = lax.axis_index("tp")
    peer = 1 - core
    f32, bf16 = jnp.float32, jnp.bfloat16
    rows, model = tokens_ref.shape
    half = model // 2
    width, hidden_cols = dense_gate_ref.shape
    units = hidden_cols // n
    outer = n // inner
    z, p = me // inner, me % inner
    side = n // 2
    owner, slot = me // side, me % side
    local_heads = bias_ref.shape[1]
    head_dim, cache_len = keys_hbm.shape[1:]
    hidden = w_gate_hbm.shape[1]
    expert_total = router_ref.shape[0]
    lanes = small.shape[0]
    router_at = 4 * units
    mix_at = router_at + expert_total
    span = rows // 2
    turns = list(range(outer - 1, 0, -1))
    direct = [j for j in range(1, inner) if j & (j - 1) == 0]
    indirect = [j for j in range(1, inner) if j & (j - 1)]
    lines = span * local_heads

    def remote(source, target, send_sem, recv_sem, ep, tp):
        return pltpu.make_async_remote_copy(
            src_ref=source,
            dst_ref=target,
            send_sem=send_sem,
            recv_sem=recv_sem,
            device_id=(ep, tp),
            device_id_type=MESH,
        )

    near = pl.ds(pl.multiple_of(core * half, half), half)
    far = pl.ds(pl.multiple_of(peer * half, half), half)
    mine = pl.ds(pl.multiple_of(core * hidden, hidden), hidden)
    quarter = model // 4
    query_parts = [pl.ds(i * quarter, quarter) for i in range(4)]
    pairs = (
        (tokens_hbm, tokens_ref),
        (attn_gain_hbm, attn_gain_ref),
        (dense_gate_hbm, dense_gate_ref),
        (dense_up_hbm, dense_up_ref),
        (routes_hbm, routes_ref),
        *[(w_query_hbm.at[part], w_query.at[part]) for part in query_parts],
        (bias_hbm, bias_ref),
        (lengths_hbm, lengths_ref),
        (down_hbm, down_ref),
        (router_hbm, router_ref),
        (mix_hbm, mix_ref),
        (gain_hbm, gain_ref),
        (w_out_hbm, w_out),
        (w_key_hbm, w_key_ref),
        (w_value_hbm, w_value_ref),
        (w_gate_hbm.at[near, :], w_gate.at[:, mine]),
        (w_up_hbm.at[near, :], w_up.at[:, mine]),
        (w_down_hbm.at[:, near], w_down.at[mine, :]),
    )
    loads = [
        pltpu.make_async_copy(source, target, load_sem.at[i])
        for i, (source, target) in enumerate(pairs)
    ]
    load_of = {id(target): load for (_, target), load in zip(pairs, loads)}

    def arrived(*targets):
        for target in targets:
            load_of[id(target)].wait()

    def keys_load(c):
        block = pl.ds(c * span, span)
        return pltpu.make_async_copy(keys_hbm.at[block], keys.at[block], keys_sem.at[c])

    def values_load(c):
        block = pl.ds(c * span, span)
        return pltpu.make_async_copy(values_hbm.at[block], values.at[block], values_sem.at[c])

    for load in loads[:12]:
        load.start()

    barrier = pltpu.get_barrier_semaphore()

    def greet(k, carry):
        other = lax.rem(me + k, n)
        pl.semaphore_signal(barrier, inc=1, device_id=(other, core), device_id_type=MESH)
        pl.semaphore_signal(barrier, inc=1, device_id=(other, peer), device_id_type=MESH)
        return carry

    lax.fori_loop(1, n, greet, 0)
    pl.semaphore_signal(barrier, inc=1, device_id=(me, peer), device_id_type=MESH)

    arrived(tokens_ref, attn_gain_ref)
    start = tokens_ref[...].astype(f32)
    normed_ref[...] = (
        start
        * lax.rsqrt(jnp.mean(start * start, axis=-1, keepdims=True) + 1e-06)
        * attn_gain_ref[...]
    ).astype(bf16)
    for c in range(2):
        keys_load(c).start()
    arrived(dense_gate_ref, dense_up_ref, routes_ref)
    small_send[:, :units, :] = dense_gate_ref[...].T.reshape(n, units, width)
    small_send[:, units:, :] = dense_up_ref[...].T.reshape(n, units, width)
    top_k = routes_ref.shape[0]
    for k in range(top_k):
        routes_all[me, :, k * rows : (k + 1) * rows] = routes_ref[k : k + 1, :].astype(f32)

    queries = jnp.zeros((rows, w_query.shape[1]), f32)
    for i in range(4):
        loads[5 + i].wait()
        if i % 2:
            values_load(i // 2).start()
        part = slice(i * quarter, (i + 1) * quarter)
        queries = queries + jnp.dot(
            normed_ref[:, part], w_query[part, :], preferred_element_type=f32
        )
    queries = queries.astype(bf16).astype(f32)
    for h in range(local_heads):
        query_ref[:, h, :] = queries[:, h * head_dim : (h + 1) * head_dim]

    block_len = min(256, cache_len)
    after_mask = (
        lax.broadcasted_iota(jnp.int32, (block_len, block_len), 0)
        > lax.broadcasted_iota(jnp.int32, (block_len, block_len), 1)
    ).astype(bf16)
    position = lax.broadcasted_iota(jnp.int32, (lines, block_len), 1)
    arrived(bias_ref, lengths_ref)
    head_row = lax.broadcasted_iota(jnp.int32, (local_heads, local_heads), 0)
    head_col = lax.broadcasted_iota(jnp.int32, (local_heads, local_heads), 1)
    bias = jnp.sum(jnp.where(head_row == head_col, bias_ref[...], 0.0), axis=1, keepdims=True)
    line_seq = lax.broadcasted_iota(jnp.int32, (lines, rows), 0) // local_heads
    seq_lane = lax.broadcasted_iota(jnp.int32, (lines, rows), 1)
    lengths_row = lengths_ref[...].astype(f32)

    for s in range(rows):
        if s % span == 0:
            keys_load(s // span).wait()
            for load in loads[12:16] if s == 0 else loads[16:]:
                load.start()
        score_ref[s] = (
            jnp.dot(query_ref[s].astype(bf16), keys[s], preferred_element_type=f32)
            * head_dim ** (-0.5)
            + bias
        )

    def stick_breaking(c):
        limits = jnp.sum(
            jnp.where(seq_lane == line_seq + c * span, lengths_row, 0.0), axis=1, keepdims=True
        ).astype(jnp.int32)
        later = jnp.zeros((lines, 1), f32)
        for first_pos in range(cache_len - block_len, -1, -block_len):
            columns = slice(first_pos, first_pos + block_len)
            scores = score_ref[c * span : (c + 1) * span, :, columns].reshape(lines, block_len)
            visible = position + first_pos < limits
            keep = -(jnp.maximum(scores, 0.0) + jnp.log(1.0 + jnp.exp(-jnp.abs(scores))))
            log_take = scores + keep
            keep = jnp.where(visible, keep, 0.0)
            top = keep.astype(bf16)
            low = (keep - top.astype(f32)).astype(bf16)
            sums = jnp.dot(
                jnp.concatenate([top, low], axis=0), after_mask, preferred_element_type=f32
            )
            after = sums[:lines] + sums[lines:] + later
            later = later + jnp.sum(keep, axis=-1, keepdims=True)
            stick = jnp.where(visible, jnp.exp(log_take + after), 0.0)
            stick_ref[c, :, columns] = stick.astype(bf16)

    def read_values(c):
        mixed = lax.dot_general(
            values[c * span : (c + 1) * span].reshape(span * head_dim, cache_len),
            stick_ref[c],
            (((1,), (1,)), ((), ())),
            preferred_element_type=f32,
        ).reshape(span, head_dim, lines)
        seq_of = lax.broadcasted_iota(jnp.int32, (head_dim, lines), 1) // local_heads
        own_seq = jnp.zeros((head_dim, lines), f32)
        for s in range(span):
            own_seq = jnp.where(seq_of == s, mixed[s], own_seq)
        read_ref[c * span : (c + 1) * span] = own_seq.T.reshape(span, local_heads, head_dim)

    pl.semaphore_wait(barrier, 2 * n - 1)
    trades = [
        remote(
            w_gate_hbm.at[far, :], w_gate.at[:, mine], pair_sems.at[0, 0], pair_sems.at[1, 0], me, peer
        ),
        remote(
            w_up_hbm.at[far, :], w_up.at[:, mine], pair_sems.at[0, 1], pair_sems.at[1, 1], me, peer
        ),
        remote(
            w_down_hbm.at[:, far], w_down.at[mine, :], pair_sems.at[0, 2], pair_sems.at[1, 2], me, peer
        ),
    ]

    def small_copy(other, tp):
        return remote(
            small_send.at[other],
            small.at[pl.ds(core * 2 * units, 2 * units), pl.ds(pl.multiple_of(slot * width, width), width)],
            small_send_sem.at[other],
            small_recv_sem.at[core, slot],
            other,
            tp,
        )

    def down_copy(other, tp):
        return remote(
            down_ref.at[pl.ds(pl.multiple_of(other * units, units), units), :],
            w_down.at[
                pl.ds(2 * hidden + core * 2 * units, units),
                pl.ds(pl.multiple_of(slot * width, width), width),
            ],
            down_send_sem.at[other],
            down_recv_sem.at[core, slot],
            other,
            tp,
        )

    def routes_copy(origin, other):
        return remote(
            routes_all.at[origin],
            routes_all.at[origin],
            routes_sems.at[0, other],
            routes_sems.at[1, origin],
            other,
            core,
        )

    arrived(down_ref)

    def send_small(k, carry):
        other = lax.rem(me + k, n)
        routes_copy(me, other).start()
        small_copy(other, owner).start()
        return carry

    def send_down(k, carry):
        down_copy(lax.rem(me + k, n), owner).start()
        return carry

    lax.fori_loop(1, n, send_small, 0)

    @pl.when(owner == core)
    def _():
        here = pl.ds(pl.multiple_of(slot * width, width), width)
        small[pl.ds(pl.multiple_of(core * 2 * units, 2 * units), 2 * units), here] = small_send[me]
        w_down[
            pl.ds(pl.multiple_of(2 * hidden + core * 2 * units, units), units), here
        ] = down_ref[pl.ds(pl.multiple_of(me * units, units), units), :]

    @pl.when(owner != core)
    def _():
        small_copy(me, peer).start()

    for c in range(2):
        values_load(c).wait()
    for c in range(2):
        stick_breaking(c)
        read_values(c)
    heads_out = jnp.concatenate([read_ref[:, h, :] for h in range(local_heads)], axis=1).astype(
        bf16
    )
    arrived(w_out)
    swaps = []
    for i in range(2):
        attn_mine[i] = jnp.dot(
            heads_out, w_out[:, i * half : (i + 1) * half], preferred_element_type=f32
        ).astype(bf16)
        swaps.append(
            remote(
                attn_mine.at[i], attn_peer.at[i], swap_sems.at[0, i], swap_sems.at[1, i], me, peer
            )
        )
        swaps[i].start()
    for trade in trades:
        trade.start()
    arrived(gain_ref)
    wide = []
    for i in range(2):
        swaps[i].wait_recv()
        columns = slice(i * half, (i + 1) * half)
        res_ref[i] = (
            tokens_ref[:, columns].astype(f32)
            + (attn_mine[i].astype(f32) + attn_peer[i].astype(f32))
        ).astype(bf16)
        wide.append(res_ref[i].astype(f32))
    squares = sum(jnp.sum(part * part, axis=-1, keepdims=True) for part in wide)
    scale = lax.rsqrt(squares / model + 1e-06)
    norm_all[me] = (
        jnp.where(core == 0, wide[0], wide[1])
        * scale
        * jnp.where(core == 0, gain_ref[:, :half], gain_ref[:, half:])
    ).astype(bf16)

    def line_copy(k):
        return remote(
            norm_all.at[me],
            norm_all.at[me],
            line_sems.at[0, k],
            line_sems.at[1, k],
            flip(z, k) * inner + p,
            core,
        )

    def spread_copy(k, j):
        origin = flip(z, k) * inner + p
        return remote(
            norm_all.at[origin],
            norm_all.at[origin],
            spread_sems.at[0, k, j],
            spread_sems.at[1, k, j],
            z * inner + flip(p, j),
            core,
        )

    for k in turns:
        line_copy(k).start()
    for j in indirect + direct:
        spread_copy(0, j).start()

    lax.fori_loop(1, n, send_down, 0)

    @pl.when(owner != core)
    def _():
        down_copy(me, peer).start()


    across = (((1,), (1,)), ((), ()))
    arrived(w_key_ref, w_value_ref)
    for weight, target in ((w_key_ref, new_keys_ref), (w_value_ref, new_values_ref)):
        target[...] = lax.dot_general(
            normed_ref[...], weight[...], across, preferred_element_type=f32
        ).astype(bf16)

    def small_taken(tp, k):
        return remote(
            small_send.at[0],
            small.at[
                pl.ds(tp * 2 * units, 2 * units), pl.ds(pl.multiple_of(k * width, width), width)
            ],
            small_send_sem.at[0],
            small_recv_sem.at[tp, k],
            me,
            peer,
        )

    def down_taken(tp, k):
        return remote(
            down_ref.at[pl.ds(0, units), :],
            w_down.at[
                pl.ds(2 * hidden + tp * 2 * units, units),
                pl.ds(pl.multiple_of(k * width, width), width),
            ],
            down_send_sem.at[0],
            down_recv_sem.at[tp, k],
            me,
            peer,
        )

    def take_all(taken):
        def take(k, carry):
            @pl.when(core * side + k != me)
            def _():
                taken(core, k).wait_recv()

            taken(peer, k).wait_recv()
            return carry

        lax.fori_loop(0, side, take, 0)

    arrived(router_ref, mix_ref)
    spread_rows = lanes - mix_at
    mix_row = mix_ref[...]
    mix_top = mix_row.astype(bf16)
    mix_rest = mix_row - mix_top.astype(f32)
    mix_mid = mix_rest.astype(bf16)
    mix_low = (mix_rest - mix_mid.astype(f32)).astype(bf16)
    mix_index = lax.broadcasted_iota(jnp.int32, (spread_rows, model), 0)
    mix_rows = jnp.where(
        mix_index == 0,
        mix_top.astype(f32),
        jnp.where(
            mix_index == 1,
            mix_mid.astype(f32),
            jnp.where(mix_index == 2, mix_low.astype(f32), 0.0),
        ),
    ).astype(bf16)
    small[pl.ds(router_at, expert_total), :] = jnp.where(
        core == 0, router_ref[:, :half], router_ref[:, half:]
    )
    small[pl.ds(mix_at, spread_rows), :] = jnp.where(
        core == 0, mix_rows[:, :half], mix_rows[:, half:]
    )
    for base in (units, 3 * units):
        w_down[pl.ds(2 * hidden + base, units), :] = jnp.zeros((units, half), bf16)
    tail = lanes - 4 * units
    w_down[pl.ds(2 * hidden + 4 * units, tail), :] = jnp.zeros((tail, half), bf16)

    for k in turns:
        line_copy(k).wait_recv()
        for j in indirect + direct:
            spread_copy(k, j).start()
    take_all(small_taken)

    arrived(*[target for _, target in pairs[18:]])
    for trade in trades:
        trade.wait_recv()

    chunk = inner * rows
    lane = lax.broadcasted_iota(jnp.int32, (chunk, lanes), 1)
    dense_lane = (lane < units) | ((lane >= 2 * units) & (lane < 3 * units))

    rest_at = 2 * hidden + lanes

    def first_copy(k):
        return remote(
            first_send.at[k], first_recv.at[k], first_sems.at[0, k], first_sems.at[1, k], me, peer
        )

    def group(k):
        return pl.ds(pl.multiple_of(flip(z, k) * inner, inner), inner)

    def first(k):
        for j in range(1, inner):
            spread_copy(k, j).wait_recv()
        x = norm_all[group(k)].reshape(chunk, half)
        first_send[k, :, : 2 * hidden] = jnp.dot(x, w_gate[...], preferred_element_type=f32)
        first_send[k, :, 2 * hidden : rest_at] = lax.dot_general(
            x, small[...], across, preferred_element_type=f32
        )
        first_send[k, :, rest_at:] = jnp.dot(x, w_up[...], preferred_element_type=f32)
        first_copy(k).start()

    def plane_copy(k, j):
        other = flip(p, j)
        return remote(
            plane_send.at[k, other],
            plane_recv.at[k, j],
            plane_sems.at[0, k, j],
            plane_sems.at[1, k, j],
            z * inner + other,
            core,
        )

    def far_copy(k, j):
        return remote(
            plane_send.at[k, flip(p, j)],
            far_recv.at[k, j],
            far_sems.at[0, k, j],
            far_sems.at[1, k, j],
            flip(z, k) * inner + p,
            core,
        )

    def send_plane(k):
        for j in direct:
            plane_copy(k, j).start()
        if k:
            for j in indirect:
                far_copy(k, j).start()

    def second(k):
        first_copy(k).wait_recv()
        gate_rows = first_send[k, :, : 2 * hidden] + first_recv[k, :, : 2 * hidden]
        up_rows = first_send[k, :, rest_at:] + first_recv[k, :, rest_at:]
        rest = first_send[k, :, 2 * hidden : rest_at] + first_recv[k, :, 2 * hidden : rest_at]
        chosen = hits_ref[group(k)].reshape(chunk, lanes)
        picked = jnp.where(chosen > 0.0, jax.nn.sigmoid(rest), 0.0)
        total = jnp.sum(picked, axis=-1, keepdims=True)
        own = jnp.sum(jnp.where(lane == router_at + me, picked, 0.0), axis=-1, keepdims=True)
        gate = own / total * 2.5
        mix_sum = jnp.sum(jnp.where(lane >= mix_at, rest, 0.0), axis=-1, keepdims=True)
        mix_gate = jax.nn.sigmoid(mix_sum)
        dense = jax.nn.silu(rest) * pltpu.roll(rest, lanes - units, 1) * mix_gate
        dense = jnp.where(dense_lane, dense, 0.0).astype(bf16)
        act = (jax.nn.silu(gate_rows) * up_rows * gate).astype(bf16)
        value = jnp.dot(act, w_down[: 2 * hidden], preferred_element_type=f32) + jnp.dot(
            dense, w_down[2 * hidden :], preferred_element_type=f32
        )
        plane_send[k] = value.astype(bf16).reshape(inner, rows, half)
        send_plane(k)

    def far_home(j):
        return remote(
            far_recv.at[0, j],
            plane_recv.at[0, j],
            plane_sems.at[0, 0, j],
            plane_sems.at[1, 0, j],
            z * inner + flip(p, j),
            core,
        )

    def back_copy(k):
        return remote(
            line_send.at[k],
            line_recv.at[k],
            back_sems.at[0, k],
            back_sems.at[1, k],
            flip(z, k) * inner + p,
            core,
        )

    def collect(k):
        total = plane_send[k, p].astype(f32)
        for j in direct:
            plane_copy(k, j).wait_recv()
            total = total + plane_recv[k, j].astype(f32)
        return total

    def third(k):
        line_send[k] = collect(k).astype(bf16)
        back_copy(k).start()

    first(0)
    def take_routes(k, carry):
        routes_copy(lax.rem(me + n - k, n), me).wait_recv()
        return carry

    lax.fori_loop(1, n, take_routes, 0)
    row_lane = (lax.broadcasted_iota(jnp.int32, (rows, lanes), 1) - router_at).astype(f32)
    named = routes_all[...].reshape(n, lanes).T
    for j in range(n):
        hit = jnp.zeros((rows, lanes), f32)
        for c in range(top_k):
            hit = jnp.where(named[c * rows : (c + 1) * rows, j : j + 1] == row_lane, 1.0, hit)
        hits_ref[j] = hit

    first(turns[0])
    take_all(down_taken)
    second(0)
    for before, k in zip(turns, turns[1:]):
        first(k)
        second(before)
    second(turns[-1])
    for k in turns:
        third(k)
    for j in indirect:
        other = flip(p, j)
        total = plane_send[0, other].astype(f32)
        for k in turns:
            far_copy(k, j).wait_recv()
            total = total + far_recv[k, j].astype(f32)
        far_recv[0, j] = total.astype(bf16)
        far_home(j).start()
    total = res_ref[core].astype(f32) + collect(0)
    for k in turns:
        back_copy(k).wait_recv()
        total = total + line_recv[k].astype(f32)
    for j in indirect:
        far_home(j).wait_recv()
        total = total + plane_recv[0, j].astype(f32)
    out_ref[...] = total.astype(bf16)

    def drain(k, carry):
        other = lax.rem(me + k, n)
        small_copy(other, owner).wait_send()
        down_copy(other, owner).wait_send()
        routes_copy(me, other).wait_send()
        return carry

    lax.fori_loop(1, n, drain, 0)

    @pl.when(owner != core)
    def _():
        small_copy(me, peer).wait_send()
        down_copy(me, peer).wait_send()

    for copy in trades + swaps:
        copy.wait_send()
    for k in range(outer):
        if k:
            line_copy(k).wait_send()
            back_copy(k).wait_send()
        first_copy(k).wait_send()
        for j in range(1, inner):
            spread_copy(k, j).wait_send()
            (far_copy if k and j in indirect else plane_copy)(k, j).wait_send()


def routed_shards(n, inner, arrays):
    tokens = arrays[0]
    w_key, head_bias = arrays[4], arrays[3]
    keys, w_gate, w_down = arrays[18], arrays[15], arrays[17]
    rows, model = tokens.shape
    half = model // 2
    width, hidden_cols = arrays[10].shape
    units = hidden_cols // n
    outer = n // inner
    seq_count, head_dim, cache_len = keys.shape
    local_heads = head_bias.shape[1]
    hidden = w_gate.shape[1]
    lanes = 128
    chunk = inner * rows
    bf16, f32 = jnp.bfloat16, jnp.float32
    vmem = pl.BlockSpec(memory_space=pltpu.VMEM)
    anywhere = pl.BlockSpec(memory_space=pltpu.HBM)
    dma = pltpu.SemaphoreType.DMA
    small_inputs = [pltpu.VMEM(a.shape, a.dtype) for a in arrays[:15]]
    results = pl.pallas_call(
        functools.partial(routed_layer, n, inner),
        out_shape=(
            jax.ShapeDtypeStruct((rows, half), bf16),
            jax.ShapeDtypeStruct((rows, w_key.shape[0]), bf16),
            jax.ShapeDtypeStruct((rows, w_key.shape[0]), bf16),
        ),
        in_specs=[anywhere] * 20,
        out_specs=(vmem, vmem, vmem),
        scratch_shapes=small_inputs
        + [
            pltpu.VMEM((half, 2 * hidden), bf16),
            pltpu.VMEM((half, 2 * hidden), bf16),
            pltpu.VMEM((2 * hidden + lanes, half), bf16),
            pltpu.VMEM(keys.shape, bf16),
            pltpu.VMEM(keys.shape, bf16),
            pltpu.VMEM((rows, local_heads, head_dim), f32),
            pltpu.VMEM((rows, local_heads, cache_len), f32),
            pltpu.VMEM((rows, local_heads, head_dim), f32),
            pltpu.VMEM((2, rows * local_heads // 2, cache_len), bf16),
            pltpu.VMEM((rows, model), bf16),
            pltpu.VMEM((n, 2 * units, width), bf16),
            pltpu.VMEM((lanes, half), bf16),
            pltpu.VMEM((n, 1, lanes), f32),
            pltpu.VMEM((n, rows, lanes), f32),
            pltpu.VMEM((2, rows, half), bf16),
            pltpu.VMEM((2, rows, half), bf16),
            pltpu.VMEM((2, rows, half), bf16),
            pltpu.VMEM((n, rows, half), bf16),
            pltpu.VMEM((outer, chunk, 4 * hidden + lanes), f32),
            pltpu.VMEM((outer, chunk, 4 * hidden + lanes), f32),
            pltpu.VMEM((outer, inner, rows, half), bf16),
            pltpu.VMEM((outer, inner, rows, half), bf16),
            pltpu.VMEM((outer, inner, rows, half), bf16),
            pltpu.VMEM((outer, rows, half), bf16),
            pltpu.VMEM((outer, rows, half), bf16),
            dma((21,)),
            dma((2,)),
            dma((2,)),
            dma((2, 3)),
            dma((2, 2)),
            dma((n,)),
            dma((2, n // 2)),
            dma((n,)),
            dma((2, n // 2)),
            dma((2, n)),
            dma((2, outer)),
            dma((2, outer, inner)),
            dma((2, outer)),
            dma((2, outer, inner)),
            dma((2, outer, inner)),
            dma((2, outer)),
        ],
        compiler_params=pltpu.CompilerParams(
            collective_id=0, has_side_effects=True, vmem_limit_bytes=48 * 1024 * 1024
        ),
        name="routed_layer",
    )(*[pltpu.with_memory_space_constraint(a, pltpu.HBM) for a in arrays])
    return pl.pallas_call(
        finish,
        out_shape=tuple(jax.ShapeDtypeStruct(r.shape, r.dtype) for r in results),
        in_specs=[vmem] * 3,
        out_specs=(anywhere,) * 3,
        scratch_shapes=[dma((3,))],
        name="finish",
    )(*[pltpu.with_memory_space_constraint(r, pltpu.VMEM) for r in results])


def shards(
    n,
    tokens,
    lengths,
    attn_gain,
    w_query,
    w_key,
    w_value,
    head_bias,
    key_cache,
    value_cache,
    w_attn_out,
    ffn_gain,
    w_router,
    routes,
    w_dense_gate,
    w_dense_up,
    w_dense_down,
    dense_mix,
    w_expert_gate,
    w_expert_up,
    w_expert_down,
):
    rows, model = tokens.shape
    half = model // 2
    width, hidden_cols = w_dense_gate.shape
    group_size = min(n, max(4, 128 // width))
    teams = n // group_size
    window = width * group_size
    seq_count, local_kv, head_dim, cache_len = key_cache.shape
    local_heads = head_bias.shape[0]
    keys = key_cache.reshape(seq_count, head_dim, cache_len)
    values = value_cache.reshape(seq_count, head_dim, cache_len)
    w_gate, w_up, w_down = w_expert_gate[0], w_expert_up[0], w_expert_down[0]
    expert_hidden = w_gate.shape[1]
    arrays = (
        tokens,
        attn_gain.reshape(1, model),
        lengths.reshape(1, seq_count),
        head_bias.reshape(1, local_heads),
        w_key.T,
        w_value.T,
        ffn_gain.reshape(1, model),
        w_router.T,
        routes.T,
        dense_mix.reshape(1, model),
        w_dense_gate,
        w_dense_up,
        w_dense_down,
        w_query,
        w_attn_out,
        w_gate,
        w_up,
        w_down,
        keys,
        values,
    )
    inner = 1
    while (2 * inner) ** 2 <= n:
        inner *= 2
    small_rows = 4 * (hidden_cols // n) + w_router.shape[1]
    if hidden_cols % (16 * n) == 0 and width % 128 == 0 and small_rows <= 112:
        return routed_shards(n, inner, arrays)
    bf16, f32 = jnp.bfloat16, jnp.float32
    block = min(n, 16) * rows
    vmem = pl.BlockSpec(memory_space=pltpu.VMEM)
    anywhere = pl.BlockSpec(memory_space=pltpu.HBM)
    dma = pltpu.SemaphoreType.DMA
    return pl.pallas_call(
        functools.partial(whole_layer, n, group_size),
        out_shape=(
            jax.ShapeDtypeStruct((rows, half), bf16),
            jax.ShapeDtypeStruct((rows, w_key.shape[1]), bf16),
            jax.ShapeDtypeStruct((rows, w_value.shape[1]), bf16),
        ),
        in_specs=[vmem] * 13 + [anywhere] * 7,
        out_specs=(vmem, vmem, vmem),
        scratch_shapes=[
            pltpu.VMEM(w_query.shape, bf16),
            pltpu.VMEM(w_attn_out.shape, bf16),
            pltpu.VMEM(w_gate.shape, bf16),
            pltpu.VMEM(w_up.shape, bf16),
            pltpu.VMEM(w_down.shape, bf16),
            pltpu.VMEM(keys.shape, bf16),
            pltpu.VMEM(values.shape, bf16),
            dma((5,)),
            dma((rows // 4,)),
            dma((rows // 4,)),
            pltpu.VMEM((rows, local_heads, head_dim), f32),
            pltpu.VMEM((rows, local_heads, cache_len), f32),
            pltpu.VMEM((rows, local_heads, head_dim), f32),
            pltpu.VMEM((rows, model), bf16),
            pltpu.VMEM((group_size, width, hidden_cols), bf16),
            pltpu.VMEM((group_size, width, hidden_cols), bf16),
            pltpu.VMEM((group_size, hidden_cols, width), bf16),
            pltpu.VMEM((rows, model), bf16),
            pltpu.VMEM((rows, model), bf16),
            pltpu.VMEM((rows, model), bf16),
            pltpu.VMEM((2, n, rows, half), bf16),
            pltpu.VMEM((teams, rows, 2 * hidden_cols), bf16),
            pltpu.VMEM((teams, rows, 2 * hidden_cols), bf16),
            pltpu.VMEM((n * rows // block, block, expert_hidden), bf16),
            pltpu.VMEM((teams, rows, hidden_cols), bf16),
            pltpu.VMEM((teams, rows, window), bf16),
            pltpu.VMEM((2, teams, rows, window), bf16),
            pltpu.VMEM((n, rows, half), bf16),
            pltpu.VMEM((n, rows, half), bf16),
            pltpu.VMEM((n, rows, half), bf16),
            pltpu.VMEM((n, rows, half), bf16),
            pltpu.VMEM((n, rows, half), bf16),
            dma((4,)),
            dma((2, group_size)),
            dma((2, group_size)),
            dma((2, group_size)),
            dma((2, n)),
            dma((2, n)),
            dma((2, teams)),
            dma((2, teams)),
            dma((teams,)),
            dma((2, teams)),
            dma((2, n)),
        ],
        compiler_params=pltpu.CompilerParams(
            collective_id=0, has_side_effects=True, vmem_limit_bytes=63 * 1024 * 1024
        ),
        name="whole_layer",
    )(*arrays)


def solution(mesh):
    return jax.shard_map(
        functools.partial(shards, mesh.shape["ep"]),
        mesh=mesh,
        in_specs=(
            P("ep", None),
            P("ep"),
            P(),
            P(None, "tp"),
            P(None, "tp"),
            P(None, "tp"),
            P("tp"),
            P("ep", "tp", None, None),
            P("ep", "tp", None, None),
            P("tp", None),
            P(),
            P(),
            P("ep", None),
            P("ep", "tp"),
            P("ep", "tp"),
            P("tp", "ep"),
            P(),
            P("ep", None, "tp"),
            P("ep", None, "tp"),
            P("ep", "tp", None),
        ),
        out_specs=(P("ep", "tp"), P("ep", "tp"), P("ep", "tp")),
        check_vma=False,
    )
```

```python
import functools

import jax
import jax.numpy as jnp
from jax import lax
from jax.experimental import pallas as pl
from jax.experimental.pallas import tpu as pltpu
from jax.sharding import PartitionSpec as P

MESH = pl.DeviceIdType.MESH


def whole_layer(
    n,
    group_size,
    tokens_ref,
    attn_gain_ref,
    lengths_ref,
    bias_ref,
    w_key_ref,
    w_value_ref,
    gain_ref,
    router_ref,
    routes_ref,
    mix_ref,
    dense_gate_ref,
    dense_up_ref,
    down_ref,
    w_query_hbm,
    w_out_hbm,
    w_gate_hbm,
    w_up_hbm,
    w_down_hbm,
    keys_hbm,
    values_hbm,
    out_ref,
    new_keys_ref,
    new_values_ref,
    w_query,
    w_out,
    w_gate,
    w_up,
    w_down,
    keys,
    values,
    load_sem,
    keys_sem,
    values_sem,
    query_ref,
    score_ref,
    read_ref,
    normed_ref,
    dense_gate_all,
    dense_up_all,
    down_all,
    attn_mine,
    attn_peer,
    res_ref,
    norm_all,
    part_send,
    part_recv,
    hidden_ref,
    dense_all,
    cols_send,
    cols_recv,
    other_ref,
    mine_ref,
    peer_ref,
    back_send,
    back_recv,
    pair_sems,
    dense_gate_sems,
    dense_up_sems,
    down_sems,
    norm_sems,
    pass_sems,
    part_sems,
    dense_sems,
    cols_send_sem,
    cols_recv_sem,
    back_sems,
):
    me = lax.axis_index("ep")
    core = lax.axis_index("tp")
    peer = 1 - core
    rows, model = tokens_ref.shape
    half = model // 2
    width = dense_gate_ref.shape[0]
    window = width * group_size
    place = me % group_size
    team = me // group_size
    teams = n // group_size
    first = team * window
    owner = first // half
    lane = pl.multiple_of(first % half, window)
    f32 = jnp.float32
    local_heads = bias_ref.shape[1]
    head_dim, cache_len = keys_hbm.shape[1:]
    span = 4

    def remote(source, target, send_sem, recv_sem, ep, tp):
        return pltpu.make_async_remote_copy(
            src_ref=source,
            dst_ref=target,
            send_sem=send_sem,
            recv_sem=recv_sem,
            device_id=(ep, tp),
            device_id_type=MESH,
        )

    pairs = (
        (w_query_hbm, w_query),
        (w_gate_hbm, w_gate),
        (w_up_hbm, w_up),
        (w_down_hbm, w_down),
        (w_out_hbm, w_out),
    )
    loads = [
        pltpu.make_async_copy(source, target, load_sem.at[i])
        for i, (source, target) in enumerate(pairs)
    ]

    def keys_load(c):
        block = pl.ds(c * span, span)
        return pltpu.make_async_copy(keys_hbm.at[block], keys.at[block], keys_sem.at[c])

    def values_load(c):
        block = pl.ds(c * span, span)
        return pltpu.make_async_copy(values_hbm.at[block], values.at[block], values_sem.at[c])

    loads[0].start()
    for c in range(rows // span):
        keys_load(c).start()
        values_load(c).start()
    for load in (loads[4], loads[1], loads[2], loads[3]):
        load.start()

    barrier = pltpu.get_barrier_semaphore()

    def greet(k, carry):
        other = lax.rem(me + k, n)
        pl.semaphore_signal(barrier, inc=1, device_id=(other, core), device_id_type=MESH)
        pl.semaphore_signal(barrier, inc=1, device_id=(other, peer), device_id_type=MESH)
        return carry

    lax.fori_loop(1, n, greet, 0)
    pl.semaphore_signal(barrier, inc=1, device_id=(me, peer), device_id_type=MESH)

    start = tokens_ref[...].astype(f32)
    normed_ref[...] = (
        start
        * lax.rsqrt(jnp.mean(start * start, axis=-1, keepdims=True) + 1e-06)
        * attn_gain_ref[...]
    ).astype(jnp.bfloat16)
    loads[0].wait()
    queries = jnp.dot(normed_ref[...], w_query[...], preferred_element_type=f32)
    queries = queries.astype(jnp.bfloat16).astype(f32)
    for h in range(local_heads):
        query_ref[:, h, :] = queries[:, h * head_dim : (h + 1) * head_dim]
    pl.semaphore_wait(barrier, 2 * n - 1)

    def team_copy(source, gathered, sems, origin, other):
        return remote(
            source,
            gathered.at[origin],
            sems.at[0, other],
            sems.at[1, origin],
            team * group_size + other,
            core,
        )

    def send_weights(k, carry):
        other = lax.rem(place + k, group_size)
        team_copy(dense_gate_ref, dense_gate_all, dense_gate_sems, place, other).start()
        team_copy(dense_up_ref, dense_up_all, dense_up_sems, place, other).start()
        team_copy(down_ref, down_all, down_sems, place, other).start()
        return carry

    lax.fori_loop(1, group_size, send_weights, 0)
    dense_gate_all[place] = dense_gate_ref[...]
    dense_up_all[place] = dense_up_ref[...]
    down_all[place] = down_ref[...]

    block_len = min(256, cache_len)
    after_mask = (
        lax.broadcasted_iota(jnp.int32, (block_len, block_len), 0)
        > lax.broadcasted_iota(jnp.int32, (block_len, block_len), 1)
    ).astype(jnp.bfloat16)
    position = lax.broadcasted_iota(jnp.int32, (span * local_heads, block_len), 1)

    head_row = lax.broadcasted_iota(jnp.int32, (local_heads, local_heads), 0)
    head_col = lax.broadcasted_iota(jnp.int32, (local_heads, local_heads), 1)
    bias = jnp.sum(jnp.where(head_row == head_col, bias_ref[...], 0.0), axis=1, keepdims=True)
    lines = span * local_heads
    line_seq = lax.broadcasted_iota(jnp.int32, (lines, rows), 0) // local_heads
    seq_lane = lax.broadcasted_iota(jnp.int32, (lines, rows), 1)
    lengths_row = lengths_ref[...].astype(f32)

    def attend(c, carry):
        keys_load(c).wait()
        for i in range(span):
            s = c * span + i
            score_ref[s] = (
                jnp.dot(query_ref[s].astype(jnp.bfloat16), keys[s], preferred_element_type=f32)
                * head_dim ** (-0.5)
                + bias
            )
        limits = jnp.sum(
            jnp.where(seq_lane == line_seq + c * span, lengths_row, 0.0), axis=1, keepdims=True
        ).astype(jnp.int32)
        later = jnp.zeros((lines, 1), f32)
        for first_pos in range(cache_len - block_len, -1, -block_len):
            columns = slice(first_pos, first_pos + block_len)
            scores = score_ref[pl.ds(c * span, span), :, columns].reshape(lines, block_len)
            visible = position + first_pos < limits
            keep = -(jnp.maximum(scores, 0.0) + jnp.log1p(jnp.exp(-jnp.abs(scores))))
            log_take = scores + keep
            keep = jnp.where(visible, keep, 0.0)
            top = keep.astype(jnp.bfloat16)
            rest = keep - top.astype(f32)
            middle = rest.astype(jnp.bfloat16)
            low = (rest - middle.astype(f32)).astype(jnp.bfloat16)
            sums = jnp.dot(
                jnp.concatenate([top, middle, low], axis=0),
                after_mask,
                preferred_element_type=f32,
            )
            after = sums[:lines] + sums[lines : 2 * lines] + sums[2 * lines :] + later
            later = later + jnp.sum(keep, axis=-1, keepdims=True)
            stick = jnp.where(visible, jnp.exp(log_take + after), 0.0)
            score_ref[pl.ds(c * span, span), :, columns] = stick.reshape(
                span, local_heads, block_len
            )
        values_load(c).wait()
        for i in range(span):
            s = c * span + i
            read_ref[s] = lax.dot_general(
                score_ref[s].astype(jnp.bfloat16),
                values[s],
                (((1,), (1,)), ((), ())),
                preferred_element_type=f32,
            )
        return carry

    lax.fori_loop(0, rows // span, attend, 0)
    heads_out = jnp.concatenate(
        [read_ref[:, h, :] for h in range(local_heads)], axis=1
    ).astype(jnp.bfloat16)
    loads[4].wait()
    attn_mine[...] = jnp.dot(heads_out, w_out[...], preferred_element_type=f32).astype(
        jnp.bfloat16
    )

    swap = remote(attn_mine, attn_peer, pair_sems.at[0], pair_sems.at[1], me, peer)
    swap.start()
    swap.wait()
    attn = attn_mine[...].astype(f32) + attn_peer[...].astype(f32)
    residual = (tokens_ref[...].astype(f32) + attn).astype(jnp.bfloat16)
    res_ref[...] = residual
    wide = residual.astype(f32)
    normed = (
        wide * lax.rsqrt(jnp.mean(wide * wide, axis=-1, keepdims=True) + 1e-06) * gain_ref[...]
    ).astype(jnp.bfloat16)
    norm_all[0, me] = normed[:, :half]
    norm_all[1, me] = normed[:, half:]

    def norm_copy(j, other):
        return remote(
            norm_all.at[core, j],
            norm_all.at[core, j],
            norm_sems.at[0, other],
            norm_sems.at[1, j],
            other,
            core,
        )

    def pass_copy(j, which):
        return remote(
            norm_all.at[which, j],
            norm_all.at[which, j],
            pass_sems.at[0, j],
            pass_sems.at[1, j],
            me,
            peer,
        )

    def send_norm(k, carry):
        norm_copy(me, lax.rem(me + k, n)).start()
        return carry

    lax.fori_loop(1, n, send_norm, 0)

    across = (((1,), (1,)), ((), ()))
    probs = jax.nn.sigmoid(
        lax.dot_general(router_ref[...], normed, across, preferred_element_type=f32)
    )
    expert_total = probs.shape[0]
    expert_row = lax.broadcasted_iota(jnp.int32, (expert_total, rows), 0)
    hits = jnp.zeros((expert_total, rows), f32)
    for k in range(routes_ref.shape[0]):
        hits = jnp.where(routes_ref[k : k + 1, :] == expert_row, 1.0, hits)
    picked = jnp.where(hits > 0.0, probs, 0.0)
    gates = (picked / jnp.sum(picked, axis=0, keepdims=True) * 2.5).T
    expert_index = lax.broadcasted_iota(jnp.int32, (rows, expert_total), 1)
    mix_gate = jax.nn.sigmoid(
        jnp.sum(normed.astype(f32) * mix_ref[...], axis=-1, keepdims=True)
    )

    for weight, target in ((w_key_ref, new_keys_ref), (w_value_ref, new_values_ref)):
        target[...] = lax.dot_general(
            normed_ref[...], weight[...], across, preferred_element_type=f32
        ).astype(jnp.bfloat16)

    def take_norm(k, carry):
        j = lax.rem(me + n - k, n)
        norm_copy(j, me).wait_recv()
        pass_copy(j, core).start()
        return carry

    lax.fori_loop(1, n, take_norm, 0)

    def take_pass(k, carry):
        pass_copy(lax.rem(me + n - k, n), peer).wait_recv()
        return carry

    lax.fori_loop(1, n, take_pass, 0)

    def part_copy(m, other):
        return remote(
            part_send.at[other],
            part_recv.at[m],
            part_sems.at[0, other],
            part_sems.at[1, m],
            other * group_size + place,
            core,
        )

    def back_copy(j, other):
        return remote(
            back_send.at[other],
            back_recv.at[j],
            back_sems.at[0, other],
            back_sems.at[1, j],
            other,
            core,
        )

    def dense_copy(m, other):
        return remote(
            dense_all.at[m],
            dense_all.at[m],
            dense_sems.at[0, other],
            dense_sems.at[1, m],
            other * group_size + place,
            core,
        )

    group = min(n, 16)
    groups = n // group
    block = group * rows

    def take_weights(k, carry):
        other = lax.rem(place + k, group_size)
        team_copy(dense_gate_ref, dense_gate_all, dense_gate_sems, other, place).wait_recv()
        team_copy(dense_up_ref, dense_up_all, dense_up_sems, other, place).wait_recv()
        team_copy(down_ref, down_all, down_sems, other, place).wait_recv()
        return carry

    lax.fori_loop(1, group_size, take_weights, 0)
    features = jnp.concatenate(
        [norm_all[owner, m * group_size + place, :, pl.ds(lane, window)] for m in range(teams)],
        axis=0,
    )
    hidden_cols = dense_gate_ref.shape[1]
    for gathered, columns in (
        (dense_gate_all, slice(0, hidden_cols)),
        (dense_up_all, slice(hidden_cols, 2 * hidden_cols)),
    ):
        value = jnp.dot(
            features, gathered[...].reshape(window, hidden_cols), preferred_element_type=f32
        )
        part_send[:, :, columns] = value.astype(jnp.bfloat16).reshape(teams, rows, hidden_cols)

    def send_part(k, carry):
        part_copy(team, lax.rem(team + k, teams)).start()
        return carry

    lax.fori_loop(1, teams, send_part, 0)

    loads[1].wait()
    loads[2].wait()

    def expert_first(c, carry):
        base = c * group
        low = norm_all[0, pl.ds(base, group)].reshape(block, half)
        high = norm_all[1, pl.ds(base, group)].reshape(block, half)
        gate_rows = jnp.dot(low, w_gate[:half], preferred_element_type=f32) + jnp.dot(
            high, w_gate[half:], preferred_element_type=f32
        )
        up_rows = jnp.dot(low, w_up[:half], preferred_element_type=f32) + jnp.dot(
            high, w_up[half:], preferred_element_type=f32
        )
        hidden_ref[pl.ds(c, 1)] = (jax.nn.silu(gate_rows) * up_rows).astype(jnp.bfloat16)[None]
        return carry

    lax.fori_loop(0, groups, expert_first, 0)

    def take_part(k, total):
        m = lax.rem(team + teams - k, teams)
        part_copy(m, team).wait_recv()
        return total + part_recv[m].astype(f32)

    paired = lax.fori_loop(1, teams, take_part, part_send[team].astype(f32))
    dense_all[team] = (jax.nn.silu(paired[:, :hidden_cols]) * paired[:, hidden_cols:]).astype(
        jnp.bfloat16
    )

    def send_dense(k, carry):
        dense_copy(team, lax.rem(team + k, teams)).start()
        return carry

    lax.fori_loop(1, teams, send_dense, 0)

    loads[3].wait()
    far = pl.ds(pl.multiple_of(peer * half, half), half)
    near = pl.ds(pl.multiple_of(core * half, half), half)

    def expert_far(c, carry):
        value = jnp.dot(hidden_ref[c], w_down[:, far], preferred_element_type=f32)
        other_ref[pl.ds(c * group, group)] = value.astype(jnp.bfloat16).reshape(group, rows, half)
        return carry

    lax.fori_loop(0, groups, expert_far, 0)
    trade = remote(other_ref, peer_ref, pair_sems.at[2], pair_sems.at[3], me, peer)
    trade.start()

    def expert_near(c, carry):
        value = jnp.dot(hidden_ref[c], w_down[:, near], preferred_element_type=f32)
        mine_ref[pl.ds(c * group, group)] = value.astype(jnp.bfloat16).reshape(group, rows, half)
        return carry

    lax.fori_loop(0, groups, expert_near, 0)
    trade.wait()

    def send_back(k, carry):
        other = lax.rem(me + k, n)
        total = mine_ref[other].astype(f32) + peer_ref[other].astype(f32)
        back_send[other] = total.astype(jnp.bfloat16)

        @pl.when(k > 0)
        def _():
            back_copy(me, other).start()

        return carry

    lax.fori_loop(0, n, send_back, 0)

    def take_dense(k, carry):
        dense_copy(lax.rem(team + teams - k, teams), team).wait_recv()
        return carry

    lax.fori_loop(1, teams, take_dense, 0)
    dense_rows = dense_all[...].reshape(teams * rows, hidden_cols)
    columns = [
        jnp.dot(dense_rows, down_all[q], preferred_element_type=f32) for q in range(group_size)
    ]
    cols_send[...] = (
        jnp.concatenate(columns, axis=1).astype(jnp.bfloat16).reshape(cols_send.shape)
    )

    def cols_copy(from_core, m, other, target):
        return remote(
            cols_send.at[other],
            cols_recv.at[from_core, m],
            cols_send_sem.at[other],
            cols_recv_sem.at[from_core, m],
            other * group_size + place,
            target,
        )

    def send_cols(k, carry):
        cols_copy(core, team, lax.rem(team + k, teams), owner).start()
        return carry

    lax.fori_loop(1, teams, send_cols, 0)

    @pl.when(owner == core)
    def _():
        cols_recv[core, team] = cols_send[team]

    @pl.when(owner != core)
    def _():
        cols_copy(core, team, team, peer).start()

    side = teams // 2

    def take_cols(k, carry):
        m = core * side + k

        @pl.when(m != team)
        def _():
            cols_copy(core, m, team, core).wait_recv()

        cols_copy(peer, m, team, core).wait_recv()
        return carry

    lax.fori_loop(0, side, take_cols, 0)
    dense = jnp.concatenate(
        [
            cols_recv[0, core * side + q].astype(f32) + cols_recv[1, core * side + q].astype(f32)
            for q in range(side)
        ],
        axis=1,
    )
    total = res_ref[:, near].astype(f32) + mix_gate * dense

    def take_back(k, total):
        j = lax.rem(me + n - k, n)

        @pl.when(k > 0)
        def _():
            back_copy(j, me).wait_recv()

        @pl.when(k == 0)
        def _():
            back_recv[me] = back_send[me]

        gate = jnp.sum(jnp.where(expert_index == j, gates, 0.0), axis=-1, keepdims=True)
        return total + gate * back_recv[j].astype(f32)

    out_ref[...] = lax.fori_loop(0, n, take_back, total).astype(jnp.bfloat16)

    def drain(k, carry):
        other = lax.rem(me + k, n)
        norm_copy(me, other).wait_send()
        pass_copy(other, core).wait_send()
        back_copy(me, other).wait_send()
        return carry

    lax.fori_loop(1, n, drain, 0)

    def drain_team(k, carry):
        other = lax.rem(place + k, group_size)
        team_copy(dense_gate_ref, dense_gate_all, dense_gate_sems, place, other).wait_send()
        team_copy(dense_up_ref, dense_up_all, dense_up_sems, place, other).wait_send()
        team_copy(down_ref, down_all, down_sems, place, other).wait_send()
        return carry

    lax.fori_loop(1, group_size, drain_team, 0)

    def drain_dense(k, carry):
        other = lax.rem(team + k, teams)
        part_copy(team, other).wait_send()
        dense_copy(team, other).wait_send()
        cols_copy(core, team, other, owner).wait_send()
        return carry

    lax.fori_loop(1, teams, drain_dense, 0)

    @pl.when(owner != core)
    def _():
        cols_copy(core, team, team, peer).wait_send()


def flip(place, k):
    result, bit = place, 1
    while bit <= k:
        if k & bit:
            result = result + bit * (1 - 2 * ((place // bit) % 2))
        bit *= 2
    return result


def finish(*refs):
    copies = [
        pltpu.make_async_copy(refs[i], refs[i + 3], refs[6].at[i]) for i in range(3)
    ]
    for copy in copies:
        copy.start()
    for copy in copies:
        copy.wait()


def routed_layer(
    n,
    inner,
    tokens_hbm,
    attn_gain_hbm,
    lengths_hbm,
    bias_hbm,
    w_key_hbm,
    w_value_hbm,
    gain_hbm,
    router_hbm,
    routes_hbm,
    mix_hbm,
    dense_gate_hbm,
    dense_up_hbm,
    down_hbm,
    w_query_hbm,
    w_out_hbm,
    w_gate_hbm,
    w_up_hbm,
    w_down_hbm,
    keys_hbm,
    values_hbm,
    out_ref,
    new_keys_ref,
    new_values_ref,
    tokens_ref,
    attn_gain_ref,
    lengths_ref,
    bias_ref,
    w_key_ref,
    w_value_ref,
    gain_ref,
    router_ref,
    routes_ref,
    mix_ref,
    dense_gate_ref,
    dense_up_ref,
    down_ref,
    w_query,
    w_out,
    w_gate,
    w_up,
    w_down,
    keys,
    values,
    query_ref,
    score_ref,
    read_ref,
    stick_ref,
    normed_ref,
    small_send,
    small,
    routes_all,
    hits_ref,
    attn_mine,
    attn_peer,
    res_ref,
    norm_all,
    first_send,
    first_recv,
    plane_send,
    plane_recv,
    far_recv,
    line_send,
    line_recv,
    load_sem,
    keys_sem,
    values_sem,
    pair_sems,
    swap_sems,
    small_send_sem,
    small_recv_sem,
    down_send_sem,
    down_recv_sem,
    routes_sems,
    line_sems,
    spread_sems,
    first_sems,
    plane_sems,
    far_sems,
    back_sems,
):
    me = lax.axis_index("ep")
    core = lax.axis_index("tp")
    peer = 1 - core
    f32, bf16 = jnp.float32, jnp.bfloat16
    rows, model = tokens_ref.shape
    half = model // 2
    width, hidden_cols = dense_gate_ref.shape
    units = hidden_cols // n
    outer = n // inner
    z, p = me // inner, me % inner
    side = n // 2
    owner, slot = me // side, me % side
    local_heads = bias_ref.shape[1]
    head_dim, cache_len = keys_hbm.shape[1:]
    hidden = w_gate_hbm.shape[1]
    expert_total = router_ref.shape[0]
    lanes = small.shape[0]
    router_at = 4 * units
    mix_at = router_at + expert_total
    span = rows // 2
    turns = list(range(outer - 1, 0, -1))
    around = turns[-2:]
    direct = [j for j in range(1, inner) if j & (j - 1) == 0]
    indirect = [j for j in range(1, inner) if j & (j - 1)]
    lines = span * local_heads

    def remote(source, target, send_sem, recv_sem, ep, tp):
        return pltpu.make_async_remote_copy(
            src_ref=source,
            dst_ref=target,
            send_sem=send_sem,
            recv_sem=recv_sem,
            device_id=(ep, tp),
            device_id_type=MESH,
        )

    near = pl.ds(pl.multiple_of(core * half, half), half)
    far = pl.ds(pl.multiple_of(peer * half, half), half)
    mine = pl.ds(pl.multiple_of(core * hidden, hidden), hidden)
    quarter = model // 4
    query_parts = [pl.ds(i * quarter, quarter) for i in range(4)]
    pairs = (
        (tokens_hbm, tokens_ref),
        (attn_gain_hbm, attn_gain_ref),
        (dense_gate_hbm, dense_gate_ref),
        (dense_up_hbm, dense_up_ref),
        (routes_hbm, routes_ref),
        *[(w_query_hbm.at[part], w_query.at[part]) for part in query_parts],
        (bias_hbm, bias_ref),
        (lengths_hbm, lengths_ref),
        (down_hbm, down_ref),
        (router_hbm, router_ref),
        (mix_hbm, mix_ref),
        (gain_hbm, gain_ref),
        (w_out_hbm, w_out),
        (w_key_hbm, w_key_ref),
        (w_value_hbm, w_value_ref),
        (w_gate_hbm.at[near, :], w_gate.at[:, mine]),
        (w_up_hbm.at[near, :], w_up.at[:, mine]),
        (w_down_hbm.at[:, near], w_down.at[mine, :]),
    )
    loads = [
        pltpu.make_async_copy(source, target, load_sem.at[i])
        for i, (source, target) in enumerate(pairs)
    ]
    load_of = {id(target): load for (_, target), load in zip(pairs, loads)}

    def arrived(*targets):
        for target in targets:
            load_of[id(target)].wait()

    def keys_load(c):
        block = pl.ds(c * span, span)
        return pltpu.make_async_copy(keys_hbm.at[block], keys.at[block], keys_sem.at[c])

    def values_load(c):
        block = pl.ds(c * span, span)
        return pltpu.make_async_copy(values_hbm.at[block], values.at[block], values_sem.at[c])

    for load in loads[:12]:
        load.start()

    barrier = pltpu.get_barrier_semaphore()

    def greet(k, carry):
        other = lax.rem(me + k, n)
        pl.semaphore_signal(barrier, inc=1, device_id=(other, core), device_id_type=MESH)
        pl.semaphore_signal(barrier, inc=1, device_id=(other, peer), device_id_type=MESH)
        return carry

    lax.fori_loop(1, n, greet, 0)
    pl.semaphore_signal(barrier, inc=1, device_id=(me, peer), device_id_type=MESH)

    arrived(tokens_ref, attn_gain_ref)
    start = tokens_ref[...].astype(f32)
    normed_ref[...] = (
        start
        * lax.rsqrt(jnp.mean(start * start, axis=-1, keepdims=True) + 1e-06)
        * attn_gain_ref[...]
    ).astype(bf16)
    for c in range(2):
        keys_load(c).start()
    arrived(dense_gate_ref, dense_up_ref, routes_ref)
    small_send[:, :units, :] = dense_gate_ref[...].T.reshape(n, units, width)
    small_send[:, units:, :] = dense_up_ref[...].T.reshape(n, units, width)
    top_k = routes_ref.shape[0]
    for k in range(top_k):
        routes_all[me, :, k * rows : (k + 1) * rows] = routes_ref[k : k + 1, :].astype(f32)

    queries = jnp.zeros((rows, w_query.shape[1]), f32)
    for i in range(4):
        loads[5 + i].wait()
        if i % 2:
            values_load(i // 2).start()
        part = slice(i * quarter, (i + 1) * quarter)
        queries = queries + jnp.dot(
            normed_ref[:, part], w_query[part, :], preferred_element_type=f32
        )
    queries = queries.astype(bf16).astype(f32)
    for h in range(local_heads):
        query_ref[:, h, :] = queries[:, h * head_dim : (h + 1) * head_dim]

    block_len = min(256, cache_len)
    after_mask = (
        lax.broadcasted_iota(jnp.int32, (block_len, block_len), 0)
        > lax.broadcasted_iota(jnp.int32, (block_len, block_len), 1)
    ).astype(bf16)
    position = lax.broadcasted_iota(jnp.int32, (lines, block_len), 1)
    arrived(bias_ref, lengths_ref)
    head_row = lax.broadcasted_iota(jnp.int32, (local_heads, local_heads), 0)
    head_col = lax.broadcasted_iota(jnp.int32, (local_heads, local_heads), 1)
    bias = jnp.sum(jnp.where(head_row == head_col, bias_ref[...], 0.0), axis=1, keepdims=True)
    line_seq = lax.broadcasted_iota(jnp.int32, (lines, rows), 0) // local_heads
    seq_lane = lax.broadcasted_iota(jnp.int32, (lines, rows), 1)
    lengths_row = lengths_ref[...].astype(f32)

    for s in range(rows):
        if s % span == 0:
            keys_load(s // span).wait()
            for load in loads[12:16] if s == 0 else loads[16:]:
                load.start()
        score_ref[s] = (
            jnp.dot(query_ref[s].astype(bf16), keys[s], preferred_element_type=f32)
            * head_dim ** (-0.5)
            + bias
        )

    def stick_breaking(c):
        limits = jnp.sum(
            jnp.where(seq_lane == line_seq + c * span, lengths_row, 0.0), axis=1, keepdims=True
        ).astype(jnp.int32)
        later = jnp.zeros((lines, 1), f32)
        for first_pos in range(cache_len - block_len, -1, -block_len):
            columns = slice(first_pos, first_pos + block_len)
            scores = score_ref[c * span : (c + 1) * span, :, columns].reshape(lines, block_len)
            visible = position + first_pos < limits
            keep = -(jnp.maximum(scores, 0.0) + jnp.log(1.0 + jnp.exp(-jnp.abs(scores))))
            log_take = scores + keep
            keep = jnp.where(visible, keep, 0.0)
            top = keep.astype(bf16)
            low = (keep - top.astype(f32)).astype(bf16)
            sums = jnp.dot(
                jnp.concatenate([top, low], axis=0), after_mask, preferred_element_type=f32
            )
            after = sums[:lines] + sums[lines:] + later
            later = later + jnp.sum(keep, axis=-1, keepdims=True)
            stick = jnp.where(visible, jnp.exp(log_take + after), 0.0)
            stick_ref[c, :, columns] = stick.astype(bf16)

    def read_values(c):
        mixed = lax.dot_general(
            values[c * span : (c + 1) * span].reshape(span * head_dim, cache_len),
            stick_ref[c],
            (((1,), (1,)), ((), ())),
            preferred_element_type=f32,
        ).reshape(span, head_dim, lines)
        seq_of = lax.broadcasted_iota(jnp.int32, (head_dim, lines), 1) // local_heads
        own_seq = jnp.zeros((head_dim, lines), f32)
        for s in range(span):
            own_seq = jnp.where(seq_of == s, mixed[s], own_seq)
        read_ref[c * span : (c + 1) * span] = own_seq.T.reshape(span, local_heads, head_dim)

    for c in range(2):
        stick_breaking(c)
    pl.semaphore_wait(barrier, 2 * n - 1)
    trades = [
        remote(
            w_gate_hbm.at[far, :], w_gate.at[:, mine], pair_sems.at[0, 0], pair_sems.at[1, 0], me, peer
        ),
        remote(
            w_up_hbm.at[far, :], w_up.at[:, mine], pair_sems.at[0, 1], pair_sems.at[1, 1], me, peer
        ),
        remote(
            w_down_hbm.at[:, far], w_down.at[mine, :], pair_sems.at[0, 2], pair_sems.at[1, 2], me, peer
        ),
    ]

    def small_copy(other, tp):
        return remote(
            small_send.at[other],
            small.at[pl.ds(core * 2 * units, 2 * units), pl.ds(pl.multiple_of(slot * width, width), width)],
            small_send_sem.at[other],
            small_recv_sem.at[core, slot],
            other,
            tp,
        )

    def down_copy(other, tp):
        return remote(
            down_ref.at[pl.ds(pl.multiple_of(other * units, units), units), :],
            w_down.at[
                pl.ds(2 * hidden + core * 2 * units, units),
                pl.ds(pl.multiple_of(slot * width, width), width),
            ],
            down_send_sem.at[other],
            down_recv_sem.at[core, slot],
            other,
            tp,
        )

    def routes_copy(origin, other):
        return remote(
            routes_all.at[origin],
            routes_all.at[origin],
            routes_sems.at[0, other],
            routes_sems.at[1, origin],
            other,
            core,
        )

    arrived(down_ref)

    def send_small(k, carry):
        other = lax.rem(me + k, n)
        routes_copy(me, other).start()
        small_copy(other, owner).start()
        return carry

    def send_down(k, carry):
        down_copy(lax.rem(me + k, n), owner).start()
        return carry

    lax.fori_loop(1, n, send_small, 0)

    @pl.when(owner == core)
    def _():
        here = pl.ds(pl.multiple_of(slot * width, width), width)
        small[pl.ds(pl.multiple_of(core * 2 * units, 2 * units), 2 * units), here] = small_send[me]
        w_down[
            pl.ds(pl.multiple_of(2 * hidden + core * 2 * units, units), units), here
        ] = down_ref[pl.ds(pl.multiple_of(me * units, units), units), :]

    @pl.when(owner != core)
    def _():
        small_copy(me, peer).start()

    for c in range(2):
        values_load(c).wait()
    for c in range(2):
        read_values(c)
    heads_out = jnp.concatenate([read_ref[:, h, :] for h in range(local_heads)], axis=1).astype(
        bf16
    )
    arrived(w_out)
    swaps = []
    for i in range(2):
        attn_mine[i] = jnp.dot(
            heads_out, w_out[:, i * half : (i + 1) * half], preferred_element_type=f32
        ).astype(bf16)
        swaps.append(
            remote(
                attn_mine.at[i], attn_peer.at[i], swap_sems.at[0, i], swap_sems.at[1, i], me, peer
            )
        )
        swaps[i].start()
    for trade in trades:
        trade.start()
    arrived(gain_ref)
    wide = []
    for i in range(2):
        swaps[i].wait_recv()
        columns = slice(i * half, (i + 1) * half)
        res_ref[i] = (
            tokens_ref[:, columns].astype(f32)
            + (attn_mine[i].astype(f32) + attn_peer[i].astype(f32))
        ).astype(bf16)
        wide.append(res_ref[i].astype(f32))
    squares = sum(jnp.sum(part * part, axis=-1, keepdims=True) for part in wide)
    scale = lax.rsqrt(squares / model + 1e-06)
    norm_all[me] = (
        jnp.where(core == 0, wide[0], wide[1])
        * scale
        * jnp.where(core == 0, gain_ref[:, :half], gain_ref[:, half:])
    ).astype(bf16)

    def line_copy(k):
        return remote(
            norm_all.at[me],
            norm_all.at[me],
            line_sems.at[0, k],
            line_sems.at[1, k],
            flip(z, k) * inner + p,
            core,
        )

    def spread_copy(k, j):
        origin = flip(z, k) * inner + p
        return remote(
            norm_all.at[origin],
            norm_all.at[origin],
            spread_sems.at[0, k, j],
            spread_sems.at[1, k, j],
            z * inner + flip(p, j),
            core,
        )

    def around_copy(k, j):
        origin = z * inner + flip(p, j)
        return remote(
            norm_all.at[origin],
            norm_all.at[origin],
            spread_sems.at[0, k, j],
            spread_sems.at[1, k, j],
            flip(z, k) * inner + p,
            core,
        )

    for k in turns:
        line_copy(k).start()
    for j in indirect + direct:
        spread_copy(0, j).start()


    lax.fori_loop(1, n, send_down, 0)

    @pl.when(owner != core)
    def _():
        down_copy(me, peer).start()

    across = (((1,), (1,)), ((), ()))
    arrived(w_key_ref, w_value_ref)
    for weight, target in ((w_key_ref, new_keys_ref), (w_value_ref, new_values_ref)):
        target[...] = lax.dot_general(
            normed_ref[...], weight[...], across, preferred_element_type=f32
        ).astype(bf16)

    def small_taken(tp, k):
        return remote(
            small_send.at[0],
            small.at[
                pl.ds(tp * 2 * units, 2 * units), pl.ds(pl.multiple_of(k * width, width), width)
            ],
            small_send_sem.at[0],
            small_recv_sem.at[tp, k],
            me,
            peer,
        )

    def down_taken(tp, k):
        return remote(
            down_ref.at[pl.ds(0, units), :],
            w_down.at[
                pl.ds(2 * hidden + tp * 2 * units, units),
                pl.ds(pl.multiple_of(k * width, width), width),
            ],
            down_send_sem.at[0],
            down_recv_sem.at[tp, k],
            me,
            peer,
        )

    def take_all(taken):
        def take(k, carry):
            @pl.when(core * side + k != me)
            def _():
                taken(core, k).wait_recv()

            taken(peer, k).wait_recv()
            return carry

        lax.fori_loop(0, side, take, 0)

    arrived(router_ref, mix_ref)
    spread_rows = lanes - mix_at
    mix_row = mix_ref[...]
    mix_top = mix_row.astype(bf16)
    mix_rest = mix_row - mix_top.astype(f32)
    mix_mid = mix_rest.astype(bf16)
    mix_low = (mix_rest - mix_mid.astype(f32)).astype(bf16)
    mix_index = lax.broadcasted_iota(jnp.int32, (spread_rows, model), 0)
    mix_rows = jnp.where(
        mix_index == 0,
        mix_top.astype(f32),
        jnp.where(
            mix_index == 1,
            mix_mid.astype(f32),
            jnp.where(mix_index == 2, mix_low.astype(f32), 0.0),
        ),
    ).astype(bf16)
    small[pl.ds(router_at, expert_total), :] = jnp.where(
        core == 0, router_ref[:, :half], router_ref[:, half:]
    )
    small[pl.ds(mix_at, spread_rows), :] = jnp.where(
        core == 0, mix_rows[:, :half], mix_rows[:, half:]
    )
    for base in (units, 3 * units):
        w_down[pl.ds(2 * hidden + base, units), :] = jnp.zeros((units, half), bf16)
    tail = lanes - 4 * units
    w_down[pl.ds(2 * hidden + 4 * units, tail), :] = jnp.zeros((tail, half), bf16)

    for k in turns:
        line_copy(k).wait_recv()
        for j in direct if k in around else indirect + direct:
            spread_copy(k, j).start()
        if k == turns[0]:
            for j in indirect:
                spread_copy(0, j).wait_recv()
                for m in around:
                    around_copy(m, j).start()
    take_all(small_taken)

    arrived(*[target for _, target in pairs[18:]])
    for trade in trades:
        trade.wait_recv()

    chunk = inner * rows
    lane = lax.broadcasted_iota(jnp.int32, (chunk, lanes), 1)
    dense_lane = (lane < units) | ((lane >= 2 * units) & (lane < 3 * units))

    rest_at = 2 * hidden + lanes

    def first_copy(k):
        return remote(
            first_send.at[k], first_recv.at[k], first_sems.at[0, k], first_sems.at[1, k], me, peer
        )

    def group(k):
        return pl.ds(pl.multiple_of(flip(z, k) * inner, inner), inner)

    def first(*ks):
        for k in ks:
            for j in range(1, inner) if k else direct:
                spread_copy(k, j).wait_recv()
        x = jnp.concatenate([norm_all[group(k)].reshape(chunk, half) for k in ks], axis=0)
        gate_rows = jnp.dot(x, w_gate[...], preferred_element_type=f32)
        rest = lax.dot_general(x, small[...], across, preferred_element_type=f32)
        up_rows = jnp.dot(x, w_up[...], preferred_element_type=f32)
        for i, k in enumerate(ks):
            own_rows = slice(i * chunk, (i + 1) * chunk)
            first_send[k, :, : 2 * hidden] = gate_rows[own_rows]
            first_send[k, :, 2 * hidden : rest_at] = rest[own_rows]
            first_send[k, :, rest_at:] = up_rows[own_rows]
        for k in ks:
            first_copy(k).start()

    def plane_copy(k, j):
        other = flip(p, j)
        return remote(
            plane_send.at[k, other],
            plane_recv.at[k, j],
            plane_sems.at[0, k, j],
            plane_sems.at[1, k, j],
            z * inner + other,
            core,
        )

    def far_copy(k, j):
        return remote(
            plane_send.at[k, flip(p, j)],
            far_recv.at[k, j],
            far_sems.at[0, k, j],
            far_sems.at[1, k, j],
            flip(z, k) * inner + p,
            core,
        )

    def send_plane(k):
        for j in indirect:
            if k in turns[:-1]:
                far_copy(k, j).start()
            elif k:
                plane_copy(k, j).start()
        for j in direct:
            plane_copy(k, j).start()

    def activations(k):
        gate_rows = first_send[k, :, : 2 * hidden] + first_recv[k, :, : 2 * hidden]
        up_rows = first_send[k, :, rest_at:] + first_recv[k, :, rest_at:]
        rest = first_send[k, :, 2 * hidden : rest_at] + first_recv[k, :, 2 * hidden : rest_at]
        chosen = hits_ref[group(k)].reshape(chunk, lanes)
        picked = jnp.where(chosen > 0.0, jax.nn.sigmoid(rest), 0.0)
        total = jnp.sum(picked, axis=-1, keepdims=True)
        own = jnp.sum(jnp.where(lane == router_at + me, picked, 0.0), axis=-1, keepdims=True)
        gate = own / total * 2.5
        mix_sum = jnp.sum(jnp.where(lane >= mix_at, rest, 0.0), axis=-1, keepdims=True)
        mix_gate = jax.nn.sigmoid(mix_sum)
        dense = jax.nn.silu(rest) * pltpu.roll(rest, lanes - units, 1) * mix_gate
        dense = jnp.where(dense_lane, dense, 0.0).astype(bf16)
        return (jax.nn.silu(gate_rows) * up_rows * gate).astype(bf16), dense

    def second(*ks):
        for k in ks:
            first_copy(k).wait_recv()
        parts = [activations(k) for k in ks]
        act = jnp.concatenate([part[0] for part in parts], axis=0)
        dense = jnp.concatenate([part[1] for part in parts], axis=0)
        value = jnp.dot(act, w_down[: 2 * hidden], preferred_element_type=f32) + jnp.dot(
            dense, w_down[2 * hidden :], preferred_element_type=f32
        )
        for i, k in enumerate(ks):
            own_rows = value[i * chunk : (i + 1) * chunk]
            plane_send[k] = own_rows.astype(bf16).reshape(inner, rows, half)
        for k in ks:
            send_plane(k)

    def far_home(j):
        return remote(
            far_recv.at[0, j],
            plane_recv.at[0, j],
            plane_sems.at[0, 0, j],
            plane_sems.at[1, 0, j],
            z * inner + flip(p, j),
            core,
        )

    def back_copy(k):
        return remote(
            line_send.at[k],
            line_recv.at[k],
            back_sems.at[0, k],
            back_sems.at[1, k],
            flip(z, k) * inner + p,
            core,
        )

    def collect(k):
        total = plane_send[k, p].astype(f32)
        for j in direct + (indirect if k == turns[-1] else []):
            plane_copy(k, j).wait_recv()
            total = total + plane_recv[k, j].astype(f32)
        return total

    def third(k):
        line_send[k] = collect(k).astype(bf16)
        back_copy(k).start()

    first(0)
    def take_routes(k, carry):
        routes_copy(lax.rem(me + n - k, n), me).wait_recv()
        return carry

    lax.fori_loop(1, n, take_routes, 0)
    row_lane = (lax.broadcasted_iota(jnp.int32, (rows, lanes), 1) - router_at).astype(f32)
    named = routes_all[...].reshape(n, lanes).T
    for j in range(n):
        hit = jnp.zeros((rows, lanes), f32)
        for c in range(top_k):
            hit = jnp.where(named[c * rows : (c + 1) * rows, j : j + 1] == row_lane, 1.0, hit)
        hits_ref[j] = hit

    take_all(down_taken)
    second(0)
    first(turns[0])
    for k in turns[1:]:
        first(k)
    for k in turns:
        second(k)
    for k in turns[:-1]:
        third(k)
    for j in indirect:
        other = flip(p, j)
        total = plane_send[0, other].astype(f32)
        for k in turns[:-1]:
            far_copy(k, j).wait_recv()
            total = total + far_recv[k, j].astype(f32)
        far_recv[0, j] = total.astype(bf16)
        far_home(j).start()
    third(turns[-1])
    total = res_ref[core].astype(f32) + collect(0)
    for k in turns:
        back_copy(k).wait_recv()
        total = total + line_recv[k].astype(f32)
    for j in indirect:
        far_home(j).wait_recv()
        total = total + plane_recv[0, j].astype(f32)
    out_ref[...] = total.astype(bf16)

    def drain(k, carry):
        other = lax.rem(me + k, n)
        small_copy(other, owner).wait_send()
        down_copy(other, owner).wait_send()
        routes_copy(me, other).wait_send()
        return carry

    lax.fori_loop(1, n, drain, 0)

    @pl.when(owner != core)
    def _():
        small_copy(me, peer).wait_send()
        down_copy(me, peer).wait_send()

    for copy in trades + swaps:
        copy.wait_send()
    for k in range(outer):
        if k:
            line_copy(k).wait_send()
            back_copy(k).wait_send()
        first_copy(k).wait_send()
        for j in range(1, inner):
            (around_copy if k in around and j in indirect else spread_copy)(k, j).wait_send()
            (far_copy if k in turns[:-1] and j in indirect else plane_copy)(k, j).wait_send()


def routed_shards(n, inner, arrays):
    tokens = arrays[0]
    w_key, head_bias = arrays[4], arrays[3]
    keys, w_gate, w_down = arrays[18], arrays[15], arrays[17]
    rows, model = tokens.shape
    half = model // 2
    width, hidden_cols = arrays[10].shape
    units = hidden_cols // n
    outer = n // inner
    seq_count, head_dim, cache_len = keys.shape
    local_heads = head_bias.shape[1]
    hidden = w_gate.shape[1]
    lanes = 128
    chunk = inner * rows
    bf16, f32 = jnp.bfloat16, jnp.float32
    vmem = pl.BlockSpec(memory_space=pltpu.VMEM)
    anywhere = pl.BlockSpec(memory_space=pltpu.HBM)
    dma = pltpu.SemaphoreType.DMA
    small_inputs = [pltpu.VMEM(a.shape, a.dtype) for a in arrays[:15]]
    results = pl.pallas_call(
        functools.partial(routed_layer, n, inner),
        out_shape=(
            jax.ShapeDtypeStruct((rows, half), bf16),
            jax.ShapeDtypeStruct((rows, w_key.shape[0]), bf16),
            jax.ShapeDtypeStruct((rows, w_key.shape[0]), bf16),
        ),
        in_specs=[anywhere] * 20,
        out_specs=(vmem, vmem, vmem),
        scratch_shapes=small_inputs
        + [
            pltpu.VMEM((half, 2 * hidden), bf16),
            pltpu.VMEM((half, 2 * hidden), bf16),
            pltpu.VMEM((2 * hidden + lanes, half), bf16),
            pltpu.VMEM(keys.shape, bf16),
            pltpu.VMEM(keys.shape, bf16),
            pltpu.VMEM((rows, local_heads, head_dim), f32),
            pltpu.VMEM((rows, local_heads, cache_len), f32),
            pltpu.VMEM((rows, local_heads, head_dim), f32),
            pltpu.VMEM((2, rows * local_heads // 2, cache_len), bf16),
            pltpu.VMEM((rows, model), bf16),
            pltpu.VMEM((n, 2 * units, width), bf16),
            pltpu.VMEM((lanes, half), bf16),
            pltpu.VMEM((n, 1, lanes), f32),
            pltpu.VMEM((n, rows, lanes), f32),
            pltpu.VMEM((2, rows, half), bf16),
            pltpu.VMEM((2, rows, half), bf16),
            pltpu.VMEM((2, rows, half), bf16),
            pltpu.VMEM((n, rows, half), bf16),
            pltpu.VMEM((outer, chunk, 4 * hidden + lanes), f32),
            pltpu.VMEM((outer, chunk, 4 * hidden + lanes), f32),
            pltpu.VMEM((outer, inner, rows, half), bf16),
            pltpu.VMEM((outer, inner, rows, half), bf16),
            pltpu.VMEM((outer, inner, rows, half), bf16),
            pltpu.VMEM((outer, rows, half), bf16),
            pltpu.VMEM((outer, rows, half), bf16),
            dma((21,)),
            dma((2,)),
            dma((2,)),
            dma((2, 3)),
            dma((2, 2)),
            dma((n,)),
            dma((2, n // 2)),
            dma((n,)),
            dma((2, n // 2)),
            dma((2, n)),
            dma((2, outer)),
            dma((2, outer, inner)),
            dma((2, outer)),
            dma((2, outer, inner)),
            dma((2, outer, inner)),
            dma((2, outer)),
        ],
        compiler_params=pltpu.CompilerParams(
            collective_id=0, has_side_effects=True, vmem_limit_bytes=48 * 1024 * 1024
        ),
        name="routed_layer",
    )(*[pltpu.with_memory_space_constraint(a, pltpu.HBM) for a in arrays])
    return pl.pallas_call(
        finish,
        out_shape=tuple(jax.ShapeDtypeStruct(r.shape, r.dtype) for r in results),
        in_specs=[vmem] * 3,
        out_specs=(anywhere,) * 3,
        scratch_shapes=[dma((3,))],
        name="finish",
    )(*[pltpu.with_memory_space_constraint(r, pltpu.VMEM) for r in results])


def shards(
    n,
    tokens,
    lengths,
    attn_gain,
    w_query,
    w_key,
    w_value,
    head_bias,
    key_cache,
    value_cache,
    w_attn_out,
    ffn_gain,
    w_router,
    routes,
    w_dense_gate,
    w_dense_up,
    w_dense_down,
    dense_mix,
    w_expert_gate,
    w_expert_up,
    w_expert_down,
):
    rows, model = tokens.shape
    half = model // 2
    width, hidden_cols = w_dense_gate.shape
    group_size = min(n, max(4, 128 // width))
    teams = n // group_size
    window = width * group_size
    seq_count, local_kv, head_dim, cache_len = key_cache.shape
    local_heads = head_bias.shape[0]
    keys = key_cache.reshape(seq_count, head_dim, cache_len)
    values = value_cache.reshape(seq_count, head_dim, cache_len)
    w_gate, w_up, w_down = w_expert_gate[0], w_expert_up[0], w_expert_down[0]
    expert_hidden = w_gate.shape[1]
    arrays = (
        tokens,
        attn_gain.reshape(1, model),
        lengths.reshape(1, seq_count),
        head_bias.reshape(1, local_heads),
        w_key.T,
        w_value.T,
        ffn_gain.reshape(1, model),
        w_router.T,
        routes.T,
        dense_mix.reshape(1, model),
        w_dense_gate,
        w_dense_up,
        w_dense_down,
        w_query,
        w_attn_out,
        w_gate,
        w_up,
        w_down,
        keys,
        values,
    )
    inner = 1
    while (2 * inner) ** 2 <= n:
        inner *= 2
    small_rows = 4 * (hidden_cols // n) + w_router.shape[1]
    if hidden_cols % (16 * n) == 0 and width % 128 == 0 and small_rows <= 112:
        return routed_shards(n, inner, arrays)
    bf16, f32 = jnp.bfloat16, jnp.float32
    block = min(n, 16) * rows
    vmem = pl.BlockSpec(memory_space=pltpu.VMEM)
    anywhere = pl.BlockSpec(memory_space=pltpu.HBM)
    dma = pltpu.SemaphoreType.DMA
    return pl.pallas_call(
        functools.partial(whole_layer, n, group_size),
        out_shape=(
            jax.ShapeDtypeStruct((rows, half), bf16),
            jax.ShapeDtypeStruct((rows, w_key.shape[1]), bf16),
            jax.ShapeDtypeStruct((rows, w_value.shape[1]), bf16),
        ),
        in_specs=[vmem] * 13 + [anywhere] * 7,
        out_specs=(vmem, vmem, vmem),
        scratch_shapes=[
            pltpu.VMEM(w_query.shape, bf16),
            pltpu.VMEM(w_attn_out.shape, bf16),
            pltpu.VMEM(w_gate.shape, bf16),
            pltpu.VMEM(w_up.shape, bf16),
            pltpu.VMEM(w_down.shape, bf16),
            pltpu.VMEM(keys.shape, bf16),
            pltpu.VMEM(values.shape, bf16),
            dma((5,)),
            dma((rows // 4,)),
            dma((rows // 4,)),
            pltpu.VMEM((rows, local_heads, head_dim), f32),
            pltpu.VMEM((rows, local_heads, cache_len), f32),
            pltpu.VMEM((rows, local_heads, head_dim), f32),
            pltpu.VMEM((rows, model), bf16),
            pltpu.VMEM((group_size, width, hidden_cols), bf16),
            pltpu.VMEM((group_size, width, hidden_cols), bf16),
            pltpu.VMEM((group_size, hidden_cols, width), bf16),
            pltpu.VMEM((rows, model), bf16),
            pltpu.VMEM((rows, model), bf16),
            pltpu.VMEM((rows, model), bf16),
            pltpu.VMEM((2, n, rows, half), bf16),
            pltpu.VMEM((teams, rows, 2 * hidden_cols), bf16),
            pltpu.VMEM((teams, rows, 2 * hidden_cols), bf16),
            pltpu.VMEM((n * rows // block, block, expert_hidden), bf16),
            pltpu.VMEM((teams, rows, hidden_cols), bf16),
            pltpu.VMEM((teams, rows, window), bf16),
            pltpu.VMEM((2, teams, rows, window), bf16),
            pltpu.VMEM((n, rows, half), bf16),
            pltpu.VMEM((n, rows, half), bf16),
            pltpu.VMEM((n, rows, half), bf16),
            pltpu.VMEM((n, rows, half), bf16),
            pltpu.VMEM((n, rows, half), bf16),
            dma((4,)),
            dma((2, group_size)),
            dma((2, group_size)),
            dma((2, group_size)),
            dma((2, n)),
            dma((2, n)),
            dma((2, teams)),
            dma((2, teams)),
            dma((teams,)),
            dma((2, teams)),
            dma((2, n)),
        ],
        compiler_params=pltpu.CompilerParams(
            collective_id=0, has_side_effects=True, vmem_limit_bytes=63 * 1024 * 1024
        ),
        name="whole_layer",
    )(*arrays)


def solution(mesh):
    return jax.shard_map(
        functools.partial(shards, mesh.shape["ep"]),
        mesh=mesh,
        in_specs=(
            P("ep", None),
            P("ep"),
            P(),
            P(None, "tp"),
            P(None, "tp"),
            P(None, "tp"),
            P("tp"),
            P("ep", "tp", None, None),
            P("ep", "tp", None, None),
            P("tp", None),
            P(),
            P(),
            P("ep", None),
            P("ep", "tp"),
            P("ep", "tp"),
            P("tp", "ep"),
            P(),
            P("ep", None, "tp"),
            P("ep", None, "tp"),
            P("ep", "tp", None),
        ),
        out_specs=(P("ep", "tp"), P("ep", "tp"), P("ep", "tp")),
        check_vma=False,
    )
```

```python
import functools

import jax
import jax.numpy as jnp
from jax import lax
from jax.experimental import pallas as pl
from jax.experimental.pallas import tpu as pltpu
from jax.sharding import PartitionSpec as P

MESH = pl.DeviceIdType.MESH


def whole_layer(
    n,
    group_size,
    tokens_ref,
    attn_gain_ref,
    lengths_ref,
    bias_ref,
    w_key_ref,
    w_value_ref,
    gain_ref,
    router_ref,
    routes_ref,
    mix_ref,
    dense_gate_ref,
    dense_up_ref,
    down_ref,
    w_query_hbm,
    w_out_hbm,
    w_gate_hbm,
    w_up_hbm,
    w_down_hbm,
    keys_hbm,
    values_hbm,
    out_ref,
    new_keys_ref,
    new_values_ref,
    w_query,
    w_out,
    w_gate,
    w_up,
    w_down,
    keys,
    values,
    load_sem,
    keys_sem,
    values_sem,
    query_ref,
    score_ref,
    read_ref,
    normed_ref,
    dense_gate_all,
    dense_up_all,
    down_all,
    attn_mine,
    attn_peer,
    res_ref,
    norm_all,
    part_send,
    part_recv,
    hidden_ref,
    dense_all,
    cols_send,
    cols_recv,
    other_ref,
    mine_ref,
    peer_ref,
    back_send,
    back_recv,
    pair_sems,
    dense_gate_sems,
    dense_up_sems,
    down_sems,
    norm_sems,
    pass_sems,
    part_sems,
    dense_sems,
    cols_send_sem,
    cols_recv_sem,
    back_sems,
):
    me = lax.axis_index("ep")
    core = lax.axis_index("tp")
    peer = 1 - core
    rows, model = tokens_ref.shape
    half = model // 2
    width = dense_gate_ref.shape[0]
    window = width * group_size
    place = me % group_size
    team = me // group_size
    teams = n // group_size
    first = team * window
    owner = first // half
    lane = pl.multiple_of(first % half, window)
    f32 = jnp.float32
    local_heads = bias_ref.shape[1]
    head_dim, cache_len = keys_hbm.shape[1:]
    span = 4

    def remote(source, target, send_sem, recv_sem, ep, tp):
        return pltpu.make_async_remote_copy(
            src_ref=source,
            dst_ref=target,
            send_sem=send_sem,
            recv_sem=recv_sem,
            device_id=(ep, tp),
            device_id_type=MESH,
        )

    pairs = (
        (w_query_hbm, w_query),
        (w_gate_hbm, w_gate),
        (w_up_hbm, w_up),
        (w_down_hbm, w_down),
        (w_out_hbm, w_out),
    )
    loads = [
        pltpu.make_async_copy(source, target, load_sem.at[i])
        for i, (source, target) in enumerate(pairs)
    ]

    def keys_load(c):
        block = pl.ds(c * span, span)
        return pltpu.make_async_copy(keys_hbm.at[block], keys.at[block], keys_sem.at[c])

    def values_load(c):
        block = pl.ds(c * span, span)
        return pltpu.make_async_copy(values_hbm.at[block], values.at[block], values_sem.at[c])

    loads[0].start()
    for c in range(rows // span):
        keys_load(c).start()
        values_load(c).start()
    for load in (loads[4], loads[1], loads[2], loads[3]):
        load.start()

    barrier = pltpu.get_barrier_semaphore()

    def greet(k, carry):
        other = lax.rem(me + k, n)
        pl.semaphore_signal(barrier, inc=1, device_id=(other, core), device_id_type=MESH)
        pl.semaphore_signal(barrier, inc=1, device_id=(other, peer), device_id_type=MESH)
        return carry

    lax.fori_loop(1, n, greet, 0)
    pl.semaphore_signal(barrier, inc=1, device_id=(me, peer), device_id_type=MESH)

    start = tokens_ref[...].astype(f32)
    normed_ref[...] = (
        start
        * lax.rsqrt(jnp.mean(start * start, axis=-1, keepdims=True) + 1e-06)
        * attn_gain_ref[...]
    ).astype(jnp.bfloat16)
    loads[0].wait()
    queries = jnp.dot(normed_ref[...], w_query[...], preferred_element_type=f32)
    queries = queries.astype(jnp.bfloat16).astype(f32)
    for h in range(local_heads):
        query_ref[:, h, :] = queries[:, h * head_dim : (h + 1) * head_dim]
    pl.semaphore_wait(barrier, 2 * n - 1)

    def team_copy(source, gathered, sems, origin, other):
        return remote(
            source,
            gathered.at[origin],
            sems.at[0, other],
            sems.at[1, origin],
            team * group_size + other,
            core,
        )

    def send_weights(k, carry):
        other = lax.rem(place + k, group_size)
        team_copy(dense_gate_ref, dense_gate_all, dense_gate_sems, place, other).start()
        team_copy(dense_up_ref, dense_up_all, dense_up_sems, place, other).start()
        team_copy(down_ref, down_all, down_sems, place, other).start()
        return carry

    lax.fori_loop(1, group_size, send_weights, 0)
    dense_gate_all[place] = dense_gate_ref[...]
    dense_up_all[place] = dense_up_ref[...]
    down_all[place] = down_ref[...]

    block_len = min(256, cache_len)
    after_mask = (
        lax.broadcasted_iota(jnp.int32, (block_len, block_len), 0)
        > lax.broadcasted_iota(jnp.int32, (block_len, block_len), 1)
    ).astype(jnp.bfloat16)
    position = lax.broadcasted_iota(jnp.int32, (span * local_heads, block_len), 1)

    head_row = lax.broadcasted_iota(jnp.int32, (local_heads, local_heads), 0)
    head_col = lax.broadcasted_iota(jnp.int32, (local_heads, local_heads), 1)
    bias = jnp.sum(jnp.where(head_row == head_col, bias_ref[...], 0.0), axis=1, keepdims=True)
    lines = span * local_heads
    line_seq = lax.broadcasted_iota(jnp.int32, (lines, rows), 0) // local_heads
    seq_lane = lax.broadcasted_iota(jnp.int32, (lines, rows), 1)
    lengths_row = lengths_ref[...].astype(f32)

    def attend(c, carry):
        keys_load(c).wait()
        for i in range(span):
            s = c * span + i
            score_ref[s] = (
                jnp.dot(query_ref[s].astype(jnp.bfloat16), keys[s], preferred_element_type=f32)
                * head_dim ** (-0.5)
                + bias
            )
        limits = jnp.sum(
            jnp.where(seq_lane == line_seq + c * span, lengths_row, 0.0), axis=1, keepdims=True
        ).astype(jnp.int32)
        later = jnp.zeros((lines, 1), f32)
        for first_pos in range(cache_len - block_len, -1, -block_len):
            columns = slice(first_pos, first_pos + block_len)
            scores = score_ref[pl.ds(c * span, span), :, columns].reshape(lines, block_len)
            visible = position + first_pos < limits
            keep = -(jnp.maximum(scores, 0.0) + jnp.log1p(jnp.exp(-jnp.abs(scores))))
            log_take = scores + keep
            keep = jnp.where(visible, keep, 0.0)
            top = keep.astype(jnp.bfloat16)
            rest = keep - top.astype(f32)
            middle = rest.astype(jnp.bfloat16)
            low = (rest - middle.astype(f32)).astype(jnp.bfloat16)
            sums = jnp.dot(
                jnp.concatenate([top, middle, low], axis=0),
                after_mask,
                preferred_element_type=f32,
            )
            after = sums[:lines] + sums[lines : 2 * lines] + sums[2 * lines :] + later
            later = later + jnp.sum(keep, axis=-1, keepdims=True)
            stick = jnp.where(visible, jnp.exp(log_take + after), 0.0)
            score_ref[pl.ds(c * span, span), :, columns] = stick.reshape(
                span, local_heads, block_len
            )
        values_load(c).wait()
        for i in range(span):
            s = c * span + i
            read_ref[s] = lax.dot_general(
                score_ref[s].astype(jnp.bfloat16),
                values[s],
                (((1,), (1,)), ((), ())),
                preferred_element_type=f32,
            )
        return carry

    lax.fori_loop(0, rows // span, attend, 0)
    heads_out = jnp.concatenate(
        [read_ref[:, h, :] for h in range(local_heads)], axis=1
    ).astype(jnp.bfloat16)
    loads[4].wait()
    attn_mine[...] = jnp.dot(heads_out, w_out[...], preferred_element_type=f32).astype(
        jnp.bfloat16
    )

    swap = remote(attn_mine, attn_peer, pair_sems.at[0], pair_sems.at[1], me, peer)
    swap.start()
    swap.wait()
    attn = attn_mine[...].astype(f32) + attn_peer[...].astype(f32)
    residual = (tokens_ref[...].astype(f32) + attn).astype(jnp.bfloat16)
    res_ref[...] = residual
    wide = residual.astype(f32)
    normed = (
        wide * lax.rsqrt(jnp.mean(wide * wide, axis=-1, keepdims=True) + 1e-06) * gain_ref[...]
    ).astype(jnp.bfloat16)
    norm_all[0, me] = normed[:, :half]
    norm_all[1, me] = normed[:, half:]

    def norm_copy(j, other):
        return remote(
            norm_all.at[core, j],
            norm_all.at[core, j],
            norm_sems.at[0, other],
            norm_sems.at[1, j],
            other,
            core,
        )

    def pass_copy(j, which):
        return remote(
            norm_all.at[which, j],
            norm_all.at[which, j],
            pass_sems.at[0, j],
            pass_sems.at[1, j],
            me,
            peer,
        )

    def send_norm(k, carry):
        norm_copy(me, lax.rem(me + k, n)).start()
        return carry

    lax.fori_loop(1, n, send_norm, 0)

    across = (((1,), (1,)), ((), ()))
    probs = jax.nn.sigmoid(
        lax.dot_general(router_ref[...], normed, across, preferred_element_type=f32)
    )
    expert_total = probs.shape[0]
    expert_row = lax.broadcasted_iota(jnp.int32, (expert_total, rows), 0)
    hits = jnp.zeros((expert_total, rows), f32)
    for k in range(routes_ref.shape[0]):
        hits = jnp.where(routes_ref[k : k + 1, :] == expert_row, 1.0, hits)
    picked = jnp.where(hits > 0.0, probs, 0.0)
    gates = (picked / jnp.sum(picked, axis=0, keepdims=True) * 2.5).T
    expert_index = lax.broadcasted_iota(jnp.int32, (rows, expert_total), 1)
    mix_gate = jax.nn.sigmoid(
        jnp.sum(normed.astype(f32) * mix_ref[...], axis=-1, keepdims=True)
    )

    for weight, target in ((w_key_ref, new_keys_ref), (w_value_ref, new_values_ref)):
        target[...] = lax.dot_general(
            normed_ref[...], weight[...], across, preferred_element_type=f32
        ).astype(jnp.bfloat16)

    def take_norm(k, carry):
        j = lax.rem(me + n - k, n)
        norm_copy(j, me).wait_recv()
        pass_copy(j, core).start()
        return carry

    lax.fori_loop(1, n, take_norm, 0)

    def take_pass(k, carry):
        pass_copy(lax.rem(me + n - k, n), peer).wait_recv()
        return carry

    lax.fori_loop(1, n, take_pass, 0)

    def part_copy(m, other):
        return remote(
            part_send.at[other],
            part_recv.at[m],
            part_sems.at[0, other],
            part_sems.at[1, m],
            other * group_size + place,
            core,
        )

    def back_copy(j, other):
        return remote(
            back_send.at[other],
            back_recv.at[j],
            back_sems.at[0, other],
            back_sems.at[1, j],
            other,
            core,
        )

    def dense_copy(m, other):
        return remote(
            dense_all.at[m],
            dense_all.at[m],
            dense_sems.at[0, other],
            dense_sems.at[1, m],
            other * group_size + place,
            core,
        )

    group = min(n, 16)
    groups = n // group
    block = group * rows

    def take_weights(k, carry):
        other = lax.rem(place + k, group_size)
        team_copy(dense_gate_ref, dense_gate_all, dense_gate_sems, other, place).wait_recv()
        team_copy(dense_up_ref, dense_up_all, dense_up_sems, other, place).wait_recv()
        team_copy(down_ref, down_all, down_sems, other, place).wait_recv()
        return carry

    lax.fori_loop(1, group_size, take_weights, 0)
    features = jnp.concatenate(
        [norm_all[owner, m * group_size + place, :, pl.ds(lane, window)] for m in range(teams)],
        axis=0,
    )
    hidden_cols = dense_gate_ref.shape[1]
    for gathered, columns in (
        (dense_gate_all, slice(0, hidden_cols)),
        (dense_up_all, slice(hidden_cols, 2 * hidden_cols)),
    ):
        value = jnp.dot(
            features, gathered[...].reshape(window, hidden_cols), preferred_element_type=f32
        )
        part_send[:, :, columns] = value.astype(jnp.bfloat16).reshape(teams, rows, hidden_cols)

    def send_part(k, carry):
        part_copy(team, lax.rem(team + k, teams)).start()
        return carry

    lax.fori_loop(1, teams, send_part, 0)

    loads[1].wait()
    loads[2].wait()

    def expert_first(c, carry):
        base = c * group
        low = norm_all[0, pl.ds(base, group)].reshape(block, half)
        high = norm_all[1, pl.ds(base, group)].reshape(block, half)
        gate_rows = jnp.dot(low, w_gate[:half], preferred_element_type=f32) + jnp.dot(
            high, w_gate[half:], preferred_element_type=f32
        )
        up_rows = jnp.dot(low, w_up[:half], preferred_element_type=f32) + jnp.dot(
            high, w_up[half:], preferred_element_type=f32
        )
        hidden_ref[pl.ds(c, 1)] = (jax.nn.silu(gate_rows) * up_rows).astype(jnp.bfloat16)[None]
        return carry

    lax.fori_loop(0, groups, expert_first, 0)

    def take_part(k, total):
        m = lax.rem(team + teams - k, teams)
        part_copy(m, team).wait_recv()
        return total + part_recv[m].astype(f32)

    paired = lax.fori_loop(1, teams, take_part, part_send[team].astype(f32))
    dense_all[team] = (jax.nn.silu(paired[:, :hidden_cols]) * paired[:, hidden_cols:]).astype(
        jnp.bfloat16
    )

    def send_dense(k, carry):
        dense_copy(team, lax.rem(team + k, teams)).start()
        return carry

    lax.fori_loop(1, teams, send_dense, 0)

    loads[3].wait()
    far = pl.ds(pl.multiple_of(peer * half, half), half)
    near = pl.ds(pl.multiple_of(core * half, half), half)

    def expert_far(c, carry):
        value = jnp.dot(hidden_ref[c], w_down[:, far], preferred_element_type=f32)
        other_ref[pl.ds(c * group, group)] = value.astype(jnp.bfloat16).reshape(group, rows, half)
        return carry

    lax.fori_loop(0, groups, expert_far, 0)
    trade = remote(other_ref, peer_ref, pair_sems.at[2], pair_sems.at[3], me, peer)
    trade.start()

    def expert_near(c, carry):
        value = jnp.dot(hidden_ref[c], w_down[:, near], preferred_element_type=f32)
        mine_ref[pl.ds(c * group, group)] = value.astype(jnp.bfloat16).reshape(group, rows, half)
        return carry

    lax.fori_loop(0, groups, expert_near, 0)
    trade.wait()

    def send_back(k, carry):
        other = lax.rem(me + k, n)
        total = mine_ref[other].astype(f32) + peer_ref[other].astype(f32)
        back_send[other] = total.astype(jnp.bfloat16)

        @pl.when(k > 0)
        def _():
            back_copy(me, other).start()

        return carry

    lax.fori_loop(0, n, send_back, 0)

    def take_dense(k, carry):
        dense_copy(lax.rem(team + teams - k, teams), team).wait_recv()
        return carry

    lax.fori_loop(1, teams, take_dense, 0)
    dense_rows = dense_all[...].reshape(teams * rows, hidden_cols)
    columns = [
        jnp.dot(dense_rows, down_all[q], preferred_element_type=f32) for q in range(group_size)
    ]
    cols_send[...] = (
        jnp.concatenate(columns, axis=1).astype(jnp.bfloat16).reshape(cols_send.shape)
    )

    def cols_copy(from_core, m, other, target):
        return remote(
            cols_send.at[other],
            cols_recv.at[from_core, m],
            cols_send_sem.at[other],
            cols_recv_sem.at[from_core, m],
            other * group_size + place,
            target,
        )

    def send_cols(k, carry):
        cols_copy(core, team, lax.rem(team + k, teams), owner).start()
        return carry

    lax.fori_loop(1, teams, send_cols, 0)

    @pl.when(owner == core)
    def _():
        cols_recv[core, team] = cols_send[team]

    @pl.when(owner != core)
    def _():
        cols_copy(core, team, team, peer).start()

    side = teams // 2

    def take_cols(k, carry):
        m = core * side + k

        @pl.when(m != team)
        def _():
            cols_copy(core, m, team, core).wait_recv()

        cols_copy(peer, m, team, core).wait_recv()
        return carry

    lax.fori_loop(0, side, take_cols, 0)
    dense = jnp.concatenate(
        [
            cols_recv[0, core * side + q].astype(f32) + cols_recv[1, core * side + q].astype(f32)
            for q in range(side)
        ],
        axis=1,
    )
    total = res_ref[:, near].astype(f32) + mix_gate * dense

    def take_back(k, total):
        j = lax.rem(me + n - k, n)

        @pl.when(k > 0)
        def _():
            back_copy(j, me).wait_recv()

        @pl.when(k == 0)
        def _():
            back_recv[me] = back_send[me]

        gate = jnp.sum(jnp.where(expert_index == j, gates, 0.0), axis=-1, keepdims=True)
        return total + gate * back_recv[j].astype(f32)

    out_ref[...] = lax.fori_loop(0, n, take_back, total).astype(jnp.bfloat16)

    def drain(k, carry):
        other = lax.rem(me + k, n)
        norm_copy(me, other).wait_send()
        pass_copy(other, core).wait_send()
        back_copy(me, other).wait_send()
        return carry

    lax.fori_loop(1, n, drain, 0)

    def drain_team(k, carry):
        other = lax.rem(place + k, group_size)
        team_copy(dense_gate_ref, dense_gate_all, dense_gate_sems, place, other).wait_send()
        team_copy(dense_up_ref, dense_up_all, dense_up_sems, place, other).wait_send()
        team_copy(down_ref, down_all, down_sems, place, other).wait_send()
        return carry

    lax.fori_loop(1, group_size, drain_team, 0)

    def drain_dense(k, carry):
        other = lax.rem(team + k, teams)
        part_copy(team, other).wait_send()
        dense_copy(team, other).wait_send()
        cols_copy(core, team, other, owner).wait_send()
        return carry

    lax.fori_loop(1, teams, drain_dense, 0)

    @pl.when(owner != core)
    def _():
        cols_copy(core, team, team, peer).wait_send()


def flip(place, k):
    result, bit = place, 1
    while bit <= k:
        if k & bit:
            result = result + bit * (1 - 2 * ((place // bit) % 2))
        bit *= 2
    return result


def finish(*refs):
    copies = [
        pltpu.make_async_copy(refs[i], refs[i + 3], refs[6].at[i]) for i in range(3)
    ]
    for copy in copies:
        copy.start()
    for copy in copies:
        copy.wait()


def routed_layer(
    n,
    inner,
    tokens_hbm,
    attn_gain_hbm,
    lengths_hbm,
    bias_hbm,
    w_key_hbm,
    w_value_hbm,
    gain_hbm,
    router_hbm,
    routes_hbm,
    mix_hbm,
    dense_gate_hbm,
    dense_up_hbm,
    down_hbm,
    w_query_hbm,
    w_out_hbm,
    w_gate_hbm,
    w_up_hbm,
    w_down_hbm,
    keys_hbm,
    values_hbm,
    out_ref,
    new_keys_ref,
    new_values_ref,
    tokens_ref,
    attn_gain_ref,
    lengths_ref,
    bias_ref,
    w_key_ref,
    w_value_ref,
    gain_ref,
    router_ref,
    routes_ref,
    mix_ref,
    dense_gate_ref,
    dense_up_ref,
    down_ref,
    w_query,
    w_out,
    w_gate,
    w_up,
    w_down,
    keys,
    values,
    query_ref,
    score_ref,
    read_ref,
    stick_ref,
    normed_ref,
    small_send,
    small,
    routes_all,
    hits_ref,
    attn_mine,
    attn_peer,
    res_ref,
    norm_all,
    first_send,
    first_recv,
    plane_send,
    plane_recv,
    far_recv,
    line_send,
    line_recv,
    load_sem,
    keys_sem,
    values_sem,
    pair_sems,
    swap_sems,
    small_send_sem,
    small_recv_sem,
    down_send_sem,
    down_recv_sem,
    routes_sems,
    line_sems,
    spread_sems,
    first_sems,
    plane_sems,
    far_sems,
    back_sems,
):
    me = lax.axis_index("ep")
    core = lax.axis_index("tp")
    peer = 1 - core
    f32, bf16 = jnp.float32, jnp.bfloat16
    rows, model = tokens_ref.shape
    half = model // 2
    width, hidden_cols = dense_gate_ref.shape
    units = hidden_cols // n
    outer = n // inner
    z, p = me // inner, me % inner
    side = n // 2
    owner, slot = me // side, me % side
    local_heads = bias_ref.shape[1]
    head_dim, cache_len = keys_hbm.shape[1:]
    hidden = w_gate_hbm.shape[1]
    expert_total = router_ref.shape[0]
    lanes = small.shape[0]
    router_at = 4 * units
    mix_at = router_at + expert_total
    span = rows // 2
    turns = list(range(outer - 1, 0, -1))
    around = turns[-2:]
    homeward = turns[:-1]
    direct = [j for j in range(1, inner) if j & (j - 1) == 0]
    indirect = [j for j in range(1, inner) if j & (j - 1)]
    lines = span * local_heads

    def remote(source, target, send_sem, recv_sem, ep, tp):
        return pltpu.make_async_remote_copy(
            src_ref=source,
            dst_ref=target,
            send_sem=send_sem,
            recv_sem=recv_sem,
            device_id=(ep, tp),
            device_id_type=MESH,
        )

    near = pl.ds(pl.multiple_of(core * half, half), half)
    far = pl.ds(pl.multiple_of(peer * half, half), half)
    mine = pl.ds(pl.multiple_of(core * hidden, hidden), hidden)
    quarter = model // 4
    query_parts = [pl.ds(i * quarter, quarter) for i in range(4)]
    pairs = (
        (tokens_hbm, tokens_ref),
        (attn_gain_hbm, attn_gain_ref),
        (dense_gate_hbm, dense_gate_ref),
        (dense_up_hbm, dense_up_ref),
        (routes_hbm, routes_ref),
        *[(w_query_hbm.at[part], w_query.at[part]) for part in query_parts],
        (bias_hbm, bias_ref),
        (lengths_hbm, lengths_ref),
        (down_hbm, down_ref),
        (router_hbm, router_ref),
        (mix_hbm, mix_ref),
        (gain_hbm, gain_ref),
        (w_out_hbm, w_out),
        (w_key_hbm, w_key_ref),
        (w_value_hbm, w_value_ref),
        (w_gate_hbm.at[near, :], w_gate.at[:, mine]),
        (w_up_hbm.at[near, :], w_up.at[:, mine]),
        (w_down_hbm.at[:, near], w_down.at[mine, :]),
    )
    loads = [
        pltpu.make_async_copy(source, target, load_sem.at[i])
        for i, (source, target) in enumerate(pairs)
    ]
    load_of = {id(target): load for (_, target), load in zip(pairs, loads)}

    def arrived(*targets):
        for target in targets:
            load_of[id(target)].wait()

    def keys_load(c):
        block = pl.ds(c * span, span)
        return pltpu.make_async_copy(keys_hbm.at[block], keys.at[block], keys_sem.at[c])

    def values_load(c):
        block = pl.ds(c * span, span)
        return pltpu.make_async_copy(values_hbm.at[block], values.at[block], values_sem.at[c])

    for load in loads[:12]:
        load.start()

    barrier = pltpu.get_barrier_semaphore()

    def greet(k, carry):
        other = lax.rem(me + k, n)
        pl.semaphore_signal(barrier, inc=1, device_id=(other, core), device_id_type=MESH)
        pl.semaphore_signal(barrier, inc=1, device_id=(other, peer), device_id_type=MESH)
        return carry

    lax.fori_loop(1, n, greet, 0)
    pl.semaphore_signal(barrier, inc=1, device_id=(me, peer), device_id_type=MESH)

    arrived(tokens_ref, attn_gain_ref)
    start = tokens_ref[...].astype(f32)
    normed_ref[...] = (
        start
        * lax.rsqrt(jnp.mean(start * start, axis=-1, keepdims=True) + 1e-06)
        * attn_gain_ref[...]
    ).astype(bf16)
    for c in range(2):
        keys_load(c).start()
    arrived(dense_gate_ref, dense_up_ref, routes_ref)
    small_send[:, :units, :] = dense_gate_ref[...].T.reshape(n, units, width)
    small_send[:, units:, :] = dense_up_ref[...].T.reshape(n, units, width)
    top_k = routes_ref.shape[0]
    for k in range(top_k):
        routes_all[me, :, k * rows : (k + 1) * rows] = routes_ref[k : k + 1, :].astype(f32)

    queries = jnp.zeros((rows, w_query.shape[1]), f32)
    for i in range(4):
        loads[5 + i].wait()
        if i % 2:
            values_load(i // 2).start()
        part = slice(i * quarter, (i + 1) * quarter)
        queries = queries + jnp.dot(
            normed_ref[:, part], w_query[part, :], preferred_element_type=f32
        )
    queries = queries.astype(bf16).astype(f32)
    for h in range(local_heads):
        query_ref[:, h, :] = queries[:, h * head_dim : (h + 1) * head_dim]

    block_len = min(256, cache_len)
    after_mask = (
        lax.broadcasted_iota(jnp.int32, (block_len, block_len), 0)
        > lax.broadcasted_iota(jnp.int32, (block_len, block_len), 1)
    ).astype(bf16)
    position = lax.broadcasted_iota(jnp.int32, (lines, block_len), 1)
    arrived(bias_ref, lengths_ref)
    head_row = lax.broadcasted_iota(jnp.int32, (local_heads, local_heads), 0)
    head_col = lax.broadcasted_iota(jnp.int32, (local_heads, local_heads), 1)
    bias = jnp.sum(jnp.where(head_row == head_col, bias_ref[...], 0.0), axis=1, keepdims=True)
    line_seq = lax.broadcasted_iota(jnp.int32, (lines, rows), 0) // local_heads
    seq_lane = lax.broadcasted_iota(jnp.int32, (lines, rows), 1)
    lengths_row = lengths_ref[...].astype(f32)

    for s in range(rows):
        if s % span == 0:
            keys_load(s // span).wait()
            for load in loads[12:16] if s == 0 else loads[16:]:
                load.start()
        score_ref[s] = (
            jnp.dot(query_ref[s].astype(bf16), keys[s], preferred_element_type=f32)
            * head_dim ** (-0.5)
            + bias
        )

    def stick_breaking(c):
        limits = jnp.sum(
            jnp.where(seq_lane == line_seq + c * span, lengths_row, 0.0), axis=1, keepdims=True
        ).astype(jnp.int32)
        later = jnp.zeros((lines, 1), f32)
        for first_pos in range(cache_len - block_len, -1, -block_len):
            columns = slice(first_pos, first_pos + block_len)
            scores = score_ref[c * span : (c + 1) * span, :, columns].reshape(lines, block_len)
            visible = position + first_pos < limits
            keep = -(jnp.maximum(scores, 0.0) + jnp.log(1.0 + jnp.exp(-jnp.abs(scores))))
            log_take = scores + keep
            keep = jnp.where(visible, keep, 0.0)
            top = keep.astype(bf16)
            low = (keep - top.astype(f32)).astype(bf16)
            sums = jnp.dot(
                jnp.concatenate([top, low], axis=0), after_mask, preferred_element_type=f32
            )
            after = sums[:lines] + sums[lines:] + later
            later = later + jnp.sum(keep, axis=-1, keepdims=True)
            stick = jnp.where(visible, jnp.exp(log_take + after), 0.0)
            stick_ref[c, :, columns] = stick.astype(bf16)

    def read_values(c):
        mixed = lax.dot_general(
            values[c * span : (c + 1) * span].reshape(span * head_dim, cache_len),
            stick_ref[c],
            (((1,), (1,)), ((), ())),
            preferred_element_type=f32,
        ).reshape(span, head_dim, lines)
        seq_of = lax.broadcasted_iota(jnp.int32, (head_dim, lines), 1) // local_heads
        own_seq = jnp.zeros((head_dim, lines), f32)
        for s in range(span):
            own_seq = jnp.where(seq_of == s, mixed[s], own_seq)
        read_ref[c * span : (c + 1) * span] = own_seq.T.reshape(span, local_heads, head_dim)

    for c in range(2):
        stick_breaking(c)
    pl.semaphore_wait(barrier, 2 * n - 1)
    trades = [
        remote(
            w_gate_hbm.at[far, :], w_gate.at[:, mine], pair_sems.at[0, 0], pair_sems.at[1, 0], me, peer
        ),
        remote(
            w_up_hbm.at[far, :], w_up.at[:, mine], pair_sems.at[0, 1], pair_sems.at[1, 1], me, peer
        ),
        remote(
            w_down_hbm.at[:, far], w_down.at[mine, :], pair_sems.at[0, 2], pair_sems.at[1, 2], me, peer
        ),
    ]

    def small_copy(other, tp):
        return remote(
            small_send.at[other],
            small.at[pl.ds(core * 2 * units, 2 * units), pl.ds(pl.multiple_of(slot * width, width), width)],
            small_send_sem.at[other],
            small_recv_sem.at[core, slot],
            other,
            tp,
        )

    def down_copy(other, tp):
        return remote(
            down_ref.at[pl.ds(pl.multiple_of(other * units, units), units), :],
            w_down.at[
                pl.ds(2 * hidden + core * 2 * units, units),
                pl.ds(pl.multiple_of(slot * width, width), width),
            ],
            down_send_sem.at[other],
            down_recv_sem.at[core, slot],
            other,
            tp,
        )

    def routes_copy(origin, other):
        return remote(
            routes_all.at[origin],
            routes_all.at[origin],
            routes_sems.at[0, other],
            routes_sems.at[1, origin],
            other,
            core,
        )

    arrived(down_ref)

    def send_small(k, carry):
        other = lax.rem(me + k, n)
        routes_copy(me, other).start()
        small_copy(other, owner).start()
        return carry

    def send_down(k, carry):
        down_copy(lax.rem(me + k, n), owner).start()
        return carry

    lax.fori_loop(1, n, send_small, 0)

    @pl.when(owner == core)
    def _():
        here = pl.ds(pl.multiple_of(slot * width, width), width)
        small[pl.ds(pl.multiple_of(core * 2 * units, 2 * units), 2 * units), here] = small_send[me]
        w_down[
            pl.ds(pl.multiple_of(2 * hidden + core * 2 * units, units), units), here
        ] = down_ref[pl.ds(pl.multiple_of(me * units, units), units), :]

    @pl.when(owner != core)
    def _():
        small_copy(me, peer).start()

    for c in range(2):
        values_load(c).wait()
    for c in range(2):
        read_values(c)
    heads_out = jnp.concatenate([read_ref[:, h, :] for h in range(local_heads)], axis=1).astype(
        bf16
    )
    arrived(w_out)
    swaps = []
    for i in range(2):
        attn_mine[i] = jnp.dot(
            heads_out, w_out[:, i * half : (i + 1) * half], preferred_element_type=f32
        ).astype(bf16)
        swaps.append(
            remote(
                attn_mine.at[i], attn_peer.at[i], swap_sems.at[0, i], swap_sems.at[1, i], me, peer
            )
        )
        swaps[i].start()
    for trade in trades:
        trade.start()
    arrived(gain_ref)
    wide = []
    for i in range(2):
        swaps[i].wait_recv()
        columns = slice(i * half, (i + 1) * half)
        res_ref[i] = (
            tokens_ref[:, columns].astype(f32)
            + (attn_mine[i].astype(f32) + attn_peer[i].astype(f32))
        ).astype(bf16)
        wide.append(res_ref[i].astype(f32))
    squares = sum(jnp.sum(part * part, axis=-1, keepdims=True) for part in wide)
    scale = lax.rsqrt(squares / model + 1e-06)
    norm_all[me] = (
        jnp.where(core == 0, wide[0], wide[1])
        * scale
        * jnp.where(core == 0, gain_ref[:, :half], gain_ref[:, half:])
    ).astype(bf16)

    def line_copy(k):
        return remote(
            norm_all.at[me],
            norm_all.at[me],
            line_sems.at[0, k],
            line_sems.at[1, k],
            flip(z, k) * inner + p,
            core,
        )

    def spread_copy(k, j):
        origin = flip(z, k) * inner + p
        return remote(
            norm_all.at[origin],
            norm_all.at[origin],
            spread_sems.at[0, k, j],
            spread_sems.at[1, k, j],
            z * inner + flip(p, j),
            core,
        )

    def around_copy(k, j):
        origin = z * inner + flip(p, j)
        return remote(
            norm_all.at[origin],
            norm_all.at[origin],
            spread_sems.at[0, k, j],
            spread_sems.at[1, k, j],
            flip(z, k) * inner + p,
            core,
        )

    for k in turns:
        line_copy(k).start()
    for j in indirect + direct:
        spread_copy(0, j).start()


    lax.fori_loop(1, n, send_down, 0)

    @pl.when(owner != core)
    def _():
        down_copy(me, peer).start()

    across = (((1,), (1,)), ((), ()))
    arrived(w_key_ref, w_value_ref)
    for weight, target in ((w_key_ref, new_keys_ref), (w_value_ref, new_values_ref)):
        target[...] = lax.dot_general(
            normed_ref[...], weight[...], across, preferred_element_type=f32
        ).astype(bf16)

    def small_taken(tp, k):
        return remote(
            small_send.at[0],
            small.at[
                pl.ds(tp * 2 * units, 2 * units), pl.ds(pl.multiple_of(k * width, width), width)
            ],
            small_send_sem.at[0],
            small_recv_sem.at[tp, k],
            me,
            peer,
        )

    def down_taken(tp, k):
        return remote(
            down_ref.at[pl.ds(0, units), :],
            w_down.at[
                pl.ds(2 * hidden + tp * 2 * units, units),
                pl.ds(pl.multiple_of(k * width, width), width),
            ],
            down_send_sem.at[0],
            down_recv_sem.at[tp, k],
            me,
            peer,
        )

    def take_all(taken):
        def take(k, carry):
            @pl.when(core * side + k != me)
            def _():
                taken(core, k).wait_recv()

            taken(peer, k).wait_recv()
            return carry

        lax.fori_loop(0, side, take, 0)

    arrived(router_ref, mix_ref)
    spread_rows = lanes - mix_at
    mix_row = mix_ref[...]
    mix_top = mix_row.astype(bf16)
    mix_rest = mix_row - mix_top.astype(f32)
    mix_mid = mix_rest.astype(bf16)
    mix_low = (mix_rest - mix_mid.astype(f32)).astype(bf16)
    mix_index = lax.broadcasted_iota(jnp.int32, (spread_rows, model), 0)
    mix_rows = jnp.where(
        mix_index == 0,
        mix_top.astype(f32),
        jnp.where(
            mix_index == 1,
            mix_mid.astype(f32),
            jnp.where(mix_index == 2, mix_low.astype(f32), 0.0),
        ),
    ).astype(bf16)
    small[pl.ds(router_at, expert_total), :] = jnp.where(
        core == 0, router_ref[:, :half], router_ref[:, half:]
    )
    small[pl.ds(mix_at, spread_rows), :] = jnp.where(
        core == 0, mix_rows[:, :half], mix_rows[:, half:]
    )
    for base in (units, 3 * units):
        w_down[pl.ds(2 * hidden + base, units), :] = jnp.zeros((units, half), bf16)
    tail = lanes - 4 * units
    w_down[pl.ds(2 * hidden + 4 * units, tail), :] = jnp.zeros((tail, half), bf16)

    for k in turns:
        line_copy(k).wait_recv()
        for j in direct if k in around else indirect + direct:
            spread_copy(k, j).start()
        if k == turns[0]:
            for j in indirect:
                spread_copy(0, j).wait_recv()
                for m in around:
                    around_copy(m, j).start()
    take_all(small_taken)

    arrived(*[target for _, target in pairs[18:]])
    for trade in trades:
        trade.wait_recv()

    chunk = inner * rows
    lane = lax.broadcasted_iota(jnp.int32, (chunk, lanes), 1)
    dense_lane = (lane < units) | ((lane >= 2 * units) & (lane < 3 * units))

    rest_at = 2 * hidden + lanes

    def first_copy(k):
        return remote(
            first_send.at[k], first_recv.at[k], first_sems.at[0, k], first_sems.at[1, k], me, peer
        )

    def group(k):
        return pl.ds(pl.multiple_of(flip(z, k) * inner, inner), inner)

    def first(*ks):
        for k in ks:
            for j in range(1, inner) if k else direct:
                spread_copy(k, j).wait_recv()
        x = jnp.concatenate([norm_all[group(k)].reshape(chunk, half) for k in ks], axis=0)
        gate_rows = jnp.dot(x, w_gate[...], preferred_element_type=f32)
        rest = lax.dot_general(x, small[...], across, preferred_element_type=f32)
        up_rows = jnp.dot(x, w_up[...], preferred_element_type=f32)
        for i, k in enumerate(ks):
            own_rows = slice(i * chunk, (i + 1) * chunk)
            first_send[k, :, : 2 * hidden] = gate_rows[own_rows]
            first_send[k, :, 2 * hidden : rest_at] = rest[own_rows]
            first_send[k, :, rest_at:] = up_rows[own_rows]
        for k in ks:
            first_copy(k).start()

    def plane_copy(k, j):
        other = flip(p, j)
        return remote(
            plane_send.at[k, other],
            plane_recv.at[k, j],
            plane_sems.at[0, k, j],
            plane_sems.at[1, k, j],
            z * inner + other,
            core,
        )

    def far_copy(k, j):
        return remote(
            plane_send.at[k, flip(p, j)],
            far_recv.at[k, j],
            far_sems.at[0, k, j],
            far_sems.at[1, k, j],
            flip(z, k) * inner + p,
            core,
        )

    def send_plane(k):
        for j in indirect:
            if k in homeward:
                far_copy(k, j).start()
            elif k:
                plane_copy(k, j).start()
        for j in direct:
            plane_copy(k, j).start()

    def activations(k):
        gate_rows = first_send[k, :, : 2 * hidden] + first_recv[k, :, : 2 * hidden]
        up_rows = first_send[k, :, rest_at:] + first_recv[k, :, rest_at:]
        rest = first_send[k, :, 2 * hidden : rest_at] + first_recv[k, :, 2 * hidden : rest_at]
        chosen = hits_ref[group(k)].reshape(chunk, lanes)
        picked = jnp.where(chosen > 0.0, jax.nn.sigmoid(rest), 0.0)
        total = jnp.sum(picked, axis=-1, keepdims=True)
        own = jnp.sum(jnp.where(lane == router_at + me, picked, 0.0), axis=-1, keepdims=True)
        gate = own / total * 2.5
        mix_sum = jnp.sum(jnp.where(lane >= mix_at, rest, 0.0), axis=-1, keepdims=True)
        mix_gate = jax.nn.sigmoid(mix_sum)
        dense = jax.nn.silu(rest) * pltpu.roll(rest, lanes - units, 1) * mix_gate
        dense = jnp.where(dense_lane, dense, 0.0).astype(bf16)
        return (jax.nn.silu(gate_rows) * up_rows * gate).astype(bf16), dense

    def second(*ks):
        for k in ks:
            first_copy(k).wait_recv()
        parts = [activations(k) for k in ks]
        act = jnp.concatenate([part[0] for part in parts], axis=0)
        dense = jnp.concatenate([part[1] for part in parts], axis=0)
        value = jnp.dot(act, w_down[: 2 * hidden], preferred_element_type=f32) + jnp.dot(
            dense, w_down[2 * hidden :], preferred_element_type=f32
        )
        for i, k in enumerate(ks):
            own_rows = value[i * chunk : (i + 1) * chunk]
            plane_send[k] = own_rows.astype(bf16).reshape(inner, rows, half)
        for k in ks:
            if k:
                send_plane(k)

    def far_home(j):
        return remote(
            far_recv.at[0, j],
            plane_recv.at[0, j],
            plane_sems.at[0, 0, j],
            plane_sems.at[1, 0, j],
            z * inner + flip(p, j),
            core,
        )

    def back_copy(k):
        return remote(
            line_send.at[k],
            line_recv.at[k],
            back_sems.at[0, k],
            back_sems.at[1, k],
            flip(z, k) * inner + p,
            core,
        )

    def collect(k):
        total = plane_send[k, p].astype(f32)
        for j in direct + (indirect if k and k not in homeward else []):
            plane_copy(k, j).wait_recv()
            total = total + plane_recv[k, j].astype(f32)
        return total

    def third(k):
        line_send[k] = collect(k).astype(bf16)
        back_copy(k).start()

    first(0)
    def take_routes(k, carry):
        routes_copy(lax.rem(me + n - k, n), me).wait_recv()
        return carry

    lax.fori_loop(1, n, take_routes, 0)
    row_lane = (lax.broadcasted_iota(jnp.int32, (rows, lanes), 1) - router_at).astype(f32)
    named = routes_all[...].reshape(n, lanes).T
    for j in range(n):
        hit = jnp.zeros((rows, lanes), f32)
        for c in range(top_k):
            hit = jnp.where(named[c * rows : (c + 1) * rows, j : j + 1] == row_lane, 1.0, hit)
        hits_ref[j] = hit

    take_all(down_taken)
    second(0)
    first(turns[0])
    for k in turns[1:]:
        first(k)
    for k in turns:
        second(k)
    send_plane(0)
    for k in turns[:-1]:
        third(k)
    for j in indirect:
        other = flip(p, j)
        total = plane_send[0, other].astype(f32)
        for k in homeward:
            far_copy(k, j).wait_recv()
            total = total + far_recv[k, j].astype(f32)
        far_recv[0, j] = total.astype(bf16)
        far_home(j).start()
    third(turns[-1])
    def drain(k, carry):
        other = lax.rem(me + k, n)
        routes_copy(me, other).wait_send()
        small_copy(other, owner).wait_send()
        down_copy(other, owner).wait_send()
        return carry

    lax.fori_loop(1, n, drain, 0)

    @pl.when(owner != core)
    def _():
        small_copy(me, peer).wait_send()
        down_copy(me, peer).wait_send()

    for copy in trades + swaps:
        copy.wait_send()
    for k in range(outer):
        if k:
            line_copy(k).wait_send()
        first_copy(k).wait_send()
        for j in range(1, inner):
            (around_copy if k in around and j in indirect else spread_copy)(k, j).wait_send()

    total = res_ref[core].astype(f32) + collect(0)
    for k in turns:
        back_copy(k).wait_recv()
        total = total + line_recv[k].astype(f32)
    for j in indirect:
        far_home(j).wait_recv()
        total = total + plane_recv[0, j].astype(f32)
    out_ref[...] = total.astype(bf16)

    for k in range(outer):
        if k:
            back_copy(k).wait_send()
        for j in range(1, inner):
            if k == 0 and j in indirect:
                far_home(j).wait_send()
            else:
                (far_copy if k in homeward and j in indirect else plane_copy)(k, j).wait_send()


def routed_shards(n, inner, arrays):
    tokens = arrays[0]
    w_key, head_bias = arrays[4], arrays[3]
    keys, w_gate, w_down = arrays[18], arrays[15], arrays[17]
    rows, model = tokens.shape
    half = model // 2
    width, hidden_cols = arrays[10].shape
    units = hidden_cols // n
    outer = n // inner
    seq_count, head_dim, cache_len = keys.shape
    local_heads = head_bias.shape[1]
    hidden = w_gate.shape[1]
    lanes = 128
    chunk = inner * rows
    bf16, f32 = jnp.bfloat16, jnp.float32
    vmem = pl.BlockSpec(memory_space=pltpu.VMEM)
    anywhere = pl.BlockSpec(memory_space=pltpu.HBM)
    dma = pltpu.SemaphoreType.DMA
    small_inputs = [pltpu.VMEM(a.shape, a.dtype) for a in arrays[:15]]
    results = pl.pallas_call(
        functools.partial(routed_layer, n, inner),
        out_shape=(
            jax.ShapeDtypeStruct((rows, half), bf16),
            jax.ShapeDtypeStruct((rows, w_key.shape[0]), bf16),
            jax.ShapeDtypeStruct((rows, w_key.shape[0]), bf16),
        ),
        in_specs=[anywhere] * 20,
        out_specs=(vmem, vmem, vmem),
        scratch_shapes=small_inputs
        + [
            pltpu.VMEM((half, 2 * hidden), bf16),
            pltpu.VMEM((half, 2 * hidden), bf16),
            pltpu.VMEM((2 * hidden + lanes, half), bf16),
            pltpu.VMEM(keys.shape, bf16),
            pltpu.VMEM(keys.shape, bf16),
            pltpu.VMEM((rows, local_heads, head_dim), f32),
            pltpu.VMEM((rows, local_heads, cache_len), f32),
            pltpu.VMEM((rows, local_heads, head_dim), f32),
            pltpu.VMEM((2, rows * local_heads // 2, cache_len), bf16),
            pltpu.VMEM((rows, model), bf16),
            pltpu.VMEM((n, 2 * units, width), bf16),
            pltpu.VMEM((lanes, half), bf16),
            pltpu.VMEM((n, 1, lanes), f32),
            pltpu.VMEM((n, rows, lanes), f32),
            pltpu.VMEM((2, rows, half), bf16),
            pltpu.VMEM((2, rows, half), bf16),
            pltpu.VMEM((2, rows, half), bf16),
            pltpu.VMEM((n, rows, half), bf16),
            pltpu.VMEM((outer, chunk, 4 * hidden + lanes), f32),
            pltpu.VMEM((outer, chunk, 4 * hidden + lanes), f32),
            pltpu.VMEM((outer, inner, rows, half), bf16),
            pltpu.VMEM((outer, inner, rows, half), bf16),
            pltpu.VMEM((outer, inner, rows, half), bf16),
            pltpu.VMEM((outer, rows, half), bf16),
            pltpu.VMEM((outer, rows, half), bf16),
            dma((21,)),
            dma((2,)),
            dma((2,)),
            dma((2, 3)),
            dma((2, 2)),
            dma((n,)),
            dma((2, n // 2)),
            dma((n,)),
            dma((2, n // 2)),
            dma((2, n)),
            dma((2, outer)),
            dma((2, outer, inner)),
            dma((2, outer)),
            dma((2, outer, inner)),
            dma((2, outer, inner)),
            dma((2, outer)),
        ],
        compiler_params=pltpu.CompilerParams(
            collective_id=0, has_side_effects=True, vmem_limit_bytes=48 * 1024 * 1024
        ),
        name="routed_layer",
    )(*[pltpu.with_memory_space_constraint(a, pltpu.HBM) for a in arrays])
    return pl.pallas_call(
        finish,
        out_shape=tuple(jax.ShapeDtypeStruct(r.shape, r.dtype) for r in results),
        in_specs=[vmem] * 3,
        out_specs=(anywhere,) * 3,
        scratch_shapes=[dma((3,))],
        name="finish",
    )(*[pltpu.with_memory_space_constraint(r, pltpu.VMEM) for r in results])


def shards(
    n,
    tokens,
    lengths,
    attn_gain,
    w_query,
    w_key,
    w_value,
    head_bias,
    key_cache,
    value_cache,
    w_attn_out,
    ffn_gain,
    w_router,
    routes,
    w_dense_gate,
    w_dense_up,
    w_dense_down,
    dense_mix,
    w_expert_gate,
    w_expert_up,
    w_expert_down,
):
    rows, model = tokens.shape
    half = model // 2
    width, hidden_cols = w_dense_gate.shape
    group_size = min(n, max(4, 128 // width))
    teams = n // group_size
    window = width * group_size
    seq_count, local_kv, head_dim, cache_len = key_cache.shape
    local_heads = head_bias.shape[0]
    keys = key_cache.reshape(seq_count, head_dim, cache_len)
    values = value_cache.reshape(seq_count, head_dim, cache_len)
    w_gate, w_up, w_down = w_expert_gate[0], w_expert_up[0], w_expert_down[0]
    expert_hidden = w_gate.shape[1]
    arrays = (
        tokens,
        attn_gain.reshape(1, model),
        lengths.reshape(1, seq_count),
        head_bias.reshape(1, local_heads),
        w_key.T,
        w_value.T,
        ffn_gain.reshape(1, model),
        w_router.T,
        routes.T,
        dense_mix.reshape(1, model),
        w_dense_gate,
        w_dense_up,
        w_dense_down,
        w_query,
        w_attn_out,
        w_gate,
        w_up,
        w_down,
        keys,
        values,
    )
    inner = 1
    while (2 * inner) ** 2 <= n:
        inner *= 2
    small_rows = 4 * (hidden_cols // n) + w_router.shape[1]
    if hidden_cols % (16 * n) == 0 and width % 128 == 0 and small_rows <= 112:
        return routed_shards(n, inner, arrays)
    bf16, f32 = jnp.bfloat16, jnp.float32
    block = min(n, 16) * rows
    vmem = pl.BlockSpec(memory_space=pltpu.VMEM)
    anywhere = pl.BlockSpec(memory_space=pltpu.HBM)
    dma = pltpu.SemaphoreType.DMA
    return pl.pallas_call(
        functools.partial(whole_layer, n, group_size),
        out_shape=(
            jax.ShapeDtypeStruct((rows, half), bf16),
            jax.ShapeDtypeStruct((rows, w_key.shape[1]), bf16),
            jax.ShapeDtypeStruct((rows, w_value.shape[1]), bf16),
        ),
        in_specs=[vmem] * 13 + [anywhere] * 7,
        out_specs=(vmem, vmem, vmem),
        scratch_shapes=[
            pltpu.VMEM(w_query.shape, bf16),
            pltpu.VMEM(w_attn_out.shape, bf16),
            pltpu.VMEM(w_gate.shape, bf16),
            pltpu.VMEM(w_up.shape, bf16),
            pltpu.VMEM(w_down.shape, bf16),
            pltpu.VMEM(keys.shape, bf16),
            pltpu.VMEM(values.shape, bf16),
            dma((5,)),
            dma((rows // 4,)),
            dma((rows // 4,)),
            pltpu.VMEM((rows, local_heads, head_dim), f32),
            pltpu.VMEM((rows, local_heads, cache_len), f32),
            pltpu.VMEM((rows, local_heads, head_dim), f32),
            pltpu.VMEM((rows, model), bf16),
            pltpu.VMEM((group_size, width, hidden_cols), bf16),
            pltpu.VMEM((group_size, width, hidden_cols), bf16),
            pltpu.VMEM((group_size, hidden_cols, width), bf16),
            pltpu.VMEM((rows, model), bf16),
            pltpu.VMEM((rows, model), bf16),
            pltpu.VMEM((rows, model), bf16),
            pltpu.VMEM((2, n, rows, half), bf16),
            pltpu.VMEM((teams, rows, 2 * hidden_cols), bf16),
            pltpu.VMEM((teams, rows, 2 * hidden_cols), bf16),
            pltpu.VMEM((n * rows // block, block, expert_hidden), bf16),
            pltpu.VMEM((teams, rows, hidden_cols), bf16),
            pltpu.VMEM((teams, rows, window), bf16),
            pltpu.VMEM((2, teams, rows, window), bf16),
            pltpu.VMEM((n, rows, half), bf16),
            pltpu.VMEM((n, rows, half), bf16),
            pltpu.VMEM((n, rows, half), bf16),
            pltpu.VMEM((n, rows, half), bf16),
            pltpu.VMEM((n, rows, half), bf16),
            dma((4,)),
            dma((2, group_size)),
            dma((2, group_size)),
            dma((2, group_size)),
            dma((2, n)),
            dma((2, n)),
            dma((2, teams)),
            dma((2, teams)),
            dma((teams,)),
            dma((2, teams)),
            dma((2, n)),
        ],
        compiler_params=pltpu.CompilerParams(
            collective_id=0, has_side_effects=True, vmem_limit_bytes=63 * 1024 * 1024
        ),
        name="whole_layer",
    )(*arrays)


def solution(mesh):
    return jax.shard_map(
        functools.partial(shards, mesh.shape["ep"]),
        mesh=mesh,
        in_specs=(
            P("ep", None),
            P("ep"),
            P(),
            P(None, "tp"),
            P(None, "tp"),
            P(None, "tp"),
            P("tp"),
            P("ep", "tp", None, None),
            P("ep", "tp", None, None),
            P("tp", None),
            P(),
            P(),
            P("ep", None),
            P("ep", "tp"),
            P("ep", "tp"),
            P("tp", "ep"),
            P(),
            P("ep", None, "tp"),
            P("ep", None, "tp"),
            P("ep", "tp", None),
        ),
        out_specs=(P("ep", "tp"), P("ep", "tp"), P("ep", "tp")),
        check_vma=False,
    )
```

```python
import functools

import jax
import jax.numpy as jnp
from jax import lax
from jax.experimental import pallas as pl
from jax.experimental.pallas import tpu as pltpu
from jax.sharding import PartitionSpec as P

MESH = pl.DeviceIdType.MESH


def whole_layer(
    n,
    group_size,
    tokens_ref,
    attn_gain_ref,
    lengths_ref,
    bias_ref,
    w_key_ref,
    w_value_ref,
    gain_ref,
    router_ref,
    routes_ref,
    mix_ref,
    dense_gate_ref,
    dense_up_ref,
    down_ref,
    w_query_hbm,
    w_out_hbm,
    w_gate_hbm,
    w_up_hbm,
    w_down_hbm,
    keys_hbm,
    values_hbm,
    out_ref,
    new_keys_ref,
    new_values_ref,
    w_query,
    w_out,
    w_gate,
    w_up,
    w_down,
    keys,
    values,
    load_sem,
    keys_sem,
    values_sem,
    query_ref,
    score_ref,
    read_ref,
    normed_ref,
    dense_gate_all,
    dense_up_all,
    down_all,
    attn_mine,
    attn_peer,
    res_ref,
    norm_all,
    part_send,
    part_recv,
    hidden_ref,
    dense_all,
    cols_send,
    cols_recv,
    other_ref,
    mine_ref,
    peer_ref,
    back_send,
    back_recv,
    pair_sems,
    dense_gate_sems,
    dense_up_sems,
    down_sems,
    norm_sems,
    pass_sems,
    part_sems,
    dense_sems,
    cols_send_sem,
    cols_recv_sem,
    back_sems,
):
    me = lax.axis_index("ep")
    core = lax.axis_index("tp")
    peer = 1 - core
    rows, model = tokens_ref.shape
    half = model // 2
    width = dense_gate_ref.shape[0]
    window = width * group_size
    place = me % group_size
    team = me // group_size
    teams = n // group_size
    first = team * window
    owner = first // half
    lane = pl.multiple_of(first % half, window)
    f32 = jnp.float32
    local_heads = bias_ref.shape[1]
    head_dim, cache_len = keys_hbm.shape[1:]
    span = 4

    def remote(source, target, send_sem, recv_sem, ep, tp):
        return pltpu.make_async_remote_copy(
            src_ref=source,
            dst_ref=target,
            send_sem=send_sem,
            recv_sem=recv_sem,
            device_id=(ep, tp),
            device_id_type=MESH,
        )

    pairs = (
        (w_query_hbm, w_query),
        (w_gate_hbm, w_gate),
        (w_up_hbm, w_up),
        (w_down_hbm, w_down),
        (w_out_hbm, w_out),
    )
    loads = [
        pltpu.make_async_copy(source, target, load_sem.at[i])
        for i, (source, target) in enumerate(pairs)
    ]

    def keys_load(c):
        block = pl.ds(c * span, span)
        return pltpu.make_async_copy(keys_hbm.at[block], keys.at[block], keys_sem.at[c])

    def values_load(c):
        block = pl.ds(c * span, span)
        return pltpu.make_async_copy(values_hbm.at[block], values.at[block], values_sem.at[c])

    loads[0].start()
    for c in range(rows // span):
        keys_load(c).start()
        values_load(c).start()
    for load in (loads[4], loads[1], loads[2], loads[3]):
        load.start()

    barrier = pltpu.get_barrier_semaphore()

    def greet(k, carry):
        other = lax.rem(me + k, n)
        pl.semaphore_signal(barrier, inc=1, device_id=(other, core), device_id_type=MESH)
        pl.semaphore_signal(barrier, inc=1, device_id=(other, peer), device_id_type=MESH)
        return carry

    lax.fori_loop(1, n, greet, 0)
    pl.semaphore_signal(barrier, inc=1, device_id=(me, peer), device_id_type=MESH)

    start = tokens_ref[...].astype(f32)
    normed_ref[...] = (
        start
        * lax.rsqrt(jnp.mean(start * start, axis=-1, keepdims=True) + 1e-06)
        * attn_gain_ref[...]
    ).astype(jnp.bfloat16)
    loads[0].wait()
    queries = jnp.dot(normed_ref[...], w_query[...], preferred_element_type=f32)
    queries = queries.astype(jnp.bfloat16).astype(f32)
    for h in range(local_heads):
        query_ref[:, h, :] = queries[:, h * head_dim : (h + 1) * head_dim]
    pl.semaphore_wait(barrier, 2 * n - 1)

    def team_copy(source, gathered, sems, origin, other):
        return remote(
            source,
            gathered.at[origin],
            sems.at[0, other],
            sems.at[1, origin],
            team * group_size + other,
            core,
        )

    def send_weights(k, carry):
        other = lax.rem(place + k, group_size)
        team_copy(dense_gate_ref, dense_gate_all, dense_gate_sems, place, other).start()
        team_copy(dense_up_ref, dense_up_all, dense_up_sems, place, other).start()
        team_copy(down_ref, down_all, down_sems, place, other).start()
        return carry

    lax.fori_loop(1, group_size, send_weights, 0)
    dense_gate_all[place] = dense_gate_ref[...]
    dense_up_all[place] = dense_up_ref[...]
    down_all[place] = down_ref[...]

    block_len = min(256, cache_len)
    after_mask = (
        lax.broadcasted_iota(jnp.int32, (block_len, block_len), 0)
        > lax.broadcasted_iota(jnp.int32, (block_len, block_len), 1)
    ).astype(jnp.bfloat16)
    position = lax.broadcasted_iota(jnp.int32, (span * local_heads, block_len), 1)

    head_row = lax.broadcasted_iota(jnp.int32, (local_heads, local_heads), 0)
    head_col = lax.broadcasted_iota(jnp.int32, (local_heads, local_heads), 1)
    bias = jnp.sum(jnp.where(head_row == head_col, bias_ref[...], 0.0), axis=1, keepdims=True)
    lines = span * local_heads
    line_seq = lax.broadcasted_iota(jnp.int32, (lines, rows), 0) // local_heads
    seq_lane = lax.broadcasted_iota(jnp.int32, (lines, rows), 1)
    lengths_row = lengths_ref[...].astype(f32)

    def attend(c, carry):
        keys_load(c).wait()
        for i in range(span):
            s = c * span + i
            score_ref[s] = (
                jnp.dot(query_ref[s].astype(jnp.bfloat16), keys[s], preferred_element_type=f32)
                * head_dim ** (-0.5)
                + bias
            )
        limits = jnp.sum(
            jnp.where(seq_lane == line_seq + c * span, lengths_row, 0.0), axis=1, keepdims=True
        ).astype(jnp.int32)
        later = jnp.zeros((lines, 1), f32)
        for first_pos in range(cache_len - block_len, -1, -block_len):
            columns = slice(first_pos, first_pos + block_len)
            scores = score_ref[pl.ds(c * span, span), :, columns].reshape(lines, block_len)
            visible = position + first_pos < limits
            keep = -(jnp.maximum(scores, 0.0) + jnp.log1p(jnp.exp(-jnp.abs(scores))))
            log_take = scores + keep
            keep = jnp.where(visible, keep, 0.0)
            top = keep.astype(jnp.bfloat16)
            rest = keep - top.astype(f32)
            middle = rest.astype(jnp.bfloat16)
            low = (rest - middle.astype(f32)).astype(jnp.bfloat16)
            sums = jnp.dot(
                jnp.concatenate([top, middle, low], axis=0),
                after_mask,
                preferred_element_type=f32,
            )
            after = sums[:lines] + sums[lines : 2 * lines] + sums[2 * lines :] + later
            later = later + jnp.sum(keep, axis=-1, keepdims=True)
            stick = jnp.where(visible, jnp.exp(log_take + after), 0.0)
            score_ref[pl.ds(c * span, span), :, columns] = stick.reshape(
                span, local_heads, block_len
            )
        values_load(c).wait()
        for i in range(span):
            s = c * span + i
            read_ref[s] = lax.dot_general(
                score_ref[s].astype(jnp.bfloat16),
                values[s],
                (((1,), (1,)), ((), ())),
                preferred_element_type=f32,
            )
        return carry

    lax.fori_loop(0, rows // span, attend, 0)
    heads_out = jnp.concatenate(
        [read_ref[:, h, :] for h in range(local_heads)], axis=1
    ).astype(jnp.bfloat16)
    loads[4].wait()
    attn_mine[...] = jnp.dot(heads_out, w_out[...], preferred_element_type=f32).astype(
        jnp.bfloat16
    )

    swap = remote(attn_mine, attn_peer, pair_sems.at[0], pair_sems.at[1], me, peer)
    swap.start()
    swap.wait()
    attn = attn_mine[...].astype(f32) + attn_peer[...].astype(f32)
    residual = (tokens_ref[...].astype(f32) + attn).astype(jnp.bfloat16)
    res_ref[...] = residual
    wide = residual.astype(f32)
    normed = (
        wide * lax.rsqrt(jnp.mean(wide * wide, axis=-1, keepdims=True) + 1e-06) * gain_ref[...]
    ).astype(jnp.bfloat16)
    norm_all[0, me] = normed[:, :half]
    norm_all[1, me] = normed[:, half:]

    def norm_copy(j, other):
        return remote(
            norm_all.at[core, j],
            norm_all.at[core, j],
            norm_sems.at[0, other],
            norm_sems.at[1, j],
            other,
            core,
        )

    def pass_copy(j, which):
        return remote(
            norm_all.at[which, j],
            norm_all.at[which, j],
            pass_sems.at[0, j],
            pass_sems.at[1, j],
            me,
            peer,
        )

    def send_norm(k, carry):
        norm_copy(me, lax.rem(me + k, n)).start()
        return carry

    lax.fori_loop(1, n, send_norm, 0)

    across = (((1,), (1,)), ((), ()))
    probs = jax.nn.sigmoid(
        lax.dot_general(router_ref[...], normed, across, preferred_element_type=f32)
    )
    expert_total = probs.shape[0]
    expert_row = lax.broadcasted_iota(jnp.int32, (expert_total, rows), 0)
    hits = jnp.zeros((expert_total, rows), f32)
    for k in range(routes_ref.shape[0]):
        hits = jnp.where(routes_ref[k : k + 1, :] == expert_row, 1.0, hits)
    picked = jnp.where(hits > 0.0, probs, 0.0)
    gates = (picked / jnp.sum(picked, axis=0, keepdims=True) * 2.5).T
    expert_index = lax.broadcasted_iota(jnp.int32, (rows, expert_total), 1)
    mix_gate = jax.nn.sigmoid(
        jnp.sum(normed.astype(f32) * mix_ref[...], axis=-1, keepdims=True)
    )

    for weight, target in ((w_key_ref, new_keys_ref), (w_value_ref, new_values_ref)):
        target[...] = lax.dot_general(
            normed_ref[...], weight[...], across, preferred_element_type=f32
        ).astype(jnp.bfloat16)

    def take_norm(k, carry):
        j = lax.rem(me + n - k, n)
        norm_copy(j, me).wait_recv()
        pass_copy(j, core).start()
        return carry

    lax.fori_loop(1, n, take_norm, 0)

    def take_pass(k, carry):
        pass_copy(lax.rem(me + n - k, n), peer).wait_recv()
        return carry

    lax.fori_loop(1, n, take_pass, 0)

    def part_copy(m, other):
        return remote(
            part_send.at[other],
            part_recv.at[m],
            part_sems.at[0, other],
            part_sems.at[1, m],
            other * group_size + place,
            core,
        )

    def back_copy(j, other):
        return remote(
            back_send.at[other],
            back_recv.at[j],
            back_sems.at[0, other],
            back_sems.at[1, j],
            other,
            core,
        )

    def dense_copy(m, other):
        return remote(
            dense_all.at[m],
            dense_all.at[m],
            dense_sems.at[0, other],
            dense_sems.at[1, m],
            other * group_size + place,
            core,
        )

    group = min(n, 16)
    groups = n // group
    block = group * rows

    def take_weights(k, carry):
        other = lax.rem(place + k, group_size)
        team_copy(dense_gate_ref, dense_gate_all, dense_gate_sems, other, place).wait_recv()
        team_copy(dense_up_ref, dense_up_all, dense_up_sems, other, place).wait_recv()
        team_copy(down_ref, down_all, down_sems, other, place).wait_recv()
        return carry

    lax.fori_loop(1, group_size, take_weights, 0)
    features = jnp.concatenate(
        [norm_all[owner, m * group_size + place, :, pl.ds(lane, window)] for m in range(teams)],
        axis=0,
    )
    hidden_cols = dense_gate_ref.shape[1]
    for gathered, columns in (
        (dense_gate_all, slice(0, hidden_cols)),
        (dense_up_all, slice(hidden_cols, 2 * hidden_cols)),
    ):
        value = jnp.dot(
            features, gathered[...].reshape(window, hidden_cols), preferred_element_type=f32
        )
        part_send[:, :, columns] = value.astype(jnp.bfloat16).reshape(teams, rows, hidden_cols)

    def send_part(k, carry):
        part_copy(team, lax.rem(team + k, teams)).start()
        return carry

    lax.fori_loop(1, teams, send_part, 0)

    loads[1].wait()
    loads[2].wait()

    def expert_first(c, carry):
        base = c * group
        low = norm_all[0, pl.ds(base, group)].reshape(block, half)
        high = norm_all[1, pl.ds(base, group)].reshape(block, half)
        gate_rows = jnp.dot(low, w_gate[:half], preferred_element_type=f32) + jnp.dot(
            high, w_gate[half:], preferred_element_type=f32
        )
        up_rows = jnp.dot(low, w_up[:half], preferred_element_type=f32) + jnp.dot(
            high, w_up[half:], preferred_element_type=f32
        )
        hidden_ref[pl.ds(c, 1)] = (jax.nn.silu(gate_rows) * up_rows).astype(jnp.bfloat16)[None]
        return carry

    lax.fori_loop(0, groups, expert_first, 0)

    def take_part(k, total):
        m = lax.rem(team + teams - k, teams)
        part_copy(m, team).wait_recv()
        return total + part_recv[m].astype(f32)

    paired = lax.fori_loop(1, teams, take_part, part_send[team].astype(f32))
    dense_all[team] = (jax.nn.silu(paired[:, :hidden_cols]) * paired[:, hidden_cols:]).astype(
        jnp.bfloat16
    )

    def send_dense(k, carry):
        dense_copy(team, lax.rem(team + k, teams)).start()
        return carry

    lax.fori_loop(1, teams, send_dense, 0)

    loads[3].wait()
    far = pl.ds(pl.multiple_of(peer * half, half), half)
    near = pl.ds(pl.multiple_of(core * half, half), half)

    def expert_far(c, carry):
        value = jnp.dot(hidden_ref[c], w_down[:, far], preferred_element_type=f32)
        other_ref[pl.ds(c * group, group)] = value.astype(jnp.bfloat16).reshape(group, rows, half)
        return carry

    lax.fori_loop(0, groups, expert_far, 0)
    trade = remote(other_ref, peer_ref, pair_sems.at[2], pair_sems.at[3], me, peer)
    trade.start()

    def expert_near(c, carry):
        value = jnp.dot(hidden_ref[c], w_down[:, near], preferred_element_type=f32)
        mine_ref[pl.ds(c * group, group)] = value.astype(jnp.bfloat16).reshape(group, rows, half)
        return carry

    lax.fori_loop(0, groups, expert_near, 0)
    trade.wait()

    def send_back(k, carry):
        other = lax.rem(me + k, n)
        total = mine_ref[other].astype(f32) + peer_ref[other].astype(f32)
        back_send[other] = total.astype(jnp.bfloat16)

        @pl.when(k > 0)
        def _():
            back_copy(me, other).start()

        return carry

    lax.fori_loop(0, n, send_back, 0)

    def take_dense(k, carry):
        dense_copy(lax.rem(team + teams - k, teams), team).wait_recv()
        return carry

    lax.fori_loop(1, teams, take_dense, 0)
    dense_rows = dense_all[...].reshape(teams * rows, hidden_cols)
    columns = [
        jnp.dot(dense_rows, down_all[q], preferred_element_type=f32) for q in range(group_size)
    ]
    cols_send[...] = (
        jnp.concatenate(columns, axis=1).astype(jnp.bfloat16).reshape(cols_send.shape)
    )

    def cols_copy(from_core, m, other, target):
        return remote(
            cols_send.at[other],
            cols_recv.at[from_core, m],
            cols_send_sem.at[other],
            cols_recv_sem.at[from_core, m],
            other * group_size + place,
            target,
        )

    def send_cols(k, carry):
        cols_copy(core, team, lax.rem(team + k, teams), owner).start()
        return carry

    lax.fori_loop(1, teams, send_cols, 0)

    @pl.when(owner == core)
    def _():
        cols_recv[core, team] = cols_send[team]

    @pl.when(owner != core)
    def _():
        cols_copy(core, team, team, peer).start()

    side = teams // 2

    def take_cols(k, carry):
        m = core * side + k

        @pl.when(m != team)
        def _():
            cols_copy(core, m, team, core).wait_recv()

        cols_copy(peer, m, team, core).wait_recv()
        return carry

    lax.fori_loop(0, side, take_cols, 0)
    dense = jnp.concatenate(
        [
            cols_recv[0, core * side + q].astype(f32) + cols_recv[1, core * side + q].astype(f32)
            for q in range(side)
        ],
        axis=1,
    )
    total = res_ref[:, near].astype(f32) + mix_gate * dense

    def take_back(k, total):
        j = lax.rem(me + n - k, n)

        @pl.when(k > 0)
        def _():
            back_copy(j, me).wait_recv()

        @pl.when(k == 0)
        def _():
            back_recv[me] = back_send[me]

        gate = jnp.sum(jnp.where(expert_index == j, gates, 0.0), axis=-1, keepdims=True)
        return total + gate * back_recv[j].astype(f32)

    out_ref[...] = lax.fori_loop(0, n, take_back, total).astype(jnp.bfloat16)

    def drain(k, carry):
        other = lax.rem(me + k, n)
        norm_copy(me, other).wait_send()
        pass_copy(other, core).wait_send()
        back_copy(me, other).wait_send()
        return carry

    lax.fori_loop(1, n, drain, 0)

    def drain_team(k, carry):
        other = lax.rem(place + k, group_size)
        team_copy(dense_gate_ref, dense_gate_all, dense_gate_sems, place, other).wait_send()
        team_copy(dense_up_ref, dense_up_all, dense_up_sems, place, other).wait_send()
        team_copy(down_ref, down_all, down_sems, place, other).wait_send()
        return carry

    lax.fori_loop(1, group_size, drain_team, 0)

    def drain_dense(k, carry):
        other = lax.rem(team + k, teams)
        part_copy(team, other).wait_send()
        dense_copy(team, other).wait_send()
        cols_copy(core, team, other, owner).wait_send()
        return carry

    lax.fori_loop(1, teams, drain_dense, 0)

    @pl.when(owner != core)
    def _():
        cols_copy(core, team, team, peer).wait_send()


def flip(place, k):
    result, bit = place, 1
    while bit <= k:
        if k & bit:
            result = result + bit * (1 - 2 * ((place // bit) % 2))
        bit *= 2
    return result


def finish(*refs):
    copies = [
        pltpu.make_async_copy(refs[i], refs[i + 3], refs[6].at[i]) for i in range(3)
    ]
    for copy in copies:
        copy.start()
    for copy in copies:
        copy.wait()


def routed_layer(
    n,
    inner,
    tokens_hbm,
    attn_gain_hbm,
    lengths_hbm,
    bias_hbm,
    w_key_hbm,
    w_value_hbm,
    gain_hbm,
    router_hbm,
    routes_hbm,
    mix_hbm,
    dense_gate_hbm,
    dense_up_hbm,
    down_hbm,
    w_query_hbm,
    w_out_hbm,
    w_gate_hbm,
    w_up_hbm,
    w_down_hbm,
    keys_hbm,
    values_hbm,
    out_ref,
    new_keys_ref,
    new_values_ref,
    tokens_ref,
    attn_gain_ref,
    lengths_ref,
    bias_ref,
    w_key_ref,
    w_value_ref,
    gain_ref,
    router_ref,
    routes_ref,
    mix_ref,
    dense_gate_ref,
    dense_up_ref,
    down_ref,
    w_query,
    w_out,
    w_gate,
    w_up,
    w_down,
    keys,
    values,
    query_ref,
    score_ref,
    read_ref,
    stick_ref,
    normed_ref,
    small_send,
    small,
    routes_all,
    hits_ref,
    attn_mine,
    attn_peer,
    res_ref,
    norm_all,
    first_send,
    first_recv,
    plane_send,
    plane_recv,
    far_recv,
    line_send,
    line_recv,
    load_sem,
    keys_sem,
    values_sem,
    pair_sems,
    swap_sems,
    small_send_sem,
    small_recv_sem,
    down_send_sem,
    down_recv_sem,
    routes_sems,
    line_sems,
    spread_sems,
    first_sems,
    plane_sems,
    far_sems,
    back_sems,
):
    me = lax.axis_index("ep")
    core = lax.axis_index("tp")
    peer = 1 - core
    f32, bf16 = jnp.float32, jnp.bfloat16
    rows, model = tokens_ref.shape
    half = model // 2
    width, hidden_cols = dense_gate_ref.shape
    units = hidden_cols // n
    outer = n // inner
    z, p = me // inner, me % inner
    side = n // 2
    owner, slot = me // side, me % side
    local_heads = bias_ref.shape[1]
    head_dim, cache_len = keys_hbm.shape[1:]
    hidden = w_gate_hbm.shape[1]
    expert_total = router_ref.shape[0]
    lanes = small.shape[0]
    router_at = 4 * units
    mix_at = router_at + expert_total
    span = rows // 2
    turns = list(range(outer - 1, 0, -1))
    around = turns[-2:]
    homeward = turns
    direct = [j for j in range(1, inner) if j & (j - 1) == 0]
    indirect = [j for j in range(1, inner) if j & (j - 1)]
    lines = span * local_heads

    def remote(source, target, send_sem, recv_sem, ep, tp):
        return pltpu.make_async_remote_copy(
            src_ref=source,
            dst_ref=target,
            send_sem=send_sem,
            recv_sem=recv_sem,
            device_id=(ep, tp),
            device_id_type=MESH,
        )

    near = pl.ds(pl.multiple_of(core * half, half), half)
    far = pl.ds(pl.multiple_of(peer * half, half), half)
    mine = pl.ds(pl.multiple_of(core * hidden, hidden), hidden)
    quarter = model // 4
    query_parts = [pl.ds(i * quarter, quarter) for i in range(4)]
    pairs = (
        (tokens_hbm, tokens_ref),
        (attn_gain_hbm, attn_gain_ref),
        (dense_gate_hbm, dense_gate_ref),
        (dense_up_hbm, dense_up_ref),
        (routes_hbm, routes_ref),
        *[(w_query_hbm.at[part], w_query.at[part]) for part in query_parts],
        (bias_hbm, bias_ref),
        (lengths_hbm, lengths_ref),
        (down_hbm, down_ref),
        (router_hbm, router_ref),
        (mix_hbm, mix_ref),
        (gain_hbm, gain_ref),
        (w_out_hbm, w_out),
        (w_key_hbm, w_key_ref),
        (w_value_hbm, w_value_ref),
        (w_gate_hbm.at[near, :], w_gate.at[:, mine]),
        (w_up_hbm.at[near, :], w_up.at[:, mine]),
        (w_down_hbm.at[:, near], w_down.at[mine, :]),
    )
    loads = [
        pltpu.make_async_copy(source, target, load_sem.at[i])
        for i, (source, target) in enumerate(pairs)
    ]
    load_of = {id(target): load for (_, target), load in zip(pairs, loads)}

    def arrived(*targets):
        for target in targets:
            load_of[id(target)].wait()

    def keys_load(c):
        block = pl.ds(c * span, span)
        return pltpu.make_async_copy(keys_hbm.at[block], keys.at[block], keys_sem.at[c])

    def values_load(c):
        block = pl.ds(c * span, span)
        return pltpu.make_async_copy(values_hbm.at[block], values.at[block], values_sem.at[c])

    for load in loads[:2] + loads[5:9]:
        load.start()

    barrier = pltpu.get_barrier_semaphore()

    def greet(k, carry):
        other = lax.rem(me + k, n)
        pl.semaphore_signal(barrier, inc=1, device_id=(other, core), device_id_type=MESH)
        pl.semaphore_signal(barrier, inc=1, device_id=(other, peer), device_id_type=MESH)
        return carry

    lax.fori_loop(1, n, greet, 0)
    pl.semaphore_signal(barrier, inc=1, device_id=(me, peer), device_id_type=MESH)
    for load in loads[2:5] + loads[9:12]:
        load.start()

    arrived(tokens_ref, attn_gain_ref)
    start = tokens_ref[...].astype(f32)
    normed_ref[...] = (
        start
        * lax.rsqrt(jnp.mean(start * start, axis=-1, keepdims=True) + 1e-06)
        * attn_gain_ref[...]
    ).astype(bf16)
    for c in range(2):
        keys_load(c).start()
    arrived(dense_gate_ref, dense_up_ref, routes_ref)
    small_send[:, :units, :] = dense_gate_ref[...].T.reshape(n, units, width)
    small_send[:, units:, :] = dense_up_ref[...].T.reshape(n, units, width)
    top_k = routes_ref.shape[0]
    for k in range(top_k):
        routes_all[me, :, k * rows : (k + 1) * rows] = routes_ref[k : k + 1, :].astype(f32)

    queries = jnp.zeros((rows, w_query.shape[1]), f32)
    for i in range(4):
        loads[5 + i].wait()
        if i % 2:
            values_load(i // 2).start()
        part = slice(i * quarter, (i + 1) * quarter)
        queries = queries + jnp.dot(
            normed_ref[:, part], w_query[part, :], preferred_element_type=f32
        )
    queries = queries.astype(bf16).astype(f32)
    for h in range(local_heads):
        query_ref[:, h, :] = queries[:, h * head_dim : (h + 1) * head_dim]

    block_len = min(256, cache_len)
    after_mask = (
        lax.broadcasted_iota(jnp.int32, (block_len, block_len), 0)
        > lax.broadcasted_iota(jnp.int32, (block_len, block_len), 1)
    ).astype(bf16)
    position = lax.broadcasted_iota(jnp.int32, (lines, block_len), 1)
    arrived(bias_ref, lengths_ref)
    head_row = lax.broadcasted_iota(jnp.int32, (local_heads, local_heads), 0)
    head_col = lax.broadcasted_iota(jnp.int32, (local_heads, local_heads), 1)
    bias = jnp.sum(jnp.where(head_row == head_col, bias_ref[...], 0.0), axis=1, keepdims=True)
    line_seq = lax.broadcasted_iota(jnp.int32, (lines, rows), 0) // local_heads
    seq_lane = lax.broadcasted_iota(jnp.int32, (lines, rows), 1)
    lengths_row = lengths_ref[...].astype(f32)

    for s in range(rows):
        if s % span == 0:
            keys_load(s // span).wait()
            for load in loads[12:16] if s == 0 else loads[16:]:
                load.start()
        score_ref[s] = (
            jnp.dot(query_ref[s].astype(bf16), keys[s], preferred_element_type=f32)
            * head_dim ** (-0.5)
            + bias
        )

    def stick_breaking(c):
        limits = jnp.sum(
            jnp.where(seq_lane == line_seq + c * span, lengths_row, 0.0), axis=1, keepdims=True
        ).astype(jnp.int32)
        later = jnp.zeros((lines, 1), f32)
        for first_pos in range(cache_len - block_len, -1, -block_len):
            columns = slice(first_pos, first_pos + block_len)
            scores = score_ref[c * span : (c + 1) * span, :, columns].reshape(lines, block_len)
            visible = position + first_pos < limits
            keep = -(jnp.maximum(scores, 0.0) + jnp.log(1.0 + jnp.exp(-jnp.abs(scores))))
            log_take = scores + keep
            keep = jnp.where(visible, keep, 0.0)
            top = keep.astype(bf16)
            low = (keep - top.astype(f32)).astype(bf16)
            sums = jnp.dot(
                jnp.concatenate([top, low], axis=0), after_mask, preferred_element_type=f32
            )
            after = sums[:lines] + sums[lines:] + later
            later = later + jnp.sum(keep, axis=-1, keepdims=True)
            stick = jnp.where(visible, jnp.exp(log_take + after), 0.0)
            stick_ref[c, :, columns] = stick.astype(bf16)

    def read_values(c):
        mixed = lax.dot_general(
            values[c * span : (c + 1) * span].reshape(span * head_dim, cache_len),
            stick_ref[c],
            (((1,), (1,)), ((), ())),
            preferred_element_type=f32,
        ).reshape(span, head_dim, lines)
        seq_of = lax.broadcasted_iota(jnp.int32, (head_dim, lines), 1) // local_heads
        own_seq = jnp.zeros((head_dim, lines), f32)
        for s in range(span):
            own_seq = jnp.where(seq_of == s, mixed[s], own_seq)
        read_ref[c * span : (c + 1) * span] = own_seq.T.reshape(span, local_heads, head_dim)

    for c in range(2):
        stick_breaking(c)
    pl.semaphore_wait(barrier, 2 * n - 1)
    trades = [
        remote(
            w_gate_hbm.at[far, :], w_gate.at[:, mine], pair_sems.at[0, 0], pair_sems.at[1, 0], me, peer
        ),
        remote(
            w_up_hbm.at[far, :], w_up.at[:, mine], pair_sems.at[0, 1], pair_sems.at[1, 1], me, peer
        ),
        remote(
            w_down_hbm.at[:, far], w_down.at[mine, :], pair_sems.at[0, 2], pair_sems.at[1, 2], me, peer
        ),
    ]

    def small_copy(other, tp):
        return remote(
            small_send.at[other],
            small.at[pl.ds(core * 2 * units, 2 * units), pl.ds(pl.multiple_of(slot * width, width), width)],
            small_send_sem.at[other],
            small_recv_sem.at[core, slot],
            other,
            tp,
        )

    def down_copy(other, tp):
        return remote(
            down_ref.at[pl.ds(pl.multiple_of(other * units, units), units), :],
            w_down.at[
                pl.ds(2 * hidden + core * 2 * units, units),
                pl.ds(pl.multiple_of(slot * width, width), width),
            ],
            down_send_sem.at[other],
            down_recv_sem.at[core, slot],
            other,
            tp,
        )

    def routes_copy(origin, other):
        return remote(
            routes_all.at[origin],
            routes_all.at[origin],
            routes_sems.at[0, other],
            routes_sems.at[1, origin],
            other,
            core,
        )

    arrived(down_ref)

    def send_small(k, carry):
        other = lax.rem(me + k, n)
        routes_copy(me, other).start()
        small_copy(other, owner).start()
        return carry

    def send_down(k, carry):
        down_copy(lax.rem(me + k, n), owner).start()
        return carry

    lax.fori_loop(1, n, send_small, 0)

    @pl.when(owner == core)
    def _():
        here = pl.ds(pl.multiple_of(slot * width, width), width)
        small[pl.ds(pl.multiple_of(core * 2 * units, 2 * units), 2 * units), here] = small_send[me]
        w_down[
            pl.ds(pl.multiple_of(2 * hidden + core * 2 * units, units), units), here
        ] = down_ref[pl.ds(pl.multiple_of(me * units, units), units), :]

    @pl.when(owner != core)
    def _():
        small_copy(me, peer).start()

    for c in range(2):
        values_load(c).wait()
    for c in range(2):
        read_values(c)
    heads_out = jnp.concatenate([read_ref[:, h, :] for h in range(local_heads)], axis=1).astype(
        bf16
    )
    arrived(w_out)
    swaps = []
    for i in range(2):
        attn_mine[i] = jnp.dot(
            heads_out, w_out[:, i * half : (i + 1) * half], preferred_element_type=f32
        ).astype(bf16)
        swaps.append(
            remote(
                attn_mine.at[i], attn_peer.at[i], swap_sems.at[0, i], swap_sems.at[1, i], me, peer
            )
        )
        swaps[i].start()
    for trade in trades:
        trade.start()
    arrived(gain_ref)
    wide = []
    for i in range(2):
        swaps[i].wait_recv()
        columns = slice(i * half, (i + 1) * half)
        res_ref[i] = (
            tokens_ref[:, columns].astype(f32)
            + (attn_mine[i].astype(f32) + attn_peer[i].astype(f32))
        ).astype(bf16)
        wide.append(res_ref[i].astype(f32))
    squares = sum(jnp.sum(part * part, axis=-1, keepdims=True) for part in wide)
    scale = lax.rsqrt(squares / model + 1e-06)
    norm_all[me] = (
        jnp.where(core == 0, wide[0], wide[1])
        * scale
        * jnp.where(core == 0, gain_ref[:, :half], gain_ref[:, half:])
    ).astype(bf16)

    def line_copy(k):
        return remote(
            norm_all.at[me],
            norm_all.at[me],
            line_sems.at[0, k],
            line_sems.at[1, k],
            flip(z, k) * inner + p,
            core,
        )

    def spread_copy(k, j):
        origin = flip(z, k) * inner + p
        return remote(
            norm_all.at[origin],
            norm_all.at[origin],
            spread_sems.at[0, k, j],
            spread_sems.at[1, k, j],
            z * inner + flip(p, j),
            core,
        )

    def around_copy(k, j):
        origin = z * inner + flip(p, j)
        return remote(
            norm_all.at[origin],
            norm_all.at[origin],
            spread_sems.at[0, k, j],
            spread_sems.at[1, k, j],
            flip(z, k) * inner + p,
            core,
        )

    for k in turns:
        line_copy(k).start()
    for j in indirect + direct:
        spread_copy(0, j).start()


    lax.fori_loop(1, n, send_down, 0)

    @pl.when(owner != core)
    def _():
        down_copy(me, peer).start()

    across = (((1,), (1,)), ((), ()))
    arrived(w_key_ref, w_value_ref)
    for weight, target in ((w_key_ref, new_keys_ref), (w_value_ref, new_values_ref)):
        target[...] = lax.dot_general(
            normed_ref[...], weight[...], across, preferred_element_type=f32
        ).astype(bf16)

    def small_taken(tp, k):
        return remote(
            small_send.at[0],
            small.at[
                pl.ds(tp * 2 * units, 2 * units), pl.ds(pl.multiple_of(k * width, width), width)
            ],
            small_send_sem.at[0],
            small_recv_sem.at[tp, k],
            me,
            peer,
        )

    def down_taken(tp, k):
        return remote(
            down_ref.at[pl.ds(0, units), :],
            w_down.at[
                pl.ds(2 * hidden + tp * 2 * units, units),
                pl.ds(pl.multiple_of(k * width, width), width),
            ],
            down_send_sem.at[0],
            down_recv_sem.at[tp, k],
            me,
            peer,
        )

    def take_all(taken):
        def take(k, carry):
            @pl.when(core * side + k != me)
            def _():
                taken(core, k).wait_recv()

            taken(peer, k).wait_recv()
            return carry

        lax.fori_loop(0, side, take, 0)

    arrived(router_ref, mix_ref)
    spread_rows = lanes - mix_at
    mix_row = mix_ref[...]
    mix_top = mix_row.astype(bf16)
    mix_rest = mix_row - mix_top.astype(f32)
    mix_mid = mix_rest.astype(bf16)
    mix_low = (mix_rest - mix_mid.astype(f32)).astype(bf16)
    mix_index = lax.broadcasted_iota(jnp.int32, (spread_rows, model), 0)
    mix_rows = jnp.where(
        mix_index == 0,
        mix_top.astype(f32),
        jnp.where(
            mix_index == 1,
            mix_mid.astype(f32),
            jnp.where(mix_index == 2, mix_low.astype(f32), 0.0),
        ),
    ).astype(bf16)
    small[pl.ds(router_at, expert_total), :] = jnp.where(
        core == 0, router_ref[:, :half], router_ref[:, half:]
    )
    small[pl.ds(mix_at, spread_rows), :] = jnp.where(
        core == 0, mix_rows[:, :half], mix_rows[:, half:]
    )
    for base in (units, 3 * units):
        w_down[pl.ds(2 * hidden + base, units), :] = jnp.zeros((units, half), bf16)
    tail = lanes - 4 * units
    w_down[pl.ds(2 * hidden + 4 * units, tail), :] = jnp.zeros((tail, half), bf16)

    for k in turns:
        line_copy(k).wait_recv()
        for j in direct if k in around else indirect + direct:
            spread_copy(k, j).start()
        if k == turns[0]:
            for j in indirect:
                spread_copy(0, j).wait_recv()
                for m in around:
                    around_copy(m, j).start()
    take_all(small_taken)

    arrived(*[target for _, target in pairs[18:]])
    for trade in trades:
        trade.wait_recv()

    chunk = inner * rows
    lane = lax.broadcasted_iota(jnp.int32, (chunk, lanes), 1)
    dense_lane = (lane < units) | ((lane >= 2 * units) & (lane < 3 * units))

    rest_at = 2 * hidden + lanes

    def first_copy(k):
        return remote(
            first_send.at[k], first_recv.at[k], first_sems.at[0, k], first_sems.at[1, k], me, peer
        )

    def group(k):
        return pl.ds(pl.multiple_of(flip(z, k) * inner, inner), inner)

    def first(*ks):
        for k in ks:
            for j in range(1, inner) if k else direct:
                spread_copy(k, j).wait_recv()
        x = jnp.concatenate([norm_all[group(k)].reshape(chunk, half) for k in ks], axis=0)
        gate_rows = jnp.dot(x, w_gate[...], preferred_element_type=f32)
        rest = lax.dot_general(x, small[...], across, preferred_element_type=f32)
        up_rows = jnp.dot(x, w_up[...], preferred_element_type=f32)
        for i, k in enumerate(ks):
            own_rows = slice(i * chunk, (i + 1) * chunk)
            first_send[k, :, : 2 * hidden] = gate_rows[own_rows]
            first_send[k, :, 2 * hidden : rest_at] = rest[own_rows]
            first_send[k, :, rest_at:] = up_rows[own_rows]
        for k in ks:
            first_copy(k).start()

    def plane_copy(k, j):
        other = flip(p, j)
        return remote(
            plane_send.at[k, other],
            plane_recv.at[k, j],
            plane_sems.at[0, k, j],
            plane_sems.at[1, k, j],
            z * inner + other,
            core,
        )

    def far_copy(k, j):
        return remote(
            plane_send.at[k, flip(p, j)],
            far_recv.at[k, j],
            far_sems.at[0, k, j],
            far_sems.at[1, k, j],
            flip(z, k) * inner + p,
            core,
        )

    def send_plane(k):
        for j in indirect:
            if k in homeward:
                far_copy(k, j).start()
            elif k:
                plane_copy(k, j).start()
        for j in direct:
            plane_copy(k, j).start()

    def activations(k):
        gate_rows = first_send[k, :, : 2 * hidden] + first_recv[k, :, : 2 * hidden]
        up_rows = first_send[k, :, rest_at:] + first_recv[k, :, rest_at:]
        rest = first_send[k, :, 2 * hidden : rest_at] + first_recv[k, :, 2 * hidden : rest_at]
        chosen = hits_ref[group(k)].reshape(chunk, lanes)
        picked = jnp.where(chosen > 0.0, jax.nn.sigmoid(rest), 0.0)
        total = jnp.sum(picked, axis=-1, keepdims=True)
        own = jnp.sum(jnp.where(lane == router_at + me, picked, 0.0), axis=-1, keepdims=True)
        gate = own / total * 2.5
        mix_sum = jnp.sum(jnp.where(lane >= mix_at, rest, 0.0), axis=-1, keepdims=True)
        mix_gate = jax.nn.sigmoid(mix_sum)
        dense = jax.nn.silu(rest) * pltpu.roll(rest, lanes - units, 1) * mix_gate
        dense = jnp.where(dense_lane, dense, 0.0).astype(bf16)
        return (jax.nn.silu(gate_rows) * up_rows * gate).astype(bf16), dense

    def second(*ks):
        for k in ks:
            first_copy(k).wait_recv()
        parts = [activations(k) for k in ks]
        act = jnp.concatenate([part[0] for part in parts], axis=0)
        dense = jnp.concatenate([part[1] for part in parts], axis=0)
        value = jnp.dot(act, w_down[: 2 * hidden], preferred_element_type=f32) + jnp.dot(
            dense, w_down[2 * hidden :], preferred_element_type=f32
        )
        for i, k in enumerate(ks):
            own_rows = value[i * chunk : (i + 1) * chunk]
            plane_send[k] = own_rows.astype(bf16).reshape(inner, rows, half)
        for k in ks:
            if k:
                send_plane(k)

    def far_home(j):
        return remote(
            far_recv.at[0, j],
            plane_recv.at[0, j],
            plane_sems.at[0, 0, j],
            plane_sems.at[1, 0, j],
            z * inner + flip(p, j),
            core,
        )

    def back_copy(k):
        return remote(
            line_send.at[k],
            line_recv.at[k],
            back_sems.at[0, k],
            back_sems.at[1, k],
            flip(z, k) * inner + p,
            core,
        )

    def collect(k):
        total = plane_send[k, p].astype(f32)
        for j in direct + (indirect if k and k not in homeward else []):
            plane_copy(k, j).wait_recv()
            total = total + plane_recv[k, j].astype(f32)
        return total

    def third(k):
        line_send[k] = collect(k).astype(bf16)
        back_copy(k).start()

    first(0)
    def take_routes(k, carry):
        routes_copy(lax.rem(me + n - k, n), me).wait_recv()
        return carry

    lax.fori_loop(1, n, take_routes, 0)
    row_lane = (lax.broadcasted_iota(jnp.int32, (rows, lanes), 1) - router_at).astype(f32)
    named = routes_all[...].reshape(n, lanes).T
    for j in range(n):
        hit = jnp.zeros((rows, lanes), f32)
        for c in range(top_k):
            hit = jnp.where(named[c * rows : (c + 1) * rows, j : j + 1] == row_lane, 1.0, hit)
        hits_ref[j] = hit

    take_all(down_taken)
    second(0)
    first(turns[0])
    for k in turns[1:]:
        first(k)
    for k in turns:
        second(k)
    send_plane(0)
    for k in turns[:-1]:
        third(k)
    for j in indirect:
        other = flip(p, j)
        total = plane_send[0, other].astype(f32)
        for k in homeward:
            far_copy(k, j).wait_recv()
            total = total + far_recv[k, j].astype(f32)
        far_recv[0, j] = total.astype(bf16)
        far_home(j).start()
    third(turns[-1])
    def drain(k, carry):
        other = lax.rem(me + k, n)
        routes_copy(me, other).wait_send()
        small_copy(other, owner).wait_send()
        down_copy(other, owner).wait_send()
        return carry

    lax.fori_loop(1, n, drain, 0)

    @pl.when(owner != core)
    def _():
        small_copy(me, peer).wait_send()
        down_copy(me, peer).wait_send()

    for copy in trades + swaps:
        copy.wait_send()
    for k in range(outer):
        if k:
            line_copy(k).wait_send()
        first_copy(k).wait_send()
        for j in range(1, inner):
            (around_copy if k in around and j in indirect else spread_copy)(k, j).wait_send()

    total = res_ref[core].astype(f32) + collect(0)
    for k in turns:
        back_copy(k).wait_recv()
        total = total + line_recv[k].astype(f32)
    for j in indirect:
        far_home(j).wait_recv()
        total = total + plane_recv[0, j].astype(f32)
    out_ref[...] = total.astype(bf16)

    for k in range(outer):
        if k:
            back_copy(k).wait_send()
        for j in range(1, inner):
            if k == 0 and j in indirect:
                far_home(j).wait_send()
            else:
                (far_copy if k in homeward and j in indirect else plane_copy)(k, j).wait_send()


def routed_shards(n, inner, arrays):
    tokens = arrays[0]
    w_key, head_bias = arrays[4], arrays[3]
    keys, w_gate, w_down = arrays[18], arrays[15], arrays[17]
    rows, model = tokens.shape
    half = model // 2
    width, hidden_cols = arrays[10].shape
    units = hidden_cols // n
    outer = n // inner
    seq_count, head_dim, cache_len = keys.shape
    local_heads = head_bias.shape[1]
    hidden = w_gate.shape[1]
    lanes = 128
    chunk = inner * rows
    bf16, f32 = jnp.bfloat16, jnp.float32
    vmem = pl.BlockSpec(memory_space=pltpu.VMEM)
    anywhere = pl.BlockSpec(memory_space=pltpu.HBM)
    dma = pltpu.SemaphoreType.DMA
    small_inputs = [pltpu.VMEM(a.shape, a.dtype) for a in arrays[:15]]
    results = pl.pallas_call(
        functools.partial(routed_layer, n, inner),
        out_shape=(
            jax.ShapeDtypeStruct((rows, half), bf16),
            jax.ShapeDtypeStruct((rows, w_key.shape[0]), bf16),
            jax.ShapeDtypeStruct((rows, w_key.shape[0]), bf16),
        ),
        in_specs=[anywhere] * 20,
        out_specs=(vmem, vmem, vmem),
        scratch_shapes=small_inputs
        + [
            pltpu.VMEM((half, 2 * hidden), bf16),
            pltpu.VMEM((half, 2 * hidden), bf16),
            pltpu.VMEM((2 * hidden + lanes, half), bf16),
            pltpu.VMEM(keys.shape, bf16),
            pltpu.VMEM(keys.shape, bf16),
            pltpu.VMEM((rows, local_heads, head_dim), f32),
            pltpu.VMEM((rows, local_heads, cache_len), f32),
            pltpu.VMEM((rows, local_heads, head_dim), f32),
            pltpu.VMEM((2, rows * local_heads // 2, cache_len), bf16),
            pltpu.VMEM((rows, model), bf16),
            pltpu.VMEM((n, 2 * units, width), bf16),
            pltpu.VMEM((lanes, half), bf16),
            pltpu.VMEM((n, 1, lanes), f32),
            pltpu.VMEM((n, rows, lanes), f32),
            pltpu.VMEM((2, rows, half), bf16),
            pltpu.VMEM((2, rows, half), bf16),
            pltpu.VMEM((2, rows, half), bf16),
            pltpu.VMEM((n, rows, half), bf16),
            pltpu.VMEM((outer, chunk, 4 * hidden + lanes), f32),
            pltpu.VMEM((outer, chunk, 4 * hidden + lanes), f32),
            pltpu.VMEM((outer, inner, rows, half), bf16),
            pltpu.VMEM((outer, inner, rows, half), bf16),
            pltpu.VMEM((outer, inner, rows, half), bf16),
            pltpu.VMEM((outer, rows, half), bf16),
            pltpu.VMEM((outer, rows, half), bf16),
            dma((21,)),
            dma((2,)),
            dma((2,)),
            dma((2, 3)),
            dma((2, 2)),
            dma((n,)),
            dma((2, n // 2)),
            dma((n,)),
            dma((2, n // 2)),
            dma((2, n)),
            dma((2, outer)),
            dma((2, outer, inner)),
            dma((2, outer)),
            dma((2, outer, inner)),
            dma((2, outer, inner)),
            dma((2, outer)),
        ],
        compiler_params=pltpu.CompilerParams(
            collective_id=0, has_side_effects=True, vmem_limit_bytes=48 * 1024 * 1024
        ),
        name="routed_layer",
    )(*[pltpu.with_memory_space_constraint(a, pltpu.HBM) for a in arrays])
    return pl.pallas_call(
        finish,
        out_shape=tuple(jax.ShapeDtypeStruct(r.shape, r.dtype) for r in results),
        in_specs=[vmem] * 3,
        out_specs=(anywhere,) * 3,
        scratch_shapes=[dma((3,))],
        name="finish",
    )(*[pltpu.with_memory_space_constraint(r, pltpu.VMEM) for r in results])


def shards(
    n,
    tokens,
    lengths,
    attn_gain,
    w_query,
    w_key,
    w_value,
    head_bias,
    key_cache,
    value_cache,
    w_attn_out,
    ffn_gain,
    w_router,
    routes,
    w_dense_gate,
    w_dense_up,
    w_dense_down,
    dense_mix,
    w_expert_gate,
    w_expert_up,
    w_expert_down,
):
    rows, model = tokens.shape
    half = model // 2
    width, hidden_cols = w_dense_gate.shape
    group_size = min(n, max(4, 128 // width))
    teams = n // group_size
    window = width * group_size
    seq_count, local_kv, head_dim, cache_len = key_cache.shape
    local_heads = head_bias.shape[0]
    keys = key_cache.reshape(seq_count, head_dim, cache_len)
    values = value_cache.reshape(seq_count, head_dim, cache_len)
    w_gate, w_up, w_down = w_expert_gate[0], w_expert_up[0], w_expert_down[0]
    expert_hidden = w_gate.shape[1]
    arrays = (
        tokens,
        attn_gain.reshape(1, model),
        lengths.reshape(1, seq_count),
        head_bias.reshape(1, local_heads),
        w_key.T,
        w_value.T,
        ffn_gain.reshape(1, model),
        w_router.T,
        routes.T,
        dense_mix.reshape(1, model),
        w_dense_gate,
        w_dense_up,
        w_dense_down,
        w_query,
        w_attn_out,
        w_gate,
        w_up,
        w_down,
        keys,
        values,
    )
    inner = 1
    while (2 * inner) ** 2 <= n:
        inner *= 2
    small_rows = 4 * (hidden_cols // n) + w_router.shape[1]
    if hidden_cols % (16 * n) == 0 and width % 128 == 0 and small_rows <= 112:
        return routed_shards(n, inner, arrays)
    bf16, f32 = jnp.bfloat16, jnp.float32
    block = min(n, 16) * rows
    vmem = pl.BlockSpec(memory_space=pltpu.VMEM)
    anywhere = pl.BlockSpec(memory_space=pltpu.HBM)
    dma = pltpu.SemaphoreType.DMA
    return pl.pallas_call(
        functools.partial(whole_layer, n, group_size),
        out_shape=(
            jax.ShapeDtypeStruct((rows, half), bf16),
            jax.ShapeDtypeStruct((rows, w_key.shape[1]), bf16),
            jax.ShapeDtypeStruct((rows, w_value.shape[1]), bf16),
        ),
        in_specs=[vmem] * 13 + [anywhere] * 7,
        out_specs=(vmem, vmem, vmem),
        scratch_shapes=[
            pltpu.VMEM(w_query.shape, bf16),
            pltpu.VMEM(w_attn_out.shape, bf16),
            pltpu.VMEM(w_gate.shape, bf16),
            pltpu.VMEM(w_up.shape, bf16),
            pltpu.VMEM(w_down.shape, bf16),
            pltpu.VMEM(keys.shape, bf16),
            pltpu.VMEM(values.shape, bf16),
            dma((5,)),
            dma((rows // 4,)),
            dma((rows // 4,)),
            pltpu.VMEM((rows, local_heads, head_dim), f32),
            pltpu.VMEM((rows, local_heads, cache_len), f32),
            pltpu.VMEM((rows, local_heads, head_dim), f32),
            pltpu.VMEM((rows, model), bf16),
            pltpu.VMEM((group_size, width, hidden_cols), bf16),
            pltpu.VMEM((group_size, width, hidden_cols), bf16),
            pltpu.VMEM((group_size, hidden_cols, width), bf16),
            pltpu.VMEM((rows, model), bf16),
            pltpu.VMEM((rows, model), bf16),
            pltpu.VMEM((rows, model), bf16),
            pltpu.VMEM((2, n, rows, half), bf16),
            pltpu.VMEM((teams, rows, 2 * hidden_cols), bf16),
            pltpu.VMEM((teams, rows, 2 * hidden_cols), bf16),
            pltpu.VMEM((n * rows // block, block, expert_hidden), bf16),
            pltpu.VMEM((teams, rows, hidden_cols), bf16),
            pltpu.VMEM((teams, rows, window), bf16),
            pltpu.VMEM((2, teams, rows, window), bf16),
            pltpu.VMEM((n, rows, half), bf16),
            pltpu.VMEM((n, rows, half), bf16),
            pltpu.VMEM((n, rows, half), bf16),
            pltpu.VMEM((n, rows, half), bf16),
            pltpu.VMEM((n, rows, half), bf16),
            dma((4,)),
            dma((2, group_size)),
            dma((2, group_size)),
            dma((2, group_size)),
            dma((2, n)),
            dma((2, n)),
            dma((2, teams)),
            dma((2, teams)),
            dma((teams,)),
            dma((2, teams)),
            dma((2, n)),
        ],
        compiler_params=pltpu.CompilerParams(
            collective_id=0, has_side_effects=True, vmem_limit_bytes=63 * 1024 * 1024
        ),
        name="whole_layer",
    )(*arrays)


def solution(mesh):
    return jax.shard_map(
        functools.partial(shards, mesh.shape["ep"]),
        mesh=mesh,
        in_specs=(
            P("ep", None),
            P("ep"),
            P(),
            P(None, "tp"),
            P(None, "tp"),
            P(None, "tp"),
            P("tp"),
            P("ep", "tp", None, None),
            P("ep", "tp", None, None),
            P("tp", None),
            P(),
            P(),
            P("ep", None),
            P("ep", "tp"),
            P("ep", "tp"),
            P("tp", "ep"),
            P(),
            P("ep", None, "tp"),
            P("ep", None, "tp"),
            P("ep", "tp", None),
        ),
        out_specs=(P("ep", "tp"), P("ep", "tp"), P("ep", "tp")),
        check_vma=False,
    )
```
